32 devices in a mesh: sp: 8 (over z, y), tp: 4 (over x, core).
Axes of the slice: x: 2, y: 2, z: 4, core: 2. Of those that a mesh axis runs over, the one named last changes fastest.
Arguments:
- gate_branch: bfloat16 [6144, 1024], P('sp', 'tp'), may hold values from -6 to 6
- recur_input: bfloat16 [6144, 1024], P('sp', 'tp'), may hold values from -6 to 6
- doc_ids: int32 [6144], P('sp'), may hold values from 0 to 3, never falling along the last dimension, each value on 1 to 4608 neighbouring positions
- conv_taps: bfloat16 [4, 1024], P(None, 'tp'), may hold values from -3 to 3
- gate_map: bfloat16 [16, 64, 64], P('tp'), may hold values from -0.75 to 0.75
- input_map: bfloat16 [16, 64, 64], P('tp'), may hold values from -0.75 to 0.75
- decay_level: float32 [1024], P('tp'), may hold values from 4.8 to 12.3
- decay_extra: float32 [6144, 1024], P('sp', 'tp'), may hold values from -2.1 to -1.9e-05
- out_weight: bfloat16 [1024, 2048], P(None, 'tp'), may hold values from -0.7875 to 0.7875
- residual: bfloat16 [6144, 2048], P('sp', 'tp'), may hold values from -44 to 44
- mix_gain: float32 [2048], P('tp'), may hold values from 0.1 to 1.9
- pre_gain: float32 [2048], P('tp'), may hold values from 0.1 to 1.9
- ffn_gain: float32 [2048], P('tp'), may hold values from 0.1 to 1.9
- gate_weight: bfloat16 [2048, 5632], P('sp', 'tp'), may hold values from -0.125 to 0.125
- up_weight: bfloat16 [2048, 5632], P('sp', 'tp'), may hold values from -0.125 to 0.125
- down_weight: bfloat16 [5632, 2048], P('tp', 'sp'), may hold values from -0.33579113 to 0.33579113
Outputs:
- layer_out: bfloat16 [6144, 2048], P('sp', 'tp')
The draws below stay inside these ranges and needn't reach their ends.
Inputs may be any that keep to these rules, and one draw needn't show every extreme that they name: `doc_ids`: document numbers start at 0 and never fall along the sequence; a document has 1 to 4608 positions, and one has exactly that many.
All inputs are finite; a program needn't handle non-finite values.
Results may differ from the reference program's by a relative error of at most 0.013.
Values may be sent and summed in bfloat16 or wider, within the bound.
A program may use at most 64 MiB of HBM per device.

```python
import math
import jax
import jax.numpy as jnp
import numpy as np
from jax import lax

D = 2048
W = 1024
HEAD = 64
FF = 5632
KCONV = 4
TOK_DEV = 768
TOKENS = 6144
DOCS = 4
N_TP = 4


def column_scales(key, columns, spread):
    ramp = jnp.exp(jnp.log(spread) * jnp.arange(columns, dtype=jnp.float32) / (columns - 1))
    jitter = jnp.exp(jax.random.uniform(key, (columns,), jnp.float32, math.log(0.7), math.log(1.4)))
    return ramp * jitter / math.sqrt(spread)


def scaled_matrix(key, row_count, columns):
    spread = 3.0
    keys = jax.random.split(key, 2)
    base = jnp.clip(jax.random.normal(keys[0], (row_count, columns), jnp.float32), -6.0, 6.0)
    return base * row_count ** (-0.5) * column_scales(keys[1], columns, spread)


def draw_out_weight(key, part):
    return scaled_matrix(jax.random.fold_in(key, 11), W, D).astype(jnp.bfloat16)


def draw_down_weight(key, part):
    return scaled_matrix(jax.random.fold_in(key, 12), FF, D).astype(jnp.bfloat16)


def draw_residual(key, part):
    keys = jax.random.split(jax.random.fold_in(key, 13), 3)
    spread = 3.0
    base = jnp.clip(jax.random.normal(keys[0], (TOKENS, D), jnp.float32), -6.0, 6.0)
    row_scale = jnp.exp(jax.random.uniform(keys[1], (TOKENS, 1), jnp.float32, math.log(0.3), math.log(3.0)))
    return (base * row_scale * column_scales(keys[2], D, spread)).astype(jnp.bfloat16)


def draw_decay_level(key, part):
    keys = jax.random.split(jax.random.fold_in(key, 14), 3)
    share = 0.5
    fast_heads = jax.random.uniform(keys[0], (W // HEAD, 1), jnp.float32) < share
    fast = jnp.broadcast_to(fast_heads, (W // HEAD, HEAD)).reshape(W)
    fast_rate = jnp.exp(jax.random.uniform(keys[1], (W,), jnp.float32, math.log(0.0025), math.log(0.008)))
    slow_rate = jnp.exp(jax.random.uniform(keys[2], (W,), jnp.float32, math.log(5e-06), math.log(2e-05)))
    target = jnp.where(fast, fast_rate, slow_rate)
    return -jnp.log(jnp.expm1(target))


def draw_decay_extra(key, part):
    keys = jax.random.split(jax.random.fold_in(key, 15), 3)
    blocks = TOKENS // TOK_DEV
    baseline = jnp.exp(jax.random.uniform(keys[0], (blocks, 1, W), jnp.float32, math.log(2e-05), math.log(0.0001)))
    baseline = jnp.broadcast_to(baseline, (blocks, TOK_DEV, W)).reshape(TOKENS, W)
    spots = jax.random.randint(keys[1], (3,), 0, TOKENS)
    hits = jnp.sum((jnp.arange(TOKENS)[:, None] == spots[None, :]).astype(jnp.float32), axis=1)
    kept = jax.random.uniform(keys[2], (TOKENS, W), jnp.float32, 0.5, 0.8)
    return -baseline + hits[:, None] * jnp.log(kept)


def level_of(stream_key, extent, cuts, low, high):
    def one(axis_at, blocks):
        draws = jax.random.uniform(jax.random.fold_in(jax.random.fold_in(stream_key, 6), axis_at), (blocks,), jnp.float32, low / len(cuts), high / len(cuts))
        return jnp.repeat(jnp.exp(draws), extent[axis_at] // blocks).reshape((-1,) + (1,) * (len(extent) - axis_at - 1))

    gain = one(*cuts[0])
    for cut in cuts[1:]:
        gain = gain * one(*cut)
    return gain


def length_profile(number_of, total, most, skew):
    loads = [(1 << 20) // math.isqrt(standing ** skew) + 1 for standing in range(2, number_of + 1)]
    spare, counts = total - most - (number_of - 1), [1] * (number_of - 1)
    while spare > 0:
        free = [i for i in range(number_of - 1) if counts[i] < most]
        whole, left = sum([loads[i] for i in free]), spare
        for i in free:
            addition = min(most - counts[i], max(1, left * loads[i] // whole), spare)
            counts[i] = counts[i] + addition
            spare = spare - addition
    return np.array([most] + counts)


def uneven_parts(stream_key, amount, total, most, lean):
    if amount == 2:
        one = jax.random.randint(stream_key, (), max(1, total - most), min(most, total - 1) + 1)
        return jnp.stack([one, total - one])
    sizes = jnp.asarray(length_profile(amount, total, most, lean), jnp.int32)
    couples = (amount - 1) // 2
    donor, taker = sizes[1:1 + 2 * couples:2], sizes[2:2 + 2 * couples:2]
    room = jnp.minimum(donor - 1, most - taker)
    passed = jax.random.randint(jax.random.fold_in(stream_key, 1), (couples,), 0, 1 << 20) % (room + 1)
    sizes = sizes.at[1:1 + 2 * couples:2].set(donor - passed).at[2:2 + 2 * couples:2].set(taker + passed)
    return sizes[jax.random.permutation(jax.random.fold_in(stream_key, 2), amount)]


def centred(key, shape, width, most, cuts=(), kind=jnp.bfloat16):
    loudness = level_of(key, shape, cuts, -0.22, 0.18) if cuts else 1.0
    entries = jax.random.normal(key, shape, jnp.float32) * width * loudness
    return jnp.minimum(jnp.maximum(entries, -most), most).astype(kind)


def setup_inputs(seed: int = 0) -> dict:
    arg_keys = jax.random.split(jax.random.key(seed), 17)
    return {
        "gate_branch": centred(arg_keys[0], (TOKENS, W), 1.0, 6.0, ((0, 8), (1, 4))),
        "recur_input": centred(arg_keys[1], (TOKENS, W), 1.0, 6.0, ((0, 8), (1, 4))),
        "doc_ids": jnp.searchsorted(jnp.cumsum(uneven_parts(arg_keys[2], DOCS, TOKENS, 6 * TOK_DEV, 0)), jnp.arange(TOKENS), side="right").astype(jnp.int32),
        "conv_taps": centred(arg_keys[3], (KCONV, W), 0.5, 3.0, ((1, 4),)),
        "gate_map": centred(arg_keys[4], (W // HEAD, HEAD, HEAD), HEAD ** -0.5, 0.75, ((0, 4),)),
        "input_map": centred(arg_keys[5], (W // HEAD, HEAD, HEAD), HEAD ** -0.5, 0.75, ((0, 4),)),
        "decay_level": draw_decay_level(jax.random.fold_in(arg_keys[16], 71), 0),
        "decay_extra": draw_decay_extra(jax.random.fold_in(arg_keys[16], 71), 0),
        "out_weight": draw_out_weight(jax.random.fold_in(arg_keys[16], 71), 0),
        "residual": draw_residual(jax.random.fold_in(arg_keys[16], 71), 0),
        "mix_gain": jnp.clip(1.0 + 0.18 * jax.random.normal(arg_keys[10], (D,), jnp.float32), 0.1, 1.9),
        "pre_gain": jnp.clip(1.0 + 0.18 * jax.random.normal(arg_keys[11], (D,), jnp.float32), 0.1, 1.9),
        "ffn_gain": jnp.clip(1.0 + 0.18 * jax.random.normal(arg_keys[12], (D,), jnp.float32), 0.1, 1.9),
        "gate_weight": centred(arg_keys[13], (D, FF), D ** -0.5, 0.125, ((0, 8), (1, 4))),
        "up_weight": centred(arg_keys[14], (D, FF), D ** -0.5, 0.125, ((0, 8), (1, 4))),
        "down_weight": draw_down_weight(jax.random.fold_in(arg_keys[16], 71), 0),
    }


epsilon = 1e-06
gate_power = 8.0

def combine(earlier, latter):
    return (earlier[0] * latter[0], latter[0] * earlier[1] + latter[1])

def inverse_rms(values, columns):
    return lax.rsqrt(lax.optimization_barrier(jnp.sum(values * values, axis=1, keepdims=True)) / columns + epsilon)

def reference(gate_branch, recur_input, doc_ids, conv_taps, gate_map, input_map, decay_level, decay_extra, out_weight, residual, mix_gain, pre_gain, ffn_gain, gate_weight, up_weight, down_weight):
    reach_rows = KCONV - 1
    padded_ids = jnp.concatenate([jnp.full((reach_rows,), -1, jnp.int32), doc_ids.astype(jnp.int32)])
    padded_rows = jnp.concatenate([jnp.zeros((reach_rows, W), jnp.float32), recur_input.astype(jnp.float32)])
    tap_weights = conv_taps.astype(jnp.float32)
    convolved = jnp.zeros((TOKENS, W), jnp.float32)
    for offset in range(KCONV):
        start_row = reach_rows - offset
        same_doc = (padded_ids[start_row:start_row + TOKENS] == doc_ids).astype(jnp.float32)[:, None]
        convolved = convolved + same_doc * padded_rows[start_row:start_row + TOKENS] * tap_weights[offset]
    conv_out = convolved.astype(jnp.bfloat16)
    head_rows = conv_out.astype(jnp.float32).reshape(TOKENS, W // HEAD, HEAD)
    recur_gate = jax.nn.sigmoid(jnp.einsum('thd,hde->the', head_rows, gate_map.astype(jnp.float32)).reshape(TOKENS, W))
    input_gate = jax.nn.sigmoid(jnp.einsum('thd,hde->the', head_rows, input_map.astype(jnp.float32)).reshape(TOKENS, W))
    log_decay = gate_power * -jax.nn.softplus(-decay_level) * recur_gate + decay_extra
    continues = (padded_ids[reach_rows - 1:reach_rows - 1 + TOKENS] == doc_ids).astype(jnp.float32)[:, None]
    factor = jnp.exp(log_decay) * continues
    driven = jnp.sqrt(-jnp.expm1(2.0 * log_decay)) * input_gate * conv_out.astype(jnp.float32)
    products, states = lax.associative_scan(combine, (factor, driven), axis=0)
    branch = (states * jax.nn.gelu(gate_branch.astype(jnp.float32))).astype(jnp.bfloat16)
    mixed_out = jnp.dot(branch, out_weight, preferred_element_type=jnp.float32).astype(jnp.bfloat16)
    mixed_f = mixed_out.astype(jnp.float32)
    stream = (residual.astype(jnp.float32) + mixed_f * inverse_rms(mixed_f, D) * mix_gain).astype(jnp.bfloat16)
    stream_f = stream.astype(jnp.float32)
    normed = (stream_f * inverse_rms(stream_f, D) * pre_gain).astype(jnp.bfloat16)
    gate_act = jnp.dot(normed, gate_weight, preferred_element_type=jnp.float32)
    up_act = jnp.dot(normed, up_weight, preferred_element_type=jnp.float32)
    hidden = (jax.nn.silu(gate_act) * up_act).astype(jnp.bfloat16)
    span_cols = FF // N_TP
    ffn_sum = jnp.zeros((TOKENS, D), jnp.float32)
    for member in range(N_TP):
        partial_value = jnp.dot(hidden[:, member * span_cols:(member + 1) * span_cols], down_weight[member * span_cols:(member + 1) * span_cols], preferred_element_type=jnp.float32)
        ffn_sum = ffn_sum + lax.optimization_barrier(partial_value.astype(jnp.bfloat16)).astype(jnp.float32)
    ffn_out = ffn_sum.astype(jnp.bfloat16)
    ffn_f = ffn_out.astype(jnp.float32)
    return (stream_f + ffn_f * inverse_rms(ffn_f, D) * ffn_gain).astype(jnp.bfloat16)
```

```python
import functools
import math

import jax
import jax.numpy as jnp
from jax import lax
from jax.experimental import pallas as pl
from jax.experimental.pallas import tpu as pltpu
from jax.sharding import PartitionSpec as P

EPS = 1e-06
GATE_POWER = 8.0
F32 = jnp.float32
BF16 = jnp.bfloat16
MESH = pl.DeviceIdType.MESH


def grid_of(n):
    ny = 1
    for c in range(1, n + 1):
        if n % c == 0 and c * c <= n:
            ny = c
    return n // ny, ny


def ring_pos(s, nz, ny):
    z, y = lax.div(s, ny), lax.rem(s, ny)
    off = lax.div(y + ny - 1, ny)
    r = nz - 1 - z
    odd = lax.rem(r, 2)
    within = (1 - odd) * (y - 1) + odd * (ny - 1 - y)
    return (1 - off) * z + off * (nz + r * (ny - 1) + within)


def ring_dev(p, nz, ny):
    off = lax.div(lax.div(p, nz) + ny - 1, ny)
    q = off * (p - nz)
    r = lax.div(q, ny - 1)
    w = lax.rem(q, ny - 1)
    odd = lax.rem(r, 2)
    y = (1 - odd) * (1 + w) + odd * (ny - 1 - w)
    return (1 - off) * (p * ny) + off * ((nz - 1 - r) * ny + y)


def one_minus_exp(u):
    series = 1.0 + u * (1 / 8)
    for k in (7, 6, 5, 4, 3, 2):
        series = 1.0 + u * (1.0 / k) * series
    return jnp.where(u > -0.35, -u * series, 1.0 - jnp.exp(u))


def kernel(
    cfg,
    gate_branch, recur, ids, taps, gmap, imap, rate, extra, out_w, residual,
    mix_gain, pre_gain, ffn_gain, gate_w, up_w, down_w,
    out,
    gate_all, up_all, down_all, xpad, idpad, halo, ihalo, bd, fac, drv, ends, bfull,
    mixed, normed, hidden, partial, shared, recvd, own, ssq,
    wsend, wrecv, lsem, hsend, hrecv, esend, erecv, bsend, brecv, nsend, nrecv, qsend, qrecv, psend, precv, msem,
):
    n, ntp, nz, ny, width = cfg
    s, t = lax.axis_index("sp"), lax.axis_index("tp")
    tok, loc = recur.shape
    dloc = residual.shape[1]
    krows = gate_w.shape[0]
    ncol = down_w.shape[1]
    ff = gate_w.shape[1]
    CH = math.gcd(tok, 64)
    BR = math.gcd(tok, 128)
    pos = ring_pos(s, nz, ny)

    barrier = pltpu.get_barrier_semaphore()
    for j in range(1, n):
        pl.semaphore_signal(barrier, inc=1, device_id=(lax.rem(s + j, n), t), device_id_type=MESH)
    for j in range(1, ntp):
        pl.semaphore_signal(barrier, inc=1, device_id=(s, lax.rem(t + j, ntp)), device_id_type=MESH)
    pl.semaphore_wait(barrier, n - 1 + ntp - 1)

    shard = (gate_w, up_w, down_w)
    whole = (gate_all, up_all, down_all)
    nxt = [ring_dev(lax.rem(pos + 1, n), nz, ny), ring_dev(lax.rem(pos + n - 1, n), nz, ny)]
    origin = [[s] + [ring_dev(lax.rem(pos + (n - k if d == 0 else k), n), nz, ny) for k in range(1, n)] for d in range(2)]

    def half(a, o, d, local=False):
        if a < 2:
            h = krows // 2
            if local:
                return shard[a].at[pl.ds(d * h, h)]
            return whole[a].at[pl.ds(pl.multiple_of(o * krows + d * h, h), h)]
        h = ff // 2
        if local:
            return shard[a].at[pl.ds(d * h, h)]
        return whole[a].at[o, pl.ds(d * h, h)]

    def ring(a, d, k):
        o = origin[d][k]
        return pltpu.make_async_remote_copy(
            src_ref=half(a, o, d, k == 0), dst_ref=half(a, o, d),
            send_sem=wsend.at[a, d, k], recv_sem=wrecv.at[a, d, k],
            device_id=(nxt[d], t), device_id_type=MESH)

    def arrived(a, d, k):
        o = origin[d][k + 1]
        pltpu.make_async_remote_copy(
            src_ref=half(a, o, d), dst_ref=half(a, o, d),
            send_sem=wsend.at[a, d, k], recv_sem=wrecv.at[a, d, k],
            device_id=(nxt[d], t), device_id_type=MESH).wait_recv()

    def serve(arrays, k):
        for a in arrays:
            for d in range(2):
                arrived(a, d, k)
                if k < n - 2:
                    ring(a, d, k + 1).start()

    for a in range(3):
        for d in range(2):
            ring(a, d, 0).start()

    def halo_copy(i):
        src, dst = ((recur.at[pl.ds(tok - 16, 16)], halo), (ids.at[pl.ds(tok - 8, 8)], ihalo))[i]
        return pltpu.make_async_remote_copy(
            src_ref=src, dst_ref=dst, send_sem=hsend.at[i], recv_sem=hrecv.at[i],
            device_id=(lax.rem(s + 1, n), t), device_id_type=MESH)

    for i in range(2):
        halo_copy(i).start()

    def local_copy(a):
        if a < 2:
            dst = whole[a].at[pl.ds(pl.multiple_of(s * krows, krows), krows)]
        else:
            dst = whole[a].at[s]
        return pltpu.make_async_copy(shard[a], dst, lsem.at[a])

    for a in range(3):
        local_copy(a).start()

    head = gmap.shape[1]
    spread = (lax.rem(lax.broadcasted_iota(jnp.int32, (head, loc), 1), head)
              == lax.broadcasted_iota(jnp.int32, (head, loc), 0)).astype(BF16)
    diag = (lax.div(lax.broadcasted_iota(jnp.int32, (loc, loc), 0), head)
            == lax.div(lax.broadcasted_iota(jnp.int32, (loc, loc), 1), head))
    for i, m in enumerate((gmap, imap)):
        tiled = jnp.dot(m[...], spread, preferred_element_type=F32)
        bd[i] = jnp.where(diag, tiled, 0.0).astype(BF16)

    for i in range(2):
        halo_copy(i).wait()
    first = s == 0
    xpad[pl.ds(0, 8)] = halo[...].astype(F32)[8:16]
    idpad[pl.ds(0, 8)] = jnp.where(first, -1, ihalo[...])

    def fill(i, _):
        r = pl.multiple_of(i * CH, CH)
        xpad[pl.ds(pl.multiple_of(r + 8, 8), CH)] = recur[pl.ds(r, CH)].astype(F32)
        idpad[pl.ds(pl.multiple_of(r + 8, 8), CH)] = ids[pl.ds(r, CH)]
        return 0

    lax.fori_loop(0, tok // CH, fill, 0)
    reps = loc // 128
    ntaps = taps.shape[0]

    def front(i, _):
        r = pl.multiple_of(i * CH, CH)
        xw = xpad[pl.ds(r, CH + 8)]
        iw = idpad[pl.ds(r, CH + 8)]
        mine = iw[8:]
        tw = taps[...]
        conv = xw[8:] * tw[0:1]
        cont = None
        for k in range(1, ntaps):
            same1 = (pltpu.roll(iw, k, axis=0)[8:] == mine).astype(F32)
            same = jnp.concatenate([same1] * reps, axis=1)
            if k == 1:
                cont = same
            conv = conv + same * pltpu.roll(xw, k, axis=0)[8:] * tw[k:k + 1]
        cb = conv.astype(BF16)
        rg = jax.nn.sigmoid(jnp.dot(cb, bd[0], preferred_element_type=F32))
        ig = jax.nn.sigmoid(jnp.dot(cb, bd[1], preferred_element_type=F32))
        ld = rate[...] * rg + extra[pl.ds(r, CH)]
        fac[pl.ds(r, CH)] = jnp.exp(ld) * cont
        drv[pl.ds(r, CH)] = jnp.sqrt(one_minus_exp(2.0 * ld)) * ig * cb.astype(F32)
        return 0

    lax.fori_loop(0, tok // CH, front, 0)

    rows8 = lax.broadcasted_iota(jnp.int32, (8, loc), 0)

    def scan(i, carry):
        pc, hc = carry
        r = pl.multiple_of(i * 8, 8)
        a, b = fac[pl.ds(r, 8)], drv[pl.ds(r, 8)]
        for sh in (1, 2, 4):
            keep = rows8 >= sh
            b = b + a * jnp.where(keep, pltpu.roll(b, sh, axis=0), 0.0)
            a = a * jnp.where(keep, pltpu.roll(a, sh, axis=0), 1.0)
        h = b + a * hc
        p = a * pc
        fac[pl.ds(r, 8)] = p
        drv[pl.ds(r, 8)] = h
        return (jnp.broadcast_to(p[7:8], (8, loc)), jnp.broadcast_to(h[7:8], (8, loc)))

    pend, hend = lax.fori_loop(0, tok // 8, scan, (jnp.ones((8, loc), F32), jnp.zeros((8, loc), F32)))
    ends[s] = jnp.concatenate([pend, hend], axis=0)

    def end_copy(j):
        return pltpu.make_async_remote_copy(
            src_ref=ends.at[s], dst_ref=ends.at[s], send_sem=esend.at[j - 1], recv_sem=erecv.at[j - 1],
            device_id=(lax.rem(s + j, n), t), device_id_type=MESH)

    def end_arrived(j):
        o = lax.rem(s + n - j, n)
        pltpu.make_async_remote_copy(
            src_ref=ends.at[o], dst_ref=ends.at[o], send_sem=esend.at[j - 1], recv_sem=erecv.at[j - 1],
            device_id=(lax.rem(s + j, n), t), device_id_type=MESH).wait_recv()

    for j in range(1, n):
        end_copy(j).start()
    serve((0, 1), 0)
    for j in range(1, n):
        end_arrived(j)
    carry = jnp.zeros((8, loc), F32)
    for o in range(n - 1):
        e = ends[o]
        carry = jnp.where(o < s, e[:8] * carry + e[8:], carry)
    cin = carry[0:1]

    def branch(i, _):
        r = pl.multiple_of(i * CH, CH)
        st = drv[pl.ds(r, CH)] + fac[pl.ds(r, CH)] * cin
        bfull[t, pl.ds(r, CH)] = (st * jax.nn.gelu(gate_branch[pl.ds(r, CH)].astype(F32))).astype(BF16)
        return 0

    lax.fori_loop(0, tok // CH, branch, 0)

    def tp_push(view, send, recv, j, start):
        o = t if start else lax.rem(t + ntp - j, ntp)
        return pltpu.make_async_remote_copy(
            src_ref=view(o), dst_ref=view(o), send_sem=send.at[j - 1], recv_sem=recv.at[j - 1],
            device_id=(s, lax.rem(t + j, ntp)), device_id_type=MESH)

    def bview(o):
        return bfull.at[o]

    chips = ntp // 2
    core = lax.rem(t, 2)
    mate = t + 1 - 2 * core

    def far(view, send, recv, c, start):
        o = t if start else lax.rem(t + ntp - 2 * c, ntp)
        return pltpu.make_async_remote_copy(
            src_ref=view(o), dst_ref=view(o), send_sem=send.at[c - 1], recv_sem=recv.at[c - 1],
            device_id=(s, lax.rem(t + 2 * c, ntp)), device_id_type=MESH)

    def near(view, send, recv, c, start):
        base = t if start else mate
        o = lax.rem(base + ntp - 2 * c, ntp)
        return pltpu.make_async_remote_copy(
            src_ref=view(o), dst_ref=view(o), send_sem=send.at[chips - 1 + c], recv_sem=recv.at[chips - 1 + c],
            device_id=(s, mate), device_id_type=MESH)

    def gather_start(view, send, recv):
        for c in range(1, chips):
            far(view, send, recv, c, True).start()
        near(view, send, recv, 0, True).start()

    def gather_share(view, send, recv):
        for c in range(1, chips):
            far(view, send, recv, c, False).wait_recv()
            near(view, send, recv, c, True).start()

    def gather_wait(view, send, recv):
        for c in range(chips):
            near(view, send, recv, c, False).wait_recv()

    def gather_sent(view, send, recv):
        for c in range(1, chips):
            far(view, send, recv, c, True).wait_send()
        for c in range(chips):
            near(view, send, recv, c, True).wait_send()

    gather_start(bview, bsend, brecv)
    serve((0, 1), 1)
    gather_share(bview, bsend, brecv)
    gather_wait(bview, bsend, brecv)

    def row_total(q, values):
        def write(i, _):
            r = pl.multiple_of(i * BR, BR)
            v = values(r)
            c = jnp.sum(v * v, axis=1, keepdims=True)
            ssq[q, t, :, pl.ds(r, BR)] = jnp.transpose(jnp.broadcast_to(c, (BR, 128)))[:8]
            return 0

        lax.fori_loop(0, tok // BR, write, 0)
        for j in range(1, ntp):
            tp_push(lambda o: ssq.at[q, o], qsend.at[q], qrecv.at[q], j, True).start()

    def wait_total(q):
        for j in range(1, ntp):
            tp_push(lambda o: ssq.at[q, o], qsend.at[q], qrecv.at[q], j, False).wait_recv()

    def inverse_rms(q, r):
        row = ssq[q, 0, 0:1, pl.ds(r, BR)]
        for o in range(1, ntp):
            row = row + ssq[q, o, 0:1, pl.ds(r, BR)]
        inv = lax.rsqrt(row / width + EPS)
        return jnp.transpose(jnp.broadcast_to(inv, (128, BR)))[:, 0:1]

    def project(i, _):
        r = pl.multiple_of(i * BR, BR)
        total = jnp.zeros((BR, dloc), F32)
        for o in range(ntp):
            total += jnp.dot(bfull[o, pl.ds(r, BR)], out_w[pl.ds(o * loc, loc)], preferred_element_type=F32)
        mixed[pl.ds(r, BR)] = total.astype(BF16)
        return 0

    lax.fori_loop(0, tok // BR, project, 0)
    row_total(0, lambda r: mixed[pl.ds(r, BR)].astype(F32))
    wait_total(0)

    def stream(i, _):
        r = pl.multiple_of(i * BR, BR)
        m = mixed[pl.ds(r, BR)].astype(F32)
        mixed[pl.ds(r, BR)] = (residual[pl.ds(r, BR)].astype(F32) + m * inverse_rms(0, r) * mix_gain[...]).astype(BF16)
        return 0

    lax.fori_loop(0, tok // BR, stream, 0)
    row_total(1, lambda r: mixed[pl.ds(r, BR)].astype(F32))
    serve((0, 1), 2)
    wait_total(1)

    def norm(i, _):
        r = pl.multiple_of(i * BR, BR)
        m = mixed[pl.ds(r, BR)].astype(F32)
        normed[pl.ds(r, BR), pl.ds(pl.multiple_of(t * dloc, dloc), dloc)] = (m * inverse_rms(1, r) * pre_gain[...]).astype(BF16)
        return 0

    lax.fori_loop(0, tok // BR, norm, 0)

    def nview(o):
        return normed.at[:, pl.ds(pl.multiple_of(o * dloc, dloc), dloc)]

    gather_start(nview, nsend, nrecv)
    serve((0, 1), 3)
    gather_share(nview, nsend, nrecv)
    for k in range(4, n - 2):
        serve((0, 1), k)
    serve((2,), 0)
    serve((0, 1), n - 2)
    gather_wait(nview, nsend, nrecv)
    for a in range(3):
        local_copy(a).wait()

    def ffn_tile(c, size):
        cols = pl.ds(c, size)
        g = jnp.dot(normed[...], gate_all[:, cols], preferred_element_type=F32)
        u = jnp.dot(normed[...], up_all[:, cols], preferred_element_type=F32)
        hidden[:, cols] = (jax.nn.silu(g) * u).astype(BF16)

    TN = 256
    tiles = ff // TN

    def ffn_step(j, _):
        ffn_tile(pl.multiple_of(j * TN, TN), TN)
        return 0

    cut = (tiles + 1) // 2
    lax.fori_loop(0, cut, ffn_step, 0)
    serve((2,), 1)
    lax.fori_loop(cut, tiles, ffn_step, 0)
    if ff % TN:
        ffn_tile(tiles * TN, ff % TN)

    per = dloc // ncol

    def place(o):
        c = lax.div(o, per)
        w = lax.rem(o, per)
        gap = lax.rem(lax.div(c, 2) - lax.div(t, 2) + chips, chips)
        return lax.rem(c, 2), w, c, gap

    def mate_copy(i):
        return pltpu.make_async_remote_copy(
            src_ref=partial.at[i], dst_ref=shared.at[i], send_sem=psend.at[i], recv_sem=msem.at[i],
            device_id=(s, mate), device_id_type=MESH)

    def far_copy(i, w, c, gap):
        g = lax.rem(gap + chips - 1, chips)
        return pltpu.make_async_remote_copy(
            src_ref=partial.at[i], dst_ref=recvd.at[g, w], send_sem=psend.at[i], recv_sem=precv.at[g, w],
            device_id=(s, c), device_id_type=MESH)

    sent = []

    def down(*blocks):
        for o in blocks:
            i = len(sent)
            sent.append(o)
            partial[i] = jnp.dot(hidden[...], down_all[o], preferred_element_type=F32).astype(BF16)
            par, w, c, gap = place(o)

            @pl.when(par != core)
            def _():
                mate_copy(i).start()

    def join(i):
        par, w, c, gap = place(sent[i])

        @pl.when(par == core)
        def _():
            mate_copy(i).wait_recv()

            def add(b, _):
                r = pl.multiple_of(b * BR, BR)
                total = partial[i, pl.ds(r, BR)].astype(F32) + shared[i, pl.ds(r, BR)].astype(F32)
                partial[i, pl.ds(r, BR)] = total.astype(BF16)
                return 0

            lax.fori_loop(0, tok // BR, add, 0)

            @pl.when(gap == 0)
            def _():
                own[w] = partial[i]

            @pl.when(gap != 0)
            def _():
                far_copy(i, w, c, gap).start()

    down(s)
    joined = 0
    for k in range(2, n - 1):
        serve((2,), k)
        have = k + 1
        if 2 * have >= n:
            if 2 * have == n:
                down(origin[0][have])
            else:
                down(origin[0][have], origin[0][n - have])
        if k == n - 2:
            upto = len(sent)
        else:
            upto = len(sent) - (1 if 2 * have == n else 2) if 2 * have >= n else len(sent)
        while joined < upto:
            join(joined)
            joined += 1

    for i, o in enumerate(sent):
        par, w, c, gap = place(o)

        @pl.when(par != core)
        def _():
            mate_copy(i).wait_send()

        @pl.when(par == core)
        def _():
            @pl.when(gap != 0)
            def _():
                far_copy(i, w, c, gap).wait_send()

    for g in range(1, chips):
        for w in range(per):
            pltpu.make_async_remote_copy(
                src_ref=partial.at[0], dst_ref=recvd.at[g - 1, w],
                send_sem=psend.at[0], recv_sem=precv.at[g - 1, w],
                device_id=(s, mate), device_id_type=MESH).wait_recv()

    def gather_sum(i, _):
        r = pl.multiple_of(i * BR, BR)
        for w in range(per):
            total = own[w, pl.ds(r, BR)].astype(F32)
            for j in range(chips - 1):
                total = total + recvd[j, w, pl.ds(r, BR)].astype(F32)
            out[pl.ds(r, BR), pl.ds(w * ncol, ncol)] = total.astype(BF16)
        return 0

    lax.fori_loop(0, tok // BR, gather_sum, 0)
    row_total(2, lambda r: out[pl.ds(r, BR)].astype(F32))
    wait_total(2)

    def finish(i, _):
        r = pl.multiple_of(i * BR, BR)
        f = out[pl.ds(r, BR)].astype(F32)
        out[pl.ds(r, BR)] = (mixed[pl.ds(r, BR)].astype(F32) + f * inverse_rms(2, r) * ffn_gain[...]).astype(BF16)
        return 0

    lax.fori_loop(0, tok // BR, finish, 0)

    for a in range(3):
        for d in range(2):
            for k in range(n - 1):
                ring(a, d, k).wait_send()
    for j in range(1, n):
        end_copy(j).wait_send()
    gather_sent(bview, bsend, brecv)
    gather_sent(nview, nsend, nrecv)
    for j in range(1, ntp):
        for q in range(3):
            tp_push(lambda o: ssq.at[q, o], qsend.at[q], qrecv.at[q], j, True).wait_send()


def plane_kernel(
    cfg,
    gate_branch, recur, ids, taps, gmap, imap, rate, extra, out_w, residual,
    mix_gain, pre_gain, ffn_gain, gate_w, up_w, down_w,
    out,
    gate_all, up_all, down_all, xpad, idpad, halo, ihalo, bd, fac, drv, ends, bfull,
    mixed, nloc, normed, hidden, partial, recvd, ssq,
    lsem, ssend, srecv, zsend, zrecv, msend, mrecv,
    hsend, hrecv, esend, erecv, bsend, brecv, nsend, nrecv, qsend, qrecv, psend, precv,
):
    n, ntp, nz, ny, width = cfg
    s, t = lax.axis_index("sp"), lax.axis_index("tp")
    tok, loc = recur.shape
    dloc = residual.shape[1]
    krows = gate_w.shape[0]
    ncol = down_w.shape[1]
    ff = gate_w.shape[1]
    CH = math.gcd(tok, 64)
    BR = math.gcd(tok, 128)
    chips = ntp // 2
    z, y = lax.div(s, ny), lax.rem(s, ny)
    x, core = lax.div(t, 2), lax.rem(t, 2)
    mate = t + 1 - 2 * core
    per = dloc // ncol

    barrier = pltpu.get_barrier_semaphore()
    peers = [(z * ny + lax.rem(y + dy, ny), lax.rem(t + dt, ntp)) for dy in range(ny) for dt in range(ntp)][1:]
    peers += [(lax.rem(z + dz, nz) * ny + lax.rem(y + dy, ny), t) for dz in range(1, nz) for dy in range(ny)]
    for p in peers:
        pl.semaphore_signal(barrier, inc=1, device_id=p, device_id_type=MESH)
    pl.semaphore_wait(barrier, len(peers))

    shard = (gate_w, up_w, down_w)
    whole = (gate_all, up_all, down_all)
    low = (2 * z < nz).astype(jnp.int32)
    near_first = []
    for k in range(1, nz):
        near_first += [z + (2 * low - 1) * k, z - (2 * low - 1) * k]
    origin = [z]
    seen = 0
    ranks = []
    for q in near_first:
        ok = jnp.logical_and(q >= 0, q < nz).astype(jnp.int32)
        seen = seen + ok
        ranks.append((q, ok, seen))
    for j in range(1, nz):
        origin.append(sum(jnp.where(jnp.logical_and(ok == 1, r == j), q, 0) for q, ok, r in ranks))

    def block(a, o, b):
        i = o * ny + b
        if a < 2:
            return whole[a].at[pl.ds(pl.multiple_of(i * krows, krows), krows)]
        return whole[a].at[i]

    def seed_local(a):
        return pltpu.make_async_copy(shard[a], block(a, z, y), lsem.at[a])

    def seed_swap(a):
        return pltpu.make_async_remote_copy(
            src_ref=shard[a], dst_ref=block(a, z, y), send_sem=ssend.at[a], recv_sem=srecv.at[a],
            device_id=(z * ny + 1 - y, mate), device_id_type=MESH)

    def z_copy(a, o, up):
        b = block(a, o, core)
        return pltpu.make_async_remote_copy(
            src_ref=b, dst_ref=b, send_sem=zsend.at[up, a, o], recv_sem=zrecv.at[a, o],
            device_id=((z + 2 * up - 1) * ny + y, t), device_id_type=MESH)

    def mate_copy(a, o, theirs=False):
        b = block(a, o, 1 - core if theirs else core)
        return pltpu.make_async_remote_copy(
            src_ref=b, dst_ref=b, send_sem=msend.at[a, o], recv_sem=mrecv.at[a, o],
            device_id=(s, mate), device_id_type=MESH)

    def fan_down(a, o, act):
        @pl.when(jnp.logical_and(o >= z, z > 0))
        def _():
            act(z_copy(a, o, 0))

    def fan_up(a, o, act):
        @pl.when(jnp.logical_and(o <= z, z < nz - 1))
        def _():
            act(z_copy(a, o, 1))

    def fan(a, o, act):
        fan_down(a, o, act)
        fan_up(a, o, act)
        act(mate_copy(a, o))

    def start(c):
        c.start()

    def push_seed(a):
        @pl.when(y == core)
        def _():
            seed_local(a).wait()

        @pl.when(y != core)
        def _():
            pltpu.make_async_remote_copy(
                src_ref=block(a, z, core), dst_ref=block(a, z, core), send_sem=ssend.at[a], recv_sem=srecv.at[a],
                device_id=(z * ny + 1 - y, mate), device_id_type=MESH).wait_recv()

        fan(a, z, start)

    def relay(a, j):
        o = origin[j]
        z_copy(a, o, 0).wait_recv()
        fan(a, o, start)

    for a in range(3):
        @pl.when(y == core)
        def _():
            seed_local(a).start()

        @pl.when(y != core)
        def _():
            seed_swap(a).start()

    def halo_copy(i):
        src, dst = ((recur.at[pl.ds(tok - 16, 16)], halo), (ids.at[pl.ds(tok - 8, 8)], ihalo))[i]
        return pltpu.make_async_remote_copy(
            src_ref=src, dst_ref=dst, send_sem=hsend.at[i], recv_sem=hrecv.at[i],
            device_id=(lax.rem(s + 1, n), t), device_id_type=MESH)

    for i in range(2):
        halo_copy(i).start()

    @pl.when(y == core)
    def _():
        push_seed(0)
        push_seed(1)

    head = gmap.shape[1]
    spread = (lax.rem(lax.broadcasted_iota(jnp.int32, (head, loc), 1), head)
              == lax.broadcasted_iota(jnp.int32, (head, loc), 0)).astype(BF16)
    diag = (lax.div(lax.broadcasted_iota(jnp.int32, (loc, loc), 0), head)
            == lax.div(lax.broadcasted_iota(jnp.int32, (loc, loc), 1), head))
    for i, m in enumerate((gmap, imap)):
        tiled = jnp.dot(m[...], spread, preferred_element_type=F32)
        bd[i] = jnp.where(diag, tiled, 0.0).astype(BF16)

    for i in range(2):
        halo_copy(i).wait()
    first = s == 0
    xpad[pl.ds(0, 8)] = halo[...].astype(F32)[8:16]
    idpad[pl.ds(0, 8)] = jnp.where(first, -1, ihalo[...])

    def fill(i, _):
        r = pl.multiple_of(i * CH, CH)
        xpad[pl.ds(pl.multiple_of(r + 8, 8), CH)] = recur[pl.ds(r, CH)].astype(F32)
        idpad[pl.ds(pl.multiple_of(r + 8, 8), CH)] = ids[pl.ds(r, CH)]
        return 0

    lax.fori_loop(0, tok // CH, fill, 0)

    @pl.when(y != core)
    def _():
        push_seed(0)

    reps = loc // 128
    ntaps = taps.shape[0]

    def front(i, _):
        r = pl.multiple_of(i * CH, CH)
        xw = xpad[pl.ds(r, CH + 8)]
        iw = idpad[pl.ds(r, CH + 8)]
        mine = iw[8:]
        tw = taps[...]
        conv = xw[8:] * tw[0:1]
        cont = None
        for k in range(1, ntaps):
            same1 = (pltpu.roll(iw, k, axis=0)[8:] == mine).astype(F32)
            same = jnp.concatenate([same1] * reps, axis=1)
            if k == 1:
                cont = same
            conv = conv + same * pltpu.roll(xw, k, axis=0)[8:] * tw[k:k + 1]
        cb = conv.astype(BF16)
        rg = jax.nn.sigmoid(jnp.dot(cb, bd[0], preferred_element_type=F32))
        ig = jax.nn.sigmoid(jnp.dot(cb, bd[1], preferred_element_type=F32))
        ld = rate[...] * rg + extra[pl.ds(r, CH)]
        fac[pl.ds(r, CH)] = jnp.exp(ld) * cont
        drv[pl.ds(r, CH)] = jnp.sqrt(one_minus_exp(2.0 * ld)) * ig * cb.astype(F32)
        return 0

    lax.fori_loop(0, tok // CH, front, 0)

    @pl.when(y != core)
    def _():
        push_seed(1)

    rows8 = lax.broadcasted_iota(jnp.int32, (8, loc), 0)

    def scan(i, carry):
        pc, hc = carry
        r = pl.multiple_of(i * 8, 8)
        a, b = fac[pl.ds(r, 8)], drv[pl.ds(r, 8)]
        for sh in (1, 2, 4):
            keep = rows8 >= sh
            b = b + a * jnp.where(keep, pltpu.roll(b, sh, axis=0), 0.0)
            a = a * jnp.where(keep, pltpu.roll(a, sh, axis=0), 1.0)
        h = b + a * hc
        p = a * pc
        fac[pl.ds(r, 8)] = p
        drv[pl.ds(r, 8)] = h
        return (jnp.broadcast_to(p[7:8], (8, loc)), jnp.broadcast_to(h[7:8], (8, loc)))

    pend, hend = lax.fori_loop(0, tok // 8, scan, (jnp.ones((8, loc), F32), jnp.zeros((8, loc), F32)))
    ends[s] = jnp.concatenate([pend, hend], axis=0)

    def end_copy(j):
        return pltpu.make_async_remote_copy(
            src_ref=ends.at[s], dst_ref=ends.at[s], send_sem=esend.at[j - 1], recv_sem=erecv.at[j - 1],
            device_id=(lax.rem(s + j, n), t), device_id_type=MESH)

    def end_arrived(j):
        o = lax.rem(s + n - j, n)
        pltpu.make_async_remote_copy(
            src_ref=ends.at[o], dst_ref=ends.at[o], send_sem=esend.at[j - 1], recv_sem=erecv.at[j - 1],
            device_id=(lax.rem(s + j, n), t), device_id_type=MESH).wait_recv()

    for j in range(1, n):
        end_copy(j).start()
    relay(0, 1)
    for j in range(1, n):
        end_arrived(j)
    carry = jnp.zeros((8, loc), F32)
    for o in range(n - 1):
        e = ends[o]
        carry = jnp.where(o < s, e[:8] * carry + e[8:], carry)
    cin = carry[0:1]

    def branch(i, _):
        r = pl.multiple_of(i * CH, CH)
        st = drv[pl.ds(r, CH)] + fac[pl.ds(r, CH)] * cin
        bfull[t, pl.ds(r, CH)] = (st * jax.nn.gelu(gate_branch[pl.ds(r, CH)].astype(F32))).astype(BF16)
        return 0

    lax.fori_loop(0, tok // CH, branch, 0)

    def tp_push(view, send, recv, j, start):
        o = t if start else lax.rem(t + ntp - j, ntp)
        return pltpu.make_async_remote_copy(
            src_ref=view(o), dst_ref=view(o), send_sem=send.at[j - 1], recv_sem=recv.at[j - 1],
            device_id=(s, lax.rem(t + j, ntp)), device_id_type=MESH)

    def bview(o):
        return bfull.at[o]

    chips = ntp // 2
    core = lax.rem(t, 2)
    mate = t + 1 - 2 * core

    def far(view, send, recv, c, start):
        o = t if start else lax.rem(t + ntp - 2 * c, ntp)
        return pltpu.make_async_remote_copy(
            src_ref=view(o), dst_ref=view(o), send_sem=send.at[c - 1], recv_sem=recv.at[c - 1],
            device_id=(s, lax.rem(t + 2 * c, ntp)), device_id_type=MESH)

    def near(view, send, recv, c, start):
        base = t if start else mate
        o = lax.rem(base + ntp - 2 * c, ntp)
        return pltpu.make_async_remote_copy(
            src_ref=view(o), dst_ref=view(o), send_sem=send.at[chips - 1 + c], recv_sem=recv.at[chips - 1 + c],
            device_id=(s, mate), device_id_type=MESH)

    def gather_start(view, send, recv):
        for c in range(1, chips):
            far(view, send, recv, c, True).start()
        near(view, send, recv, 0, True).start()

    def gather_share(view, send, recv):
        for c in range(1, chips):
            far(view, send, recv, c, False).wait_recv()
            near(view, send, recv, c, True).start()

    def gather_wait(view, send, recv):
        for c in range(chips):
            near(view, send, recv, c, False).wait_recv()

    def gather_sent(view, send, recv):
        for c in range(1, chips):
            far(view, send, recv, c, True).wait_send()
        for c in range(chips):
            near(view, send, recv, c, True).wait_send()

    gather_start(bview, bsend, brecv)
    relay(1, 1)
    gather_share(bview, bsend, brecv)
    gather_wait(bview, bsend, brecv)

    def row_total(q, values):
        def write(i, _):
            r = pl.multiple_of(i * BR, BR)
            v = values(r)
            c = jnp.sum(v * v, axis=1, keepdims=True)
            ssq[q, t, :, pl.ds(r, BR)] = jnp.transpose(jnp.broadcast_to(c, (BR, 128)))[:8]
            return 0

        lax.fori_loop(0, tok // BR, write, 0)
        for j in range(1, ntp):
            tp_push(lambda o: ssq.at[q, o], qsend.at[q], qrecv.at[q], j, True).start()

    def wait_total(q):
        for j in range(1, ntp):
            tp_push(lambda o: ssq.at[q, o], qsend.at[q], qrecv.at[q], j, False).wait_recv()

    def inverse_rms(q, r):
        row = ssq[q, 0, 0:1, pl.ds(r, BR)]
        for o in range(1, ntp):
            row = row + ssq[q, o, 0:1, pl.ds(r, BR)]
        inv = lax.rsqrt(row / width + EPS)
        return jnp.transpose(jnp.broadcast_to(inv, (128, BR)))[:, 0:1]

    def project(i, _):
        r = pl.multiple_of(i * BR, BR)
        total = jnp.zeros((BR, dloc), F32)
        for o in range(ntp):
            total += jnp.dot(bfull[o, pl.ds(r, BR)], out_w[pl.ds(o * loc, loc)], preferred_element_type=F32)
        mixed[pl.ds(r, BR)] = total.astype(BF16)
        return 0

    lax.fori_loop(0, tok // BR, project, 0)
    row_total(0, lambda r: mixed[pl.ds(r, BR)].astype(F32))
    wait_total(0)

    def stream(i, _):
        r = pl.multiple_of(i * BR, BR)
        m = mixed[pl.ds(r, BR)].astype(F32)
        mixed[pl.ds(r, BR)] = (residual[pl.ds(r, BR)].astype(F32) + m * inverse_rms(0, r) * mix_gain[...]).astype(BF16)
        return 0

    lax.fori_loop(0, tok // BR, stream, 0)
    row_total(1, lambda r: mixed[pl.ds(r, BR)].astype(F32))
    relay(0, 2)
    wait_total(1)

    cols = pl.ds(pl.multiple_of(t * dloc, dloc), dloc)

    def norm(i, _):
        r = pl.multiple_of(i * BR, BR)
        m = mixed[pl.ds(r, BR)].astype(F32)
        v = (m * inverse_rms(1, r) * pre_gain[...]).astype(BF16)
        nloc[pl.ds(r, BR)] = v

        @pl.when(y == core)
        def _():
            normed[pl.ds(r, BR), cols] = v

        return 0

    lax.fori_loop(0, tok // BR, norm, 0)

    def n_copy(dy, dx):
        return pltpu.make_async_remote_copy(
            src_ref=nloc, dst_ref=normed.at[:, cols], send_sem=nsend.at[dy, dx], recv_sem=nrecv.at[t],
            device_id=(z * ny + lax.rem(y + dy, ny), 2 * lax.rem(x + dx, chips) + y), device_id_type=MESH)

    def to_plane(act):
        for dy in range(ny):
            for dx in range(chips):
                if dy or dx:
                    act(n_copy(dy, dx))
                else:
                    @pl.when(y != core)
                    def _():
                        act(n_copy(0, 0))

    def n_wait(dt):
        o = lax.rem(t + dt, ntp)
        view = normed.at[:, pl.ds(pl.multiple_of(o * dloc, dloc), dloc)]
        pltpu.make_async_remote_copy(
            src_ref=view, dst_ref=view, send_sem=nsend.at[0, 0], recv_sem=nrecv.at[o],
            device_id=(s, mate), device_id_type=MESH).wait_recv()

    to_plane(start)
    relay(1, 2)
    ends_line = jnp.logical_or(z == 0, z == nz - 1)

    @pl.when(ends_line)
    def _():
        push_seed(2)

    for j in range(3, nz):
        relay(0, j)
        relay(1, j)

    @pl.when(jnp.logical_not(ends_line))
    def _():
        push_seed(2)

    for dt in range(1, ntp):
        n_wait(dt)

    @pl.when(y != core)
    def _():
        n_wait(0)

    for a in range(2):
        for o in range(nz):
            mate_copy(a, o, True).wait_recv()

    def ffn_tile(c, size):
        cs = pl.ds(c, size)
        g = jnp.dot(normed[...], gate_all[:, cs], preferred_element_type=F32)
        u = jnp.dot(normed[...], up_all[:, cs], preferred_element_type=F32)
        hidden[:, cs] = (jax.nn.silu(g) * u).astype(BF16)

    TN = 256
    tiles = ff // TN

    def ffn_step(j, _):
        ffn_tile(pl.multiple_of(j * TN, TN), TN)
        return 0

    lax.fori_loop(0, tiles, ffn_step, 0)
    if ff % TN:
        ffn_tile(tiles * TN, ff % TN)

    me = y * chips + x

    def p_copy(i):
        return pltpu.make_async_remote_copy(
            src_ref=partial.at[i], dst_ref=recvd.at[me, lax.rem(i, per)], send_sem=psend.at[i],
            recv_sem=precv.at[me, lax.rem(i, per)],
            device_id=(z * ny + core, lax.div(i, per)), device_id_type=MESH)

    def owned(i):
        return jnp.logical_and(y == core, lax.div(i, per) == t)

    for j in range(nz):
        o = origin[j]
        if j:
            relay(2, j)
        for b in range(ny):
            @pl.when(b != core)
            def _():
                mate_copy(2, o, True).wait_recv()

            i = o * ny + b
            partial[i] = jnp.dot(hidden[...], down_all[i], preferred_element_type=F32).astype(BF16)

            @pl.when(owned(i))
            def _():
                recvd[me, lax.rem(i, per)] = partial[i]

            @pl.when(jnp.logical_not(owned(i)))
            def _():
                p_copy(i).start()

    def p_wait(dy, dx):
        k = lax.rem(y + dy, ny) * chips + lax.rem(x + dx, chips)
        for w in range(per):
            pltpu.make_async_remote_copy(
                src_ref=partial.at[0], dst_ref=recvd.at[k, w], send_sem=psend.at[0], recv_sem=precv.at[k, w],
                device_id=(s, mate), device_id_type=MESH).wait_recv()

    for dy in range(ny):
        for dx in range(chips):
            if dy or dx:
                p_wait(dy, dx)

    @pl.when(y != core)
    def _():
        p_wait(0, 0)

    def gather_sum(i, _):
        r = pl.multiple_of(i * BR, BR)
        for w in range(per):
            total = recvd[0, w, pl.ds(r, BR)].astype(F32)
            for k in range(1, ny * chips):
                total = total + recvd[k, w, pl.ds(r, BR)].astype(F32)
            out[pl.ds(r, BR), pl.ds(w * ncol, ncol)] = total.astype(BF16)
        return 0

    lax.fori_loop(0, tok // BR, gather_sum, 0)
    row_total(2, lambda r: out[pl.ds(r, BR)].astype(F32))
    wait_total(2)

    def finish(i, _):
        r = pl.multiple_of(i * BR, BR)
        f = out[pl.ds(r, BR)].astype(F32)
        out[pl.ds(r, BR)] = (mixed[pl.ds(r, BR)].astype(F32) + f * inverse_rms(2, r) * ffn_gain[...]).astype(BF16)
        return 0

    lax.fori_loop(0, tok // BR, finish, 0)

    def sent(c):
        c.wait_send()

    for a in range(3):
        @pl.when(y != core)
        def _():
            seed_swap(a).wait_send()

        for j in range(nz):
            fan(a, origin[j], sent)
    for j in range(1, n):
        end_copy(j).wait_send()
    gather_sent(bview, bsend, brecv)
    to_plane(sent)
    for i in range(n):
        @pl.when(jnp.logical_not(owned(i)))
        def _():
            p_copy(i).wait_send()
    for j in range(1, ntp):
        for q in range(3):
            tp_push(lambda o: ssq.at[q, o], qsend.at[q], qrecv.at[q], j, True).wait_send()


def body(n, ntp, gate_branch, recur_input, doc_ids, conv_taps, gate_map, input_map, decay_level, decay_extra,
         out_weight, residual, mix_gain, pre_gain, ffn_gain, gate_weight, up_weight, down_weight):
    tok, loc = recur_input.shape
    dloc = residual.shape[1]
    krows, ff = gate_weight.shape
    ncol = down_weight.shape[1]
    heads, head, _ = gate_map.shape
    nz, ny = grid_of(n)
    ids = jnp.broadcast_to(doc_ids[:, None], (tok, 128))
    rate = (GATE_POWER * -jax.nn.softplus(-decay_level))[None, :]
    args = (gate_branch, recur_input, ids, conv_taps.astype(F32), gate_map.reshape(heads * head, head),
            input_map.reshape(heads * head, head), rate, decay_extra, out_weight, residual,
            mix_gain[None, :], pre_gain[None, :], ffn_gain[None, :], gate_weight, up_weight, down_weight)
    vm = pl.BlockSpec(memory_space=pltpu.VMEM)
    hbm = pl.BlockSpec(memory_space=pl.ANY)
    V, S = pltpu.VMEM, pltpu.SemaphoreType.DMA
    per = dloc // ncol
    chips = ntp // 2
    if ny == 2:
        fn = plane_kernel
        scratch = [
            V((n * krows, ff), BF16), V((n * krows, ff), BF16), V((n, ff, ncol), BF16),
            V((tok + 8, loc), F32), V((tok + 8, 128), jnp.int32), V((16, loc), BF16), V((8, 128), jnp.int32),
            V((2, loc, loc), BF16), V((tok, loc), F32), V((tok, loc), F32), V((n, 16, loc), F32),
            V((ntp, tok, loc), BF16), V((tok, dloc), BF16), V((tok, dloc), BF16), V((tok, dloc * ntp), BF16),
            V((tok, ff), BF16), V((n, tok, ncol), BF16), V((ny * chips, per, tok, ncol), BF16), V((3, ntp, 8, tok), F32),
            S((3,)), S((3,)), S((3,)), S((2, 3, nz)), S((3, nz)), S((3, nz)), S((3, nz)),
            S((2,)), S((2,)), S((n - 1,)), S((n - 1,)), S((ntp - 1,)), S((ntp - 1,)),
            S((ny, chips)), S((ntp,)), S((3, ntp - 1)), S((3, ntp - 1)), S((n,)), S((ny * chips, per)),
        ]
    else:
        fn = kernel
        scratch = [
            V((n * krows, ff), BF16), V((n * krows, ff), BF16), V((n, ff, ncol), BF16),
            V((tok + 8, loc), F32), V((tok + 8, 128), jnp.int32), V((16, loc), BF16), V((8, 128), jnp.int32),
            V((2, loc, loc), BF16), V((tok, loc), F32), V((tok, loc), F32), V((n, 16, loc), F32),
            V((ntp, tok, loc), BF16), V((tok, dloc), BF16), V((tok, dloc * ntp), BF16), V((tok, ff), BF16),
            V((n, tok, ncol), BF16), V((n, tok, ncol), BF16), V((chips - 1, per, tok, ncol), BF16), V((per, tok, ncol), BF16),
            V((3, ntp, 8, tok), F32),
            S((3, 2, n - 1)), S((3, 2, n - 1)), S((3,)), S((2,)), S((2,)), S((n - 1,)), S((n - 1,)),
            S((ntp - 1,)), S((ntp - 1,)), S((ntp - 1,)), S((ntp - 1,)), S((3, ntp - 1)), S((3, ntp - 1)),
            S((n,)), S((chips - 1, per)), S((n,)),
        ]
    return pl.pallas_call(
        functools.partial(fn, (n, ntp, nz, ny, dloc * ntp)),
        out_shape=jax.ShapeDtypeStruct((tok, dloc), BF16),
        in_specs=[vm] * 13 + [hbm] * 3,
        out_specs=vm,
        scratch_shapes=scratch,
        compiler_params=pltpu.CompilerParams(
            collective_id=0, has_side_effects=True, vmem_limit_bytes=62 * 1024 * 1024),
    )(*args)


def solution(mesh):
    in_specs = (
        P("sp", "tp"), P("sp", "tp"), P("sp"), P(None, "tp"), P("tp", None, None), P("tp", None, None),
        P("tp"), P("sp", "tp"), P(None, "tp"), P("sp", "tp"), P("tp"), P("tp"), P("tp"),
        P("sp", "tp"), P("sp", "tp"), P("tp", "sp"),
    )
    fn = functools.partial(body, mesh.shape["sp"], mesh.shape["tp"])
    return jax.shard_map(fn, mesh=mesh, in_specs=in_specs, out_specs=P("sp", "tp"), check_vma=False)
```

```python
import functools
import math

import jax
import jax.numpy as jnp
from jax import lax
from jax.experimental import pallas as pl
from jax.experimental.pallas import tpu as pltpu
from jax.sharding import PartitionSpec as P

EPS = 1e-06
GATE_POWER = 8.0
F32 = jnp.float32
BF16 = jnp.bfloat16
MESH = pl.DeviceIdType.MESH


def grid_of(n):
    ny = 1
    for c in range(1, n + 1):
        if n % c == 0 and c * c <= n:
            ny = c
    return n // ny, ny


def ring_pos(s, nz, ny):
    z, y = lax.div(s, ny), lax.rem(s, ny)
    off = lax.div(y + ny - 1, ny)
    r = nz - 1 - z
    odd = lax.rem(r, 2)
    within = (1 - odd) * (y - 1) + odd * (ny - 1 - y)
    return (1 - off) * z + off * (nz + r * (ny - 1) + within)


def ring_dev(p, nz, ny):
    off = lax.div(lax.div(p, nz) + ny - 1, ny)
    q = off * (p - nz)
    r = lax.div(q, ny - 1)
    w = lax.rem(q, ny - 1)
    odd = lax.rem(r, 2)
    y = (1 - odd) * (1 + w) + odd * (ny - 1 - w)
    return (1 - off) * (p * ny) + off * ((nz - 1 - r) * ny + y)


def one_minus_exp(u):
    series = 1.0 + u * (1 / 8)
    for k in (7, 6, 5, 4, 3, 2):
        series = 1.0 + u * (1.0 / k) * series
    return jnp.where(u > -0.35, -u * series, 1.0 - jnp.exp(u))


def kernel(
    cfg,
    gate_branch, recur, ids, taps, gmap, imap, rate, extra, out_w, residual,
    mix_gain, pre_gain, ffn_gain, gate_w, up_w, down_w,
    out,
    gate_all, up_all, down_all, xpad, idpad, halo, ihalo, bd, fac, drv, ends, bfull,
    mixed, normed, hidden, partial, shared, recvd, own, ssq,
    wsend, wrecv, lsem, hsend, hrecv, esend, erecv, bsend, brecv, nsend, nrecv, qsend, qrecv, psend, precv, msem,
):
    n, ntp, nz, ny, width = cfg
    s, t = lax.axis_index("sp"), lax.axis_index("tp")
    tok, loc = recur.shape
    dloc = residual.shape[1]
    krows = gate_w.shape[0]
    ncol = down_w.shape[1]
    ff = gate_w.shape[1]
    CH = math.gcd(tok, 64)
    BR = math.gcd(tok, 128)
    pos = ring_pos(s, nz, ny)

    barrier = pltpu.get_barrier_semaphore()
    for j in range(1, n):
        pl.semaphore_signal(barrier, inc=1, device_id=(lax.rem(s + j, n), t), device_id_type=MESH)
    for j in range(1, ntp):
        pl.semaphore_signal(barrier, inc=1, device_id=(s, lax.rem(t + j, ntp)), device_id_type=MESH)
    pl.semaphore_wait(barrier, n - 1 + ntp - 1)

    shard = (gate_w, up_w, down_w)
    whole = (gate_all, up_all, down_all)
    nxt = [ring_dev(lax.rem(pos + 1, n), nz, ny), ring_dev(lax.rem(pos + n - 1, n), nz, ny)]
    origin = [[s] + [ring_dev(lax.rem(pos + (n - k if d == 0 else k), n), nz, ny) for k in range(1, n)] for d in range(2)]

    def half(a, o, d, local=False):
        if a < 2:
            h = krows // 2
            if local:
                return shard[a].at[pl.ds(d * h, h)]
            return whole[a].at[pl.ds(pl.multiple_of(o * krows + d * h, h), h)]
        h = ff // 2
        if local:
            return shard[a].at[pl.ds(d * h, h)]
        return whole[a].at[o, pl.ds(d * h, h)]

    def ring(a, d, k):
        o = origin[d][k]
        return pltpu.make_async_remote_copy(
            src_ref=half(a, o, d, k == 0), dst_ref=half(a, o, d),
            send_sem=wsend.at[a, d, k], recv_sem=wrecv.at[a, d, k],
            device_id=(nxt[d], t), device_id_type=MESH)

    def arrived(a, d, k):
        o = origin[d][k + 1]
        pltpu.make_async_remote_copy(
            src_ref=half(a, o, d), dst_ref=half(a, o, d),
            send_sem=wsend.at[a, d, k], recv_sem=wrecv.at[a, d, k],
            device_id=(nxt[d], t), device_id_type=MESH).wait_recv()

    def serve(arrays, k):
        for a in arrays:
            for d in range(2):
                arrived(a, d, k)
                if k < n - 2:
                    ring(a, d, k + 1).start()

    for a in range(3):
        for d in range(2):
            ring(a, d, 0).start()

    def halo_copy(i):
        src, dst = ((recur.at[pl.ds(tok - 16, 16)], halo), (ids.at[pl.ds(tok - 8, 8)], ihalo))[i]
        return pltpu.make_async_remote_copy(
            src_ref=src, dst_ref=dst, send_sem=hsend.at[i], recv_sem=hrecv.at[i],
            device_id=(lax.rem(s + 1, n), t), device_id_type=MESH)

    for i in range(2):
        halo_copy(i).start()

    def local_copy(a):
        if a < 2:
            dst = whole[a].at[pl.ds(pl.multiple_of(s * krows, krows), krows)]
        else:
            dst = whole[a].at[s]
        return pltpu.make_async_copy(shard[a], dst, lsem.at[a])

    for a in range(3):
        local_copy(a).start()

    head = gmap.shape[1]
    spread = (lax.rem(lax.broadcasted_iota(jnp.int32, (head, loc), 1), head)
              == lax.broadcasted_iota(jnp.int32, (head, loc), 0)).astype(BF16)
    diag = (lax.div(lax.broadcasted_iota(jnp.int32, (loc, loc), 0), head)
            == lax.div(lax.broadcasted_iota(jnp.int32, (loc, loc), 1), head))
    for i, m in enumerate((gmap, imap)):
        tiled = jnp.dot(m[...], spread, preferred_element_type=F32)
        bd[i] = jnp.where(diag, tiled, 0.0).astype(BF16)

    for i in range(2):
        halo_copy(i).wait()
    first = s == 0
    xpad[pl.ds(0, 8)] = halo[...].astype(F32)[8:16]
    idpad[pl.ds(0, 8)] = jnp.where(first, -1, ihalo[...])

    def fill(i, _):
        r = pl.multiple_of(i * CH, CH)
        xpad[pl.ds(pl.multiple_of(r + 8, 8), CH)] = recur[pl.ds(r, CH)].astype(F32)
        idpad[pl.ds(pl.multiple_of(r + 8, 8), CH)] = ids[pl.ds(r, CH)]
        return 0

    lax.fori_loop(0, tok // CH, fill, 0)
    reps = loc // 128
    ntaps = taps.shape[0]

    def front(i, _):
        r = pl.multiple_of(i * CH, CH)
        xw = xpad[pl.ds(r, CH + 8)]
        iw = idpad[pl.ds(r, CH + 8)]
        mine = iw[8:]
        tw = taps[...]
        conv = xw[8:] * tw[0:1]
        cont = None
        for k in range(1, ntaps):
            same1 = (pltpu.roll(iw, k, axis=0)[8:] == mine).astype(F32)
            same = jnp.concatenate([same1] * reps, axis=1)
            if k == 1:
                cont = same
            conv = conv + same * pltpu.roll(xw, k, axis=0)[8:] * tw[k:k + 1]
        cb = conv.astype(BF16)
        rg = jax.nn.sigmoid(jnp.dot(cb, bd[0], preferred_element_type=F32))
        ig = jax.nn.sigmoid(jnp.dot(cb, bd[1], preferred_element_type=F32))
        ld = rate[...] * rg + extra[pl.ds(r, CH)]
        fac[pl.ds(r, CH)] = jnp.exp(ld) * cont
        drv[pl.ds(r, CH)] = jnp.sqrt(one_minus_exp(2.0 * ld)) * ig * cb.astype(F32)
        return 0

    lax.fori_loop(0, tok // CH, front, 0)

    rows8 = lax.broadcasted_iota(jnp.int32, (8, loc), 0)

    def scan(i, carry):
        pc, hc = carry
        r = pl.multiple_of(i * 8, 8)
        a, b = fac[pl.ds(r, 8)], drv[pl.ds(r, 8)]
        for sh in (1, 2, 4):
            keep = rows8 >= sh
            b = b + a * jnp.where(keep, pltpu.roll(b, sh, axis=0), 0.0)
            a = a * jnp.where(keep, pltpu.roll(a, sh, axis=0), 1.0)
        h = b + a * hc
        p = a * pc
        fac[pl.ds(r, 8)] = p
        drv[pl.ds(r, 8)] = h
        return (jnp.broadcast_to(p[7:8], (8, loc)), jnp.broadcast_to(h[7:8], (8, loc)))

    pend, hend = lax.fori_loop(0, tok // 8, scan, (jnp.ones((8, loc), F32), jnp.zeros((8, loc), F32)))
    ends[s] = jnp.concatenate([pend, hend], axis=0)

    def end_copy(j):
        return pltpu.make_async_remote_copy(
            src_ref=ends.at[s], dst_ref=ends.at[s], send_sem=esend.at[j - 1], recv_sem=erecv.at[j - 1],
            device_id=(lax.rem(s + j, n), t), device_id_type=MESH)

    def end_arrived(j):
        o = lax.rem(s + n - j, n)
        pltpu.make_async_remote_copy(
            src_ref=ends.at[o], dst_ref=ends.at[o], send_sem=esend.at[j - 1], recv_sem=erecv.at[j - 1],
            device_id=(lax.rem(s + j, n), t), device_id_type=MESH).wait_recv()

    for j in range(1, n):
        end_copy(j).start()
    serve((0, 1), 0)
    for j in range(1, n):
        end_arrived(j)
    carry = jnp.zeros((8, loc), F32)
    for o in range(n - 1):
        e = ends[o]
        carry = jnp.where(o < s, e[:8] * carry + e[8:], carry)
    cin = carry[0:1]

    def branch(i, _):
        r = pl.multiple_of(i * CH, CH)
        st = drv[pl.ds(r, CH)] + fac[pl.ds(r, CH)] * cin
        bfull[t, pl.ds(r, CH)] = (st * jax.nn.gelu(gate_branch[pl.ds(r, CH)].astype(F32))).astype(BF16)
        return 0

    lax.fori_loop(0, tok // CH, branch, 0)

    def tp_push(view, send, recv, j, start):
        o = t if start else lax.rem(t + ntp - j, ntp)
        return pltpu.make_async_remote_copy(
            src_ref=view(o), dst_ref=view(o), send_sem=send.at[j - 1], recv_sem=recv.at[j - 1],
            device_id=(s, lax.rem(t + j, ntp)), device_id_type=MESH)

    def bview(o):
        return bfull.at[o]

    chips = ntp // 2
    core = lax.rem(t, 2)
    mate = t + 1 - 2 * core

    def far(view, send, recv, c, start):
        o = t if start else lax.rem(t + ntp - 2 * c, ntp)
        return pltpu.make_async_remote_copy(
            src_ref=view(o), dst_ref=view(o), send_sem=send.at[c - 1], recv_sem=recv.at[c - 1],
            device_id=(s, lax.rem(t + 2 * c, ntp)), device_id_type=MESH)

    def near(view, send, recv, c, start):
        base = t if start else mate
        o = lax.rem(base + ntp - 2 * c, ntp)
        return pltpu.make_async_remote_copy(
            src_ref=view(o), dst_ref=view(o), send_sem=send.at[chips - 1 + c], recv_sem=recv.at[chips - 1 + c],
            device_id=(s, mate), device_id_type=MESH)

    def gather_start(view, send, recv):
        for c in range(1, chips):
            far(view, send, recv, c, True).start()
        near(view, send, recv, 0, True).start()

    def gather_share(view, send, recv):
        for c in range(1, chips):
            far(view, send, recv, c, False).wait_recv()
            near(view, send, recv, c, True).start()

    def gather_wait(view, send, recv):
        for c in range(chips):
            near(view, send, recv, c, False).wait_recv()

    def gather_sent(view, send, recv):
        for c in range(1, chips):
            far(view, send, recv, c, True).wait_send()
        for c in range(chips):
            near(view, send, recv, c, True).wait_send()

    gather_start(bview, bsend, brecv)
    serve((0, 1), 1)
    gather_share(bview, bsend, brecv)
    gather_wait(bview, bsend, brecv)

    def row_total(q, values):
        def write(i, _):
            r = pl.multiple_of(i * BR, BR)
            v = values(r)
            c = jnp.sum(v * v, axis=1, keepdims=True)
            ssq[q, t, :, pl.ds(r, BR)] = jnp.transpose(jnp.broadcast_to(c, (BR, 128)))[:8]
            return 0

        lax.fori_loop(0, tok // BR, write, 0)
        for j in range(1, ntp):
            tp_push(lambda o: ssq.at[q, o], qsend.at[q], qrecv.at[q], j, True).start()

    def wait_total(q):
        for j in range(1, ntp):
            tp_push(lambda o: ssq.at[q, o], qsend.at[q], qrecv.at[q], j, False).wait_recv()

    def inverse_rms(q, r):
        row = ssq[q, 0, 0:1, pl.ds(r, BR)]
        for o in range(1, ntp):
            row = row + ssq[q, o, 0:1, pl.ds(r, BR)]
        inv = lax.rsqrt(row / width + EPS)
        return jnp.transpose(jnp.broadcast_to(inv, (128, BR)))[:, 0:1]

    def project(i, _):
        r = pl.multiple_of(i * BR, BR)
        total = jnp.zeros((BR, dloc), F32)
        for o in range(ntp):
            total += jnp.dot(bfull[o, pl.ds(r, BR)], out_w[pl.ds(o * loc, loc)], preferred_element_type=F32)
        mixed[pl.ds(r, BR)] = total.astype(BF16)
        return 0

    lax.fori_loop(0, tok // BR, project, 0)
    row_total(0, lambda r: mixed[pl.ds(r, BR)].astype(F32))
    wait_total(0)

    def stream(i, _):
        r = pl.multiple_of(i * BR, BR)
        m = mixed[pl.ds(r, BR)].astype(F32)
        mixed[pl.ds(r, BR)] = (residual[pl.ds(r, BR)].astype(F32) + m * inverse_rms(0, r) * mix_gain[...]).astype(BF16)
        return 0

    lax.fori_loop(0, tok // BR, stream, 0)
    row_total(1, lambda r: mixed[pl.ds(r, BR)].astype(F32))
    serve((0, 1), 2)
    wait_total(1)

    def norm(i, _):
        r = pl.multiple_of(i * BR, BR)
        m = mixed[pl.ds(r, BR)].astype(F32)
        normed[pl.ds(r, BR), pl.ds(pl.multiple_of(t * dloc, dloc), dloc)] = (m * inverse_rms(1, r) * pre_gain[...]).astype(BF16)
        return 0

    lax.fori_loop(0, tok // BR, norm, 0)

    def nview(o):
        return normed.at[:, pl.ds(pl.multiple_of(o * dloc, dloc), dloc)]

    gather_start(nview, nsend, nrecv)
    serve((0, 1), 3)
    gather_share(nview, nsend, nrecv)
    for k in range(4, n - 2):
        serve((0, 1), k)
    serve((2,), 0)
    serve((0, 1), n - 2)
    gather_wait(nview, nsend, nrecv)
    for a in range(3):
        local_copy(a).wait()

    def ffn_tile(c, size):
        cols = pl.ds(c, size)
        g = jnp.dot(normed[...], gate_all[:, cols], preferred_element_type=F32)
        u = jnp.dot(normed[...], up_all[:, cols], preferred_element_type=F32)
        hidden[:, cols] = (jax.nn.silu(g) * u).astype(BF16)

    TN = 256
    tiles = ff // TN

    def ffn_step(j, _):
        ffn_tile(pl.multiple_of(j * TN, TN), TN)
        return 0

    cut = (tiles + 1) // 2
    lax.fori_loop(0, cut, ffn_step, 0)
    serve((2,), 1)
    lax.fori_loop(cut, tiles, ffn_step, 0)
    if ff % TN:
        ffn_tile(tiles * TN, ff % TN)

    per = dloc // ncol

    def place(o):
        c = lax.div(o, per)
        w = lax.rem(o, per)
        gap = lax.rem(lax.div(c, 2) - lax.div(t, 2) + chips, chips)
        return lax.rem(c, 2), w, c, gap

    def mate_copy(i):
        return pltpu.make_async_remote_copy(
            src_ref=partial.at[i], dst_ref=shared.at[i], send_sem=psend.at[i], recv_sem=msem.at[i],
            device_id=(s, mate), device_id_type=MESH)

    def far_copy(i, w, c, gap):
        g = lax.rem(gap + chips - 1, chips)
        return pltpu.make_async_remote_copy(
            src_ref=partial.at[i], dst_ref=recvd.at[g, w], send_sem=psend.at[i], recv_sem=precv.at[g, w],
            device_id=(s, c), device_id_type=MESH)

    sent = []

    def down(*blocks):
        for o in blocks:
            i = len(sent)
            sent.append(o)
            partial[i] = jnp.dot(hidden[...], down_all[o], preferred_element_type=F32).astype(BF16)
            par, w, c, gap = place(o)

            @pl.when(par != core)
            def _():
                mate_copy(i).start()

    def join(i):
        par, w, c, gap = place(sent[i])

        @pl.when(par == core)
        def _():
            mate_copy(i).wait_recv()

            def add(b, _):
                r = pl.multiple_of(b * BR, BR)
                total = partial[i, pl.ds(r, BR)].astype(F32) + shared[i, pl.ds(r, BR)].astype(F32)
                partial[i, pl.ds(r, BR)] = total.astype(BF16)
                return 0

            lax.fori_loop(0, tok // BR, add, 0)

            @pl.when(gap == 0)
            def _():
                own[w] = partial[i]

            @pl.when(gap != 0)
            def _():
                far_copy(i, w, c, gap).start()

    down(s)
    joined = 0
    for k in range(2, n - 1):
        serve((2,), k)
        have = k + 1
        if 2 * have >= n:
            if 2 * have == n:
                down(origin[0][have])
            else:
                down(origin[0][have], origin[0][n - have])
        if k == n - 2:
            upto = len(sent)
        else:
            upto = len(sent) - (1 if 2 * have == n else 2) if 2 * have >= n else len(sent)
        while joined < upto:
            join(joined)
            joined += 1

    for i, o in enumerate(sent):
        par, w, c, gap = place(o)

        @pl.when(par != core)
        def _():
            mate_copy(i).wait_send()

        @pl.when(par == core)
        def _():
            @pl.when(gap != 0)
            def _():
                far_copy(i, w, c, gap).wait_send()

    for g in range(1, chips):
        for w in range(per):
            pltpu.make_async_remote_copy(
                src_ref=partial.at[0], dst_ref=recvd.at[g - 1, w],
                send_sem=psend.at[0], recv_sem=precv.at[g - 1, w],
                device_id=(s, mate), device_id_type=MESH).wait_recv()

    def gather_sum(i, _):
        r = pl.multiple_of(i * BR, BR)
        for w in range(per):
            total = own[w, pl.ds(r, BR)].astype(F32)
            for j in range(chips - 1):
                total = total + recvd[j, w, pl.ds(r, BR)].astype(F32)
            out[pl.ds(r, BR), pl.ds(w * ncol, ncol)] = total.astype(BF16)
        return 0

    lax.fori_loop(0, tok // BR, gather_sum, 0)
    row_total(2, lambda r: out[pl.ds(r, BR)].astype(F32))
    wait_total(2)

    def finish(i, _):
        r = pl.multiple_of(i * BR, BR)
        f = out[pl.ds(r, BR)].astype(F32)
        out[pl.ds(r, BR)] = (mixed[pl.ds(r, BR)].astype(F32) + f * inverse_rms(2, r) * ffn_gain[...]).astype(BF16)
        return 0

    lax.fori_loop(0, tok // BR, finish, 0)

    for a in range(3):
        for d in range(2):
            for k in range(n - 1):
                ring(a, d, k).wait_send()
    for j in range(1, n):
        end_copy(j).wait_send()
    gather_sent(bview, bsend, brecv)
    gather_sent(nview, nsend, nrecv)
    for j in range(1, ntp):
        for q in range(3):
            tp_push(lambda o: ssq.at[q, o], qsend.at[q], qrecv.at[q], j, True).wait_send()


def plane_kernel(
    cfg,
    gate_branch, recur, ids, taps, gmap, imap, rate, extra, out_w, residual,
    mix_gain, pre_gain, ffn_gain, gate_w, up_w, down_w,
    out,
    gate_all, up_all, down_all, xpad, idpad, halo, ihalo, bd, fac, drv, ends, bfull,
    mixed, nloc, normed, gsum, usum, hidden, partial, recvd, ssq,
    lsem, ssend, srecv, zsend, zrecv, msend, mrecv,
    hsend, hrecv, esend, erecv, bsend, brecv, nsend, nrecv, qsend, qrecv, psend, precv,
):
    n, ntp, nz, ny, width = cfg
    s, t = lax.axis_index("sp"), lax.axis_index("tp")
    tok, loc = recur.shape
    dloc = residual.shape[1]
    krows = gate_w.shape[0]
    ncol = down_w.shape[1]
    ff = gate_w.shape[1]
    CH = math.gcd(tok, 64)
    BR = math.gcd(tok, 128)
    chips = ntp // 2
    z, y = lax.div(s, ny), lax.rem(s, ny)
    x, core = lax.div(t, 2), lax.rem(t, 2)
    mate = t + 1 - 2 * core
    per = dloc // ncol

    barrier = pltpu.get_barrier_semaphore()
    peers = [(z * ny + lax.rem(y + dy, ny), lax.rem(t + dt, ntp)) for dy in range(ny) for dt in range(ntp)][1:]
    peers += [(lax.rem(z + dz, nz) * ny + lax.rem(y + dy, ny), t) for dz in range(1, nz) for dy in range(ny)]
    for p in peers:
        pl.semaphore_signal(barrier, inc=1, device_id=p, device_id_type=MESH)
    pl.semaphore_wait(barrier, len(peers))

    low = (2 * z < nz).astype(jnp.int32)
    near_first = []
    for k in range(1, nz):
        near_first += [z + (2 * low - 1) * k, z - (2 * low - 1) * k]
    origin = [z]
    seen = 0
    ranks = []
    for q in near_first:
        ok = jnp.logical_and(q >= 0, q < nz).astype(jnp.int32)
        seen = seen + ok
        ranks.append((q, ok, seen))
    for j in range(1, nz):
        origin.append(sum(jnp.where(jnp.logical_and(ok == 1, r == j), q, 0) for q, ok, r in ranks))

    hcol = ncol // 2
    hrow = krows // 2
    GATE, UP, DOWN = (0, 1), (2,), (3, 4)

    def block(a, o, b):
        i = o * ny + b
        if a in GATE:
            return gate_all.at[pl.ds(pl.multiple_of(i * krows + a * hrow, hrow), hrow)]
        if a in UP:
            return up_all.at[pl.ds(pl.multiple_of(i * krows, krows), krows)]
        return down_all.at[i, :, pl.ds((a - DOWN[0]) * hcol, hcol)]

    def own_shard(a):
        if a in GATE:
            return gate_w.at[pl.ds(a * hrow, hrow)]
        if a in UP:
            return up_w
        return down_w.at[:, pl.ds((a - DOWN[0]) * hcol, hcol)]

    def seed_local(a):
        return pltpu.make_async_copy(own_shard(a), block(a, z, y), lsem.at[a])

    def seed_swap(a):
        return pltpu.make_async_remote_copy(
            src_ref=own_shard(a), dst_ref=block(a, z, y), send_sem=ssend.at[a], recv_sem=srecv.at[a],
            device_id=(z * ny + 1 - y, mate), device_id_type=MESH)

    def z_copy(a, o, up):
        b = block(a, o, core)
        return pltpu.make_async_remote_copy(
            src_ref=b, dst_ref=b, send_sem=zsend.at[up, a, o], recv_sem=zrecv.at[a, o],
            device_id=((z + 2 * up - 1) * ny + y, t), device_id_type=MESH)

    def mate_copy(a, o, theirs=False):
        b = block(a, o, 1 - core if theirs else core)
        return pltpu.make_async_remote_copy(
            src_ref=b, dst_ref=b, send_sem=msend.at[a, o], recv_sem=mrecv.at[a, o],
            device_id=(s, mate), device_id_type=MESH)

    def fan_down(a, o, act):
        @pl.when(jnp.logical_and(o >= z, z > 0))
        def _():
            act(z_copy(a, o, 0))

    def fan_up(a, o, act):
        @pl.when(jnp.logical_and(o <= z, z < nz - 1))
        def _():
            act(z_copy(a, o, 1))

    def fan(a, o, act):
        fan_down(a, o, act)
        fan_up(a, o, act)
        act(mate_copy(a, o))

    def start(c):
        c.start()

    def seed_ready(a):
        @pl.when(y == core)
        def _():
            seed_local(a).wait()

        @pl.when(y != core)
        def _():
            pltpu.make_async_remote_copy(
                src_ref=block(a, z, core), dst_ref=block(a, z, core), send_sem=ssend.at[a], recv_sem=srecv.at[a],
                device_id=(z * ny + 1 - y, mate), device_id_type=MESH).wait_recv()

    def push_seed(a):
        seed_ready(a)
        fan(a, z, start)

    def relay_from(a, o):
        z_copy(a, o, 0).wait_recv()
        fan(a, o, start)

    def relay(items, j):
        for a in items:
            relay_from(a, origin[j])

    def load_seed(a):
        @pl.when(y == core)
        def _():
            seed_local(a).start()

        @pl.when(y != core)
        def _():
            seed_swap(a).start()

    def halo_copy(i):
        src, dst = ((recur.at[pl.ds(tok - 16, 16)], halo), (ids.at[pl.ds(tok - 8, 8)], ihalo))[i]
        return pltpu.make_async_remote_copy(
            src_ref=src, dst_ref=dst, send_sem=hsend.at[i], recv_sem=hrecv.at[i],
            device_id=(lax.rem(s + 1, n), t), device_id_type=MESH)

    for i in range(2):
        halo_copy(i).start()

    for a in GATE:
        load_seed(a)

    @pl.when(y == core)
    def _():
        for a in GATE:
            push_seed(a)

    head = gmap.shape[1]
    spread = (lax.rem(lax.broadcasted_iota(jnp.int32, (head, loc), 1), head)
              == lax.broadcasted_iota(jnp.int32, (head, loc), 0)).astype(BF16)
    diag = (lax.div(lax.broadcasted_iota(jnp.int32, (loc, loc), 0), head)
            == lax.div(lax.broadcasted_iota(jnp.int32, (loc, loc), 1), head))
    for i, m in enumerate((gmap, imap)):
        tiled = jnp.dot(m[...], spread, preferred_element_type=F32)
        bd[i] = jnp.where(diag, tiled, 0.0).astype(BF16)

    for i in range(2):
        halo_copy(i).wait()
    first = s == 0
    xpad[pl.ds(0, 8)] = halo[...].astype(F32)[8:16]
    idpad[pl.ds(0, 8)] = jnp.where(first, -1, ihalo[...])

    def fill(i, _):
        r = pl.multiple_of(i * CH, CH)
        xpad[pl.ds(pl.multiple_of(r + 8, 8), CH)] = recur[pl.ds(r, CH)].astype(F32)
        idpad[pl.ds(pl.multiple_of(r + 8, 8), CH)] = ids[pl.ds(r, CH)]
        return 0

    lax.fori_loop(0, tok // CH, fill, 0)

    reps = loc // 128
    ntaps = taps.shape[0]

    def front(i, _):
        r = pl.multiple_of(i * CH, CH)
        xw = xpad[pl.ds(r, CH + 8)]
        iw = idpad[pl.ds(r, CH + 8)]
        mine = iw[8:]
        tw = taps[...]
        conv = xw[8:] * tw[0:1]
        cont = None
        for k in range(1, ntaps):
            same1 = (pltpu.roll(iw, k, axis=0)[8:] == mine).astype(F32)
            same = jnp.concatenate([same1] * reps, axis=1)
            if k == 1:
                cont = same
            conv = conv + same * pltpu.roll(xw, k, axis=0)[8:] * tw[k:k + 1]
        cb = conv.astype(BF16)
        rg = jax.nn.sigmoid(jnp.dot(cb, bd[0], preferred_element_type=F32))
        ig = jax.nn.sigmoid(jnp.dot(cb, bd[1], preferred_element_type=F32))
        ld = rate[...] * rg + extra[pl.ds(r, CH)]
        fac[pl.ds(r, CH)] = jnp.exp(ld) * cont
        drv[pl.ds(r, CH)] = jnp.sqrt(one_minus_exp(2.0 * ld)) * ig * cb.astype(F32)
        return 0

    lax.fori_loop(0, tok // CH, front, 0)

    @pl.when(y == core)
    def _():
        load_seed(UP[0])

    @pl.when(y != core)
    def _():
        push_seed(GATE[0])

    rows8 = lax.broadcasted_iota(jnp.int32, (8, loc), 0)

    def scan(i, carry):
        pc, hc = carry
        r = pl.multiple_of(i * 8, 8)
        a, b = fac[pl.ds(r, 8)], drv[pl.ds(r, 8)]
        for sh in (1, 2, 4):
            keep = rows8 >= sh
            b = b + a * jnp.where(keep, pltpu.roll(b, sh, axis=0), 0.0)
            a = a * jnp.where(keep, pltpu.roll(a, sh, axis=0), 1.0)
        h = b + a * hc
        p = a * pc
        fac[pl.ds(r, 8)] = p
        drv[pl.ds(r, 8)] = h
        return (jnp.broadcast_to(p[7:8], (8, loc)), jnp.broadcast_to(h[7:8], (8, loc)))

    pend, hend = lax.fori_loop(0, tok // 8, scan, (jnp.ones((8, loc), F32), jnp.zeros((8, loc), F32)))
    ends[s] = jnp.concatenate([pend, hend], axis=0)

    def end_copy(j):
        return pltpu.make_async_remote_copy(
            src_ref=ends.at[s], dst_ref=ends.at[s], send_sem=esend.at[j - 1], recv_sem=erecv.at[j - 1],
            device_id=(lax.rem(s + j, n), t), device_id_type=MESH)

    def end_arrived(j):
        o = lax.rem(s + n - j, n)
        pltpu.make_async_remote_copy(
            src_ref=ends.at[o], dst_ref=ends.at[o], send_sem=esend.at[j - 1], recv_sem=erecv.at[j - 1],
            device_id=(lax.rem(s + j, n), t), device_id_type=MESH).wait_recv()

    for j in range(1, n):
        end_copy(j).start()

    @pl.when(y != core)
    def _():
        load_seed(UP[0])
        push_seed(GATE[1])

    for a in DOWN:
        load_seed(a)

    @pl.when(y == core)
    def _():
        push_seed(UP[0])

    inner = jnp.logical_and(z > 0, z < nz - 1)
    early = min(2, nz - 1)
    for j in range(1, n):
        end_arrived(j)
    carry = jnp.zeros((8, loc), F32)
    for o in range(n - 1):
        e = ends[o]
        carry = jnp.where(o < s, e[:8] * carry + e[8:], carry)
    cin = carry[0:1]

    def branch(i, _):
        r = pl.multiple_of(i * CH, CH)
        st = drv[pl.ds(r, CH)] + fac[pl.ds(r, CH)] * cin
        bfull[t, pl.ds(r, CH)] = (st * jax.nn.gelu(gate_branch[pl.ds(r, CH)].astype(F32))).astype(BF16)
        return 0

    lax.fori_loop(0, tok // CH, branch, 0)

    def tp_push(view, send, recv, j, start):
        o = t if start else lax.rem(t + ntp - j, ntp)
        return pltpu.make_async_remote_copy(
            src_ref=view(o), dst_ref=view(o), send_sem=send.at[j - 1], recv_sem=recv.at[j - 1],
            device_id=(s, lax.rem(t + j, ntp)), device_id_type=MESH)

    def bview(o):
        return bfull.at[o]

    chips = ntp // 2
    core = lax.rem(t, 2)
    mate = t + 1 - 2 * core

    def far(view, send, recv, c, start):
        o = t if start else lax.rem(t + ntp - 2 * c, ntp)
        return pltpu.make_async_remote_copy(
            src_ref=view(o), dst_ref=view(o), send_sem=send.at[c - 1], recv_sem=recv.at[c - 1],
            device_id=(s, lax.rem(t + 2 * c, ntp)), device_id_type=MESH)

    def near(view, send, recv, c, start):
        base = t if start else mate
        o = lax.rem(base + ntp - 2 * c, ntp)
        return pltpu.make_async_remote_copy(
            src_ref=view(o), dst_ref=view(o), send_sem=send.at[chips - 1 + c], recv_sem=recv.at[chips - 1 + c],
            device_id=(s, mate), device_id_type=MESH)

    def gather_start(view, send, recv):
        for c in range(1, chips):
            far(view, send, recv, c, True).start()
        near(view, send, recv, 0, True).start()

    def gather_share(view, send, recv):
        for c in range(1, chips):
            far(view, send, recv, c, False).wait_recv()
            near(view, send, recv, c, True).start()

    def gather_wait(view, send, recv):
        for c in range(chips):
            near(view, send, recv, c, False).wait_recv()

    def gather_sent(view, send, recv):
        for c in range(1, chips):
            far(view, send, recv, c, True).wait_send()
        for c in range(chips):
            near(view, send, recv, c, True).wait_send()

    gather_start(bview, bsend, brecv)

    @pl.when(y != core)
    def _():
        push_seed(UP[0])

    @pl.when(inner)
    def _():
        for j in range(1, early + 1):
            relay(GATE, j)

    gather_share(bview, bsend, brecv)
    gather_wait(bview, bsend, brecv)

    def row_total(q, values):
        def write(i, _):
            r = pl.multiple_of(i * BR, BR)
            v = values(r)
            c = jnp.sum(v * v, axis=1, keepdims=True)
            ssq[q, t, :, pl.ds(r, BR)] = jnp.transpose(jnp.broadcast_to(c, (BR, 128)))[:8]
            return 0

        lax.fori_loop(0, tok // BR, write, 0)
        for j in range(1, ntp):
            tp_push(lambda o: ssq.at[q, o], qsend.at[q], qrecv.at[q], j, True).start()

    def wait_total(q):
        for j in range(1, ntp):
            tp_push(lambda o: ssq.at[q, o], qsend.at[q], qrecv.at[q], j, False).wait_recv()

    def inverse_rms(q, r):
        row = ssq[q, 0, 0:1, pl.ds(r, BR)]
        for o in range(1, ntp):
            row = row + ssq[q, o, 0:1, pl.ds(r, BR)]
        inv = lax.rsqrt(row / width + EPS)
        return jnp.transpose(jnp.broadcast_to(inv, (128, BR)))[:, 0:1]

    def project(i, _):
        r = pl.multiple_of(i * BR, BR)
        total = jnp.zeros((BR, dloc), F32)
        for o in range(ntp):
            total += jnp.dot(bfull[o, pl.ds(r, BR)], out_w[pl.ds(o * loc, loc)], preferred_element_type=F32)
        mixed[pl.ds(r, BR)] = total.astype(BF16)
        return 0

    lax.fori_loop(0, tok // BR, project, 0)
    row_total(0, lambda r: mixed[pl.ds(r, BR)].astype(F32))

    @pl.when(inner)
    def _():
        for j in range(1, early + 1):
            relay(UP, j)

    wait_total(0)

    def stream(i, _):
        r = pl.multiple_of(i * BR, BR)
        m = mixed[pl.ds(r, BR)].astype(F32)
        mixed[pl.ds(r, BR)] = (residual[pl.ds(r, BR)].astype(F32) + m * inverse_rms(0, r) * mix_gain[...]).astype(BF16)
        return 0

    lax.fori_loop(0, tok // BR, stream, 0)
    row_total(1, lambda r: mixed[pl.ds(r, BR)].astype(F32))
    wait_total(1)

    cols = pl.ds(pl.multiple_of(t * dloc, dloc), dloc)

    def norm(i, _):
        r = pl.multiple_of(i * BR, BR)
        m = mixed[pl.ds(r, BR)].astype(F32)
        v = (m * inverse_rms(1, r) * pre_gain[...]).astype(BF16)
        nloc[pl.ds(r, BR)] = v

        @pl.when(y == core)
        def _():
            normed[pl.ds(r, BR), cols] = v

        return 0

    lax.fori_loop(0, tok // BR, norm, 0)

    def n_copy(dy, dx):
        return pltpu.make_async_remote_copy(
            src_ref=nloc, dst_ref=normed.at[:, cols], send_sem=nsend.at[dy, dx], recv_sem=nrecv.at[t],
            device_id=(z * ny + lax.rem(y + dy, ny), 2 * lax.rem(x + dx, chips) + y), device_id_type=MESH)

    def to_plane(act):
        for dy in range(ny):
            for dx in range(chips):
                if dy or dx:
                    act(n_copy(dy, dx))
                else:
                    @pl.when(y != core)
                    def _():
                        act(n_copy(0, 0))

    def n_wait(dt):
        o = lax.rem(t + dt, ntp)
        view = normed.at[:, pl.ds(pl.multiple_of(o * dloc, dloc), dloc)]
        pltpu.make_async_remote_copy(
            src_ref=view, dst_ref=view, send_sem=nsend.at[0, 0], recv_sem=nrecv.at[o],
            device_id=(s, mate), device_id_type=MESH).wait_recv()

    to_plane(start)

    @pl.when(jnp.logical_not(inner))
    def _():
        for a in DOWN:
            push_seed(a)
        for j in range(1, early + 1):
            relay(GATE, j)
            relay(UP, j)

    def outward_seed():
        for a in DOWN:
            @pl.when(low == 1)
            def _():
                fan_down(a, z, start)

            @pl.when(low == 0)
            def _():
                fan_up(a, z, start)

    def mates(js):
        for j in js:
            for a in GATE + UP:
                mate_copy(a, origin[j], True).wait_recv()

    def n_ready():
        for dt in range(1, ntp):
            n_wait(dt)

        @pl.when(y != core)
        def _():
            n_wait(0)

    kblk = ny * krows
    TN = 256
    tiles = ff // TN

    def sums(js, cs):
        g = u = None
        for j in js:
            k = pl.ds(pl.multiple_of(origin[j] * kblk, kblk), kblk)
            a = normed[:, k]
            gj = jnp.dot(a, gate_all[k, cs], preferred_element_type=F32)
            uj = jnp.dot(a, up_all[k, cs], preferred_element_type=F32)
            g, u = (gj, uj) if g is None else (g + gj, u + uj)
        return g, u

    def first_tile(c, size):
        cs = pl.ds(c, size)
        gsum[:, cs], usum[:, cs] = sums(range(nz - 1), cs)

    def last_tile(c, size):
        cs = pl.ds(c, size)
        g, u = sums((nz - 1,), cs)
        g, u = g + gsum[:, cs], u + usum[:, cs]
        hidden[:, cs] = (jax.nn.silu(g) * u).astype(BF16)

    def over_tiles(tile):
        def step(j, _):
            tile(pl.multiple_of(j * TN, TN), TN)
            return 0

        lax.fori_loop(0, tiles, step, 0)
        if ff % TN:
            tile(tiles * TN, ff % TN)

    @pl.when(inner)
    def _():
        for j in range(early + 1, nz):
            relay(GATE, j)
            relay(UP, j)
        for a in DOWN:
            seed_ready(a)
            mate_copy(a, z).start()

            @pl.when(low == 1)
            def _():
                fan_up(a, z, start)

            @pl.when(low == 0)
            def _():
                fan_down(a, z, start)

        @pl.when(core == 0)
        def _():
            outward_seed()

    n_ready()
    mates(range(nz - 1))
    over_tiles(first_tile)

    @pl.when(jnp.logical_not(inner))
    def _():
        for j in range(early + 1, nz):
            relay(GATE, j)
            relay(UP, j)

    mates((nz - 1,))
    over_tiles(last_tile)

    me = y * chips + x

    def p_copy(i, h):
        c = pl.ds(h * hcol, hcol)
        return pltpu.make_async_remote_copy(
            src_ref=partial.at[i, :, c], dst_ref=recvd.at[me, lax.rem(i, per), :, c], send_sem=psend.at[i, h],
            recv_sem=precv.at[me, lax.rem(i, per), h],
            device_id=(z * ny + core, lax.div(i, per)), device_id_type=MESH)

    def owned(i):
        return jnp.logical_and(y == core, lax.div(i, per) == t)

    def ship(i, hs):
        @pl.when(owned(i))
        def _():
            for h in hs:
                c = pl.ds(h * hcol, hcol)
                recvd[me, lax.rem(i, per), :, c] = partial[i, :, c]

        @pl.when(jnp.logical_not(owned(i)))
        def _():
            for h in hs:
                p_copy(i, h).start()

    def mate_ready(a, o, b):
        @pl.when(b != core)
        def _():
            mate_copy(a, o, True).wait_recv()

    def order(b, j):
        if b == 0 or j == 0:
            return origin[j]
        return jnp.where(inner, origin[j], origin[1 + j % (nz - 1)])

    for j in range(nz):
        mine = jnp.where(core == 0, order(0, j), order(1, j))
        if j < nz - 1:
            if j:
                for a in DOWN:
                    relay_from(a, mine)
            for b in range(ny):
                i = order(b, j) * ny + b
                for a in DOWN:
                    mate_ready(a, order(b, j), b)
                partial[i] = jnp.dot(hidden[...], down_all[i], preferred_element_type=F32).astype(BF16)
                ship(i, (0, 1))
        else:
            for h in range(2):
                relay_from(DOWN[h], mine)
                if h == 1:
                    @pl.when(jnp.logical_and(inner, core == 1))
                    def _():
                        outward_seed()

                c = pl.ds(h * hcol, hcol)
                for b in range(ny):
                    i = order(b, j) * ny + b
                    mate_ready(DOWN[h], order(b, j), b)
                    partial[i, :, c] = jnp.dot(hidden[...], down_all[i, :, c], preferred_element_type=F32).astype(BF16)
                    ship(i, (h,))

    def p_wait(dy, dx):
        k = lax.rem(y + dy, ny) * chips + lax.rem(x + dx, chips)
        for w in range(per):
            for h in range(2):
                view = recvd.at[k, w, :, pl.ds(h * hcol, hcol)]
                pltpu.make_async_remote_copy(
                    src_ref=view, dst_ref=view, send_sem=psend.at[0, 0], recv_sem=precv.at[k, w, h],
                    device_id=(s, mate), device_id_type=MESH).wait_recv()

    for dy in range(ny):
        for dx in range(chips):
            if dy or dx:
                p_wait(dy, dx)

    @pl.when(y != core)
    def _():
        p_wait(0, 0)

    def gather_sum(i, _):
        r = pl.multiple_of(i * BR, BR)
        for w in range(per):
            total = recvd[0, w, pl.ds(r, BR)].astype(F32)
            for k in range(1, ny * chips):
                total = total + recvd[k, w, pl.ds(r, BR)].astype(F32)
            out[pl.ds(r, BR), pl.ds(w * ncol, ncol)] = total.astype(BF16)
        return 0

    lax.fori_loop(0, tok // BR, gather_sum, 0)
    row_total(2, lambda r: out[pl.ds(r, BR)].astype(F32))
    wait_total(2)

    def finish(i, _):
        r = pl.multiple_of(i * BR, BR)
        f = out[pl.ds(r, BR)].astype(F32)
        out[pl.ds(r, BR)] = (mixed[pl.ds(r, BR)].astype(F32) + f * inverse_rms(2, r) * ffn_gain[...]).astype(BF16)
        return 0

    lax.fori_loop(0, tok // BR, finish, 0)

    def sent(c):
        c.wait_send()

    for a in GATE + UP + DOWN:
        @pl.when(y != core)
        def _():
            seed_swap(a).wait_send()

        for j in range(nz):
            fan(a, origin[j], sent)
    for j in range(1, n):
        end_copy(j).wait_send()
    gather_sent(bview, bsend, brecv)
    to_plane(sent)
    for i in range(n):
        @pl.when(jnp.logical_not(owned(i)))
        def _():
            for h in range(2):
                p_copy(i, h).wait_send()
    for j in range(1, ntp):
        for q in range(3):
            tp_push(lambda o: ssq.at[q, o], qsend.at[q], qrecv.at[q], j, True).wait_send()


def body(n, ntp, gate_branch, recur_input, doc_ids, conv_taps, gate_map, input_map, decay_level, decay_extra,
         out_weight, residual, mix_gain, pre_gain, ffn_gain, gate_weight, up_weight, down_weight):
    tok, loc = recur_input.shape
    dloc = residual.shape[1]
    krows, ff = gate_weight.shape
    ncol = down_weight.shape[1]
    heads, head, _ = gate_map.shape
    nz, ny = grid_of(n)
    ids = jnp.broadcast_to(doc_ids[:, None], (tok, 128))
    rate = (GATE_POWER * -jax.nn.softplus(-decay_level))[None, :]
    args = (gate_branch, recur_input, ids, conv_taps.astype(F32), gate_map.reshape(heads * head, head),
            input_map.reshape(heads * head, head), rate, decay_extra, out_weight, residual,
            mix_gain[None, :], pre_gain[None, :], ffn_gain[None, :], gate_weight, up_weight, down_weight)
    vm = pl.BlockSpec(memory_space=pltpu.VMEM)
    hbm = pl.BlockSpec(memory_space=pl.ANY)
    V, S = pltpu.VMEM, pltpu.SemaphoreType.DMA
    per = dloc // ncol
    chips = ntp // 2
    if ny == 2:
        fn = plane_kernel
        scratch = [
            V((n * krows, ff), BF16), V((n * krows, ff), BF16), V((n, ff, ncol), BF16),
            V((tok + 8, loc), F32), V((tok + 8, 128), jnp.int32), V((16, loc), BF16), V((8, 128), jnp.int32),
            V((2, loc, loc), BF16), V((tok, loc), F32), V((tok, loc), F32), V((n, 16, loc), F32),
            V((ntp, tok, loc), BF16), V((tok, dloc), BF16), V((tok, dloc), BF16), V((tok, dloc * ntp), BF16),
            V((tok, ff), F32), V((tok, ff), F32), V((tok, ff), BF16), V((n, tok, ncol), BF16), V((ny * chips, per, tok, ncol), BF16), V((3, ntp, 8, tok), F32),
            S((5,)), S((5,)), S((5,)), S((2, 5, nz)), S((5, nz)), S((5, nz)), S((5, nz)),
            S((2,)), S((2,)), S((n - 1,)), S((n - 1,)), S((ntp - 1,)), S((ntp - 1,)),
            S((ny, chips)), S((ntp,)), S((3, ntp - 1)), S((3, ntp - 1)), S((n, 2)), S((ny * chips, per, 2)),
        ]
    else:
        fn = kernel
        scratch = [
            V((n * krows, ff), BF16), V((n * krows, ff), BF16), V((n, ff, ncol), BF16),
            V((tok + 8, loc), F32), V((tok + 8, 128), jnp.int32), V((16, loc), BF16), V((8, 128), jnp.int32),
            V((2, loc, loc), BF16), V((tok, loc), F32), V((tok, loc), F32), V((n, 16, loc), F32),
            V((ntp, tok, loc), BF16), V((tok, dloc), BF16), V((tok, dloc * ntp), BF16), V((tok, ff), BF16),
            V((n, tok, ncol), BF16), V((n, tok, ncol), BF16), V((chips - 1, per, tok, ncol), BF16), V((per, tok, ncol), BF16),
            V((3, ntp, 8, tok), F32),
            S((3, 2, n - 1)), S((3, 2, n - 1)), S((3,)), S((2,)), S((2,)), S((n - 1,)), S((n - 1,)),
            S((ntp - 1,)), S((ntp - 1,)), S((ntp - 1,)), S((ntp - 1,)), S((3, ntp - 1)), S((3, ntp - 1)),
            S((n,)), S((chips - 1, per)), S((n,)),
        ]
    return pl.pallas_call(
        functools.partial(fn, (n, ntp, nz, ny, dloc * ntp)),
        out_shape=jax.ShapeDtypeStruct((tok, dloc), BF16),
        in_specs=[vm] * 13 + [hbm] * 3,
        out_specs=vm,
        scratch_shapes=scratch,
        compiler_params=pltpu.CompilerParams(
            collective_id=0, has_side_effects=True, vmem_limit_bytes=62 * 1024 * 1024),
    )(*args)


def solution(mesh):
    in_specs = (
        P("sp", "tp"), P("sp", "tp"), P("sp"), P(None, "tp"), P("tp", None, None), P("tp", None, None),
        P("tp"), P("sp", "tp"), P(None, "tp"), P("sp", "tp"), P("tp"), P("tp"), P("tp"),
        P("sp", "tp"), P("sp", "tp"), P("tp", "sp"),
    )
    fn = functools.partial(body, mesh.shape["sp"], mesh.shape["tp"])
    return jax.shard_map(fn, mesh=mesh, in_specs=in_specs, out_specs=P("sp", "tp"), check_vma=False)
```

```python
import functools
import math

import jax
import jax.numpy as jnp
from jax import lax
from jax.experimental import pallas as pl
from jax.experimental.pallas import tpu as pltpu
from jax.sharding import PartitionSpec as P

EPS = 1e-06
GATE_POWER = 8.0
F32 = jnp.float32
BF16 = jnp.bfloat16
MESH = pl.DeviceIdType.MESH


def grid_of(n):
    ny = 1
    for c in range(1, n + 1):
        if n % c == 0 and c * c <= n:
            ny = c
    return n // ny, ny


def ring_pos(s, nz, ny):
    z, y = lax.div(s, ny), lax.rem(s, ny)
    off = lax.div(y + ny - 1, ny)
    r = nz - 1 - z
    odd = lax.rem(r, 2)
    within = (1 - odd) * (y - 1) + odd * (ny - 1 - y)
    return (1 - off) * z + off * (nz + r * (ny - 1) + within)


def ring_dev(p, nz, ny):
    off = lax.div(lax.div(p, nz) + ny - 1, ny)
    q = off * (p - nz)
    r = lax.div(q, ny - 1)
    w = lax.rem(q, ny - 1)
    odd = lax.rem(r, 2)
    y = (1 - odd) * (1 + w) + odd * (ny - 1 - w)
    return (1 - off) * (p * ny) + off * ((nz - 1 - r) * ny + y)


def one_minus_exp(u):
    series = 1.0 + u * (1 / 8)
    for k in (7, 6, 5, 4, 3, 2):
        series = 1.0 + u * (1.0 / k) * series
    return jnp.where(u > -0.35, -u * series, 1.0 - jnp.exp(u))


def kernel(
    cfg,
    gate_branch, recur, ids, taps, gmap, imap, rate, extra, out_w, residual,
    mix_gain, pre_gain, ffn_gain, gate_w, up_w, down_w,
    out,
    gate_all, up_all, down_all, xpad, idpad, halo, ihalo, bd, fac, drv, ends, bfull,
    mixed, normed, hidden, partial, shared, recvd, own, ssq,
    wsend, wrecv, lsem, hsend, hrecv, esend, erecv, bsend, brecv, nsend, nrecv, qsend, qrecv, psend, precv, msem,
):
    n, ntp, nz, ny, width = cfg
    s, t = lax.axis_index("sp"), lax.axis_index("tp")
    tok, loc = recur.shape
    dloc = residual.shape[1]
    krows = gate_w.shape[0]
    ncol = down_w.shape[1]
    ff = gate_w.shape[1]
    CH = math.gcd(tok, 64)
    BR = math.gcd(tok, 128)
    pos = ring_pos(s, nz, ny)

    barrier = pltpu.get_barrier_semaphore()
    for j in range(1, n):
        pl.semaphore_signal(barrier, inc=1, device_id=(lax.rem(s + j, n), t), device_id_type=MESH)
    for j in range(1, ntp):
        pl.semaphore_signal(barrier, inc=1, device_id=(s, lax.rem(t + j, ntp)), device_id_type=MESH)
    pl.semaphore_wait(barrier, n - 1 + ntp - 1)

    shard = (gate_w, up_w, down_w)
    whole = (gate_all, up_all, down_all)
    nxt = [ring_dev(lax.rem(pos + 1, n), nz, ny), ring_dev(lax.rem(pos + n - 1, n), nz, ny)]
    origin = [[s] + [ring_dev(lax.rem(pos + (n - k if d == 0 else k), n), nz, ny) for k in range(1, n)] for d in range(2)]

    def half(a, o, d, local=False):
        if a < 2:
            h = krows // 2
            if local:
                return shard[a].at[pl.ds(d * h, h)]
            return whole[a].at[pl.ds(pl.multiple_of(o * krows + d * h, h), h)]
        h = ff // 2
        if local:
            return shard[a].at[pl.ds(d * h, h)]
        return whole[a].at[o, pl.ds(d * h, h)]

    def ring(a, d, k):
        o = origin[d][k]
        return pltpu.make_async_remote_copy(
            src_ref=half(a, o, d, k == 0), dst_ref=half(a, o, d),
            send_sem=wsend.at[a, d, k], recv_sem=wrecv.at[a, d, k],
            device_id=(nxt[d], t), device_id_type=MESH)

    def arrived(a, d, k):
        o = origin[d][k + 1]
        pltpu.make_async_remote_copy(
            src_ref=half(a, o, d), dst_ref=half(a, o, d),
            send_sem=wsend.at[a, d, k], recv_sem=wrecv.at[a, d, k],
            device_id=(nxt[d], t), device_id_type=MESH).wait_recv()

    def serve(arrays, k):
        for a in arrays:
            for d in range(2):
                arrived(a, d, k)
                if k < n - 2:
                    ring(a, d, k + 1).start()

    for a in range(3):
        for d in range(2):
            ring(a, d, 0).start()

    def halo_copy(i):
        src, dst = ((recur.at[pl.ds(tok - 16, 16)], halo), (ids.at[pl.ds(tok - 8, 8)], ihalo))[i]
        return pltpu.make_async_remote_copy(
            src_ref=src, dst_ref=dst, send_sem=hsend.at[i], recv_sem=hrecv.at[i],
            device_id=(lax.rem(s + 1, n), t), device_id_type=MESH)

    for i in range(2):
        halo_copy(i).start()

    def local_copy(a):
        if a < 2:
            dst = whole[a].at[pl.ds(pl.multiple_of(s * krows, krows), krows)]
        else:
            dst = whole[a].at[s]
        return pltpu.make_async_copy(shard[a], dst, lsem.at[a])

    for a in range(3):
        local_copy(a).start()

    head = gmap.shape[1]
    spread = (lax.rem(lax.broadcasted_iota(jnp.int32, (head, loc), 1), head)
              == lax.broadcasted_iota(jnp.int32, (head, loc), 0)).astype(BF16)
    diag = (lax.div(lax.broadcasted_iota(jnp.int32, (loc, loc), 0), head)
            == lax.div(lax.broadcasted_iota(jnp.int32, (loc, loc), 1), head))
    for i, m in enumerate((gmap, imap)):
        tiled = jnp.dot(m[...], spread, preferred_element_type=F32)
        bd[i] = jnp.where(diag, tiled, 0.0).astype(BF16)

    for i in range(2):
        halo_copy(i).wait()
    first = s == 0
    xpad[pl.ds(0, 8)] = halo[...].astype(F32)[8:16]
    idpad[pl.ds(0, 8)] = jnp.where(first, -1, ihalo[...])

    def fill(i, _):
        r = pl.multiple_of(i * CH, CH)
        xpad[pl.ds(pl.multiple_of(r + 8, 8), CH)] = recur[pl.ds(r, CH)].astype(F32)
        idpad[pl.ds(pl.multiple_of(r + 8, 8), CH)] = ids[pl.ds(r, CH)]
        return 0

    lax.fori_loop(0, tok // CH, fill, 0)
    reps = loc // 128
    ntaps = taps.shape[0]

    def front(i, _):
        r = pl.multiple_of(i * CH, CH)
        xw = xpad[pl.ds(r, CH + 8)]
        iw = idpad[pl.ds(r, CH + 8)]
        mine = iw[8:]
        tw = taps[...]
        conv = xw[8:] * tw[0:1]
        cont = None
        for k in range(1, ntaps):
            same1 = (pltpu.roll(iw, k, axis=0)[8:] == mine).astype(F32)
            same = jnp.concatenate([same1] * reps, axis=1)
            if k == 1:
                cont = same
            conv = conv + same * pltpu.roll(xw, k, axis=0)[8:] * tw[k:k + 1]
        cb = conv.astype(BF16)
        rg = jax.nn.sigmoid(jnp.dot(cb, bd[0], preferred_element_type=F32))
        ig = jax.nn.sigmoid(jnp.dot(cb, bd[1], preferred_element_type=F32))
        ld = rate[...] * rg + extra[pl.ds(r, CH)]
        fac[pl.ds(r, CH)] = jnp.exp(ld) * cont
        drv[pl.ds(r, CH)] = jnp.sqrt(one_minus_exp(2.0 * ld)) * ig * cb.astype(F32)
        return 0

    lax.fori_loop(0, tok // CH, front, 0)

    rows8 = lax.broadcasted_iota(jnp.int32, (8, loc), 0)

    def scan(i, carry):
        pc, hc = carry
        r = pl.multiple_of(i * 8, 8)
        a, b = fac[pl.ds(r, 8)], drv[pl.ds(r, 8)]
        for sh in (1, 2, 4):
            keep = rows8 >= sh
            b = b + a * jnp.where(keep, pltpu.roll(b, sh, axis=0), 0.0)
            a = a * jnp.where(keep, pltpu.roll(a, sh, axis=0), 1.0)
        h = b + a * hc
        p = a * pc
        fac[pl.ds(r, 8)] = p
        drv[pl.ds(r, 8)] = h
        return (jnp.broadcast_to(p[7:8], (8, loc)), jnp.broadcast_to(h[7:8], (8, loc)))

    pend, hend = lax.fori_loop(0, tok // 8, scan, (jnp.ones((8, loc), F32), jnp.zeros((8, loc), F32)))
    ends[s] = jnp.concatenate([pend, hend], axis=0)

    def end_copy(j):
        return pltpu.make_async_remote_copy(
            src_ref=ends.at[s], dst_ref=ends.at[s], send_sem=esend.at[j - 1], recv_sem=erecv.at[j - 1],
            device_id=(lax.rem(s + j, n), t), device_id_type=MESH)

    def end_arrived(j):
        o = lax.rem(s + n - j, n)
        pltpu.make_async_remote_copy(
            src_ref=ends.at[o], dst_ref=ends.at[o], send_sem=esend.at[j - 1], recv_sem=erecv.at[j - 1],
            device_id=(lax.rem(s + j, n), t), device_id_type=MESH).wait_recv()

    for j in range(1, n):
        end_copy(j).start()
    serve((0, 1), 0)
    for j in range(1, n):
        end_arrived(j)
    carry = jnp.zeros((8, loc), F32)
    for o in range(n - 1):
        e = ends[o]
        carry = jnp.where(o < s, e[:8] * carry + e[8:], carry)
    cin = carry[0:1]

    def branch(i, _):
        r = pl.multiple_of(i * CH, CH)
        st = drv[pl.ds(r, CH)] + fac[pl.ds(r, CH)] * cin
        bfull[t, pl.ds(r, CH)] = (st * jax.nn.gelu(gate_branch[pl.ds(r, CH)].astype(F32))).astype(BF16)
        return 0

    lax.fori_loop(0, tok // CH, branch, 0)

    def tp_push(view, send, recv, j, start):
        o = t if start else lax.rem(t + ntp - j, ntp)
        return pltpu.make_async_remote_copy(
            src_ref=view(o), dst_ref=view(o), send_sem=send.at[j - 1], recv_sem=recv.at[j - 1],
            device_id=(s, lax.rem(t + j, ntp)), device_id_type=MESH)

    def bview(o):
        return bfull.at[o]

    chips = ntp // 2
    core = lax.rem(t, 2)
    mate = t + 1 - 2 * core

    def far(view, send, recv, c, start):
        o = t if start else lax.rem(t + ntp - 2 * c, ntp)
        return pltpu.make_async_remote_copy(
            src_ref=view(o), dst_ref=view(o), send_sem=send.at[c - 1], recv_sem=recv.at[c - 1],
            device_id=(s, lax.rem(t + 2 * c, ntp)), device_id_type=MESH)

    def near(view, send, recv, c, start):
        base = t if start else mate
        o = lax.rem(base + ntp - 2 * c, ntp)
        return pltpu.make_async_remote_copy(
            src_ref=view(o), dst_ref=view(o), send_sem=send.at[chips - 1 + c], recv_sem=recv.at[chips - 1 + c],
            device_id=(s, mate), device_id_type=MESH)

    def gather_start(view, send, recv):
        for c in range(1, chips):
            far(view, send, recv, c, True).start()
        near(view, send, recv, 0, True).start()

    def gather_share(view, send, recv):
        for c in range(1, chips):
            far(view, send, recv, c, False).wait_recv()
            near(view, send, recv, c, True).start()

    def gather_wait(view, send, recv):
        for c in range(chips):
            near(view, send, recv, c, False).wait_recv()

    def gather_sent(view, send, recv):
        for c in range(1, chips):
            far(view, send, recv, c, True).wait_send()
        for c in range(chips):
            near(view, send, recv, c, True).wait_send()

    gather_start(bview, bsend, brecv)
    serve((0, 1), 1)
    gather_share(bview, bsend, brecv)
    gather_wait(bview, bsend, brecv)

    def row_total(q, values):
        def write(i, _):
            r = pl.multiple_of(i * BR, BR)
            v = values(r)
            c = jnp.sum(v * v, axis=1, keepdims=True)
            ssq[q, t, :, pl.ds(r, BR)] = jnp.transpose(jnp.broadcast_to(c, (BR, 128)))[:8]
            return 0

        lax.fori_loop(0, tok // BR, write, 0)
        for j in range(1, ntp):
            tp_push(lambda o: ssq.at[q, o], qsend.at[q], qrecv.at[q], j, True).start()

    def wait_total(q):
        for j in range(1, ntp):
            tp_push(lambda o: ssq.at[q, o], qsend.at[q], qrecv.at[q], j, False).wait_recv()

    def inverse_rms(q, r):
        row = ssq[q, 0, 0:1, pl.ds(r, BR)]
        for o in range(1, ntp):
            row = row + ssq[q, o, 0:1, pl.ds(r, BR)]
        inv = lax.rsqrt(row / width + EPS)
        return jnp.transpose(jnp.broadcast_to(inv, (128, BR)))[:, 0:1]

    def project(i, _):
        r = pl.multiple_of(i * BR, BR)
        total = jnp.zeros((BR, dloc), F32)
        for o in range(ntp):
            total += jnp.dot(bfull[o, pl.ds(r, BR)], out_w[pl.ds(o * loc, loc)], preferred_element_type=F32)
        mixed[pl.ds(r, BR)] = total.astype(BF16)
        return 0

    lax.fori_loop(0, tok // BR, project, 0)
    row_total(0, lambda r: mixed[pl.ds(r, BR)].astype(F32))
    wait_total(0)

    def stream(i, _):
        r = pl.multiple_of(i * BR, BR)
        m = mixed[pl.ds(r, BR)].astype(F32)
        mixed[pl.ds(r, BR)] = (residual[pl.ds(r, BR)].astype(F32) + m * inverse_rms(0, r) * mix_gain[...]).astype(BF16)
        return 0

    lax.fori_loop(0, tok // BR, stream, 0)
    row_total(1, lambda r: mixed[pl.ds(r, BR)].astype(F32))
    serve((0, 1), 2)
    wait_total(1)

    def norm(i, _):
        r = pl.multiple_of(i * BR, BR)
        m = mixed[pl.ds(r, BR)].astype(F32)
        normed[pl.ds(r, BR), pl.ds(pl.multiple_of(t * dloc, dloc), dloc)] = (m * inverse_rms(1, r) * pre_gain[...]).astype(BF16)
        return 0

    lax.fori_loop(0, tok // BR, norm, 0)

    def nview(o):
        return normed.at[:, pl.ds(pl.multiple_of(o * dloc, dloc), dloc)]

    gather_start(nview, nsend, nrecv)
    serve((0, 1), 3)
    gather_share(nview, nsend, nrecv)
    for k in range(4, n - 2):
        serve((0, 1), k)
    serve((2,), 0)
    serve((0, 1), n - 2)
    gather_wait(nview, nsend, nrecv)
    for a in range(3):
        local_copy(a).wait()

    def ffn_tile(c, size):
        cols = pl.ds(c, size)
        g = jnp.dot(normed[...], gate_all[:, cols], preferred_element_type=F32)
        u = jnp.dot(normed[...], up_all[:, cols], preferred_element_type=F32)
        hidden[:, cols] = (jax.nn.silu(g) * u).astype(BF16)

    TN = 256
    tiles = ff // TN

    def ffn_step(j, _):
        ffn_tile(pl.multiple_of(j * TN, TN), TN)
        return 0

    cut = (tiles + 1) // 2
    lax.fori_loop(0, cut, ffn_step, 0)
    serve((2,), 1)
    lax.fori_loop(cut, tiles, ffn_step, 0)
    if ff % TN:
        ffn_tile(tiles * TN, ff % TN)

    per = dloc // ncol

    def place(o):
        c = lax.div(o, per)
        w = lax.rem(o, per)
        gap = lax.rem(lax.div(c, 2) - lax.div(t, 2) + chips, chips)
        return lax.rem(c, 2), w, c, gap

    def mate_copy(i):
        return pltpu.make_async_remote_copy(
            src_ref=partial.at[i], dst_ref=shared.at[i], send_sem=psend.at[i], recv_sem=msem.at[i],
            device_id=(s, mate), device_id_type=MESH)

    def far_copy(i, w, c, gap):
        g = lax.rem(gap + chips - 1, chips)
        return pltpu.make_async_remote_copy(
            src_ref=partial.at[i], dst_ref=recvd.at[g, w], send_sem=psend.at[i], recv_sem=precv.at[g, w],
            device_id=(s, c), device_id_type=MESH)

    sent = []

    def down(*blocks):
        for o in blocks:
            i = len(sent)
            sent.append(o)
            partial[i] = jnp.dot(hidden[...], down_all[o], preferred_element_type=F32).astype(BF16)
            par, w, c, gap = place(o)

            @pl.when(par != core)
            def _():
                mate_copy(i).start()

    def join(i):
        par, w, c, gap = place(sent[i])

        @pl.when(par == core)
        def _():
            mate_copy(i).wait_recv()

            def add(b, _):
                r = pl.multiple_of(b * BR, BR)
                total = partial[i, pl.ds(r, BR)].astype(F32) + shared[i, pl.ds(r, BR)].astype(F32)
                partial[i, pl.ds(r, BR)] = total.astype(BF16)
                return 0

            lax.fori_loop(0, tok // BR, add, 0)

            @pl.when(gap == 0)
            def _():
                own[w] = partial[i]

            @pl.when(gap != 0)
            def _():
                far_copy(i, w, c, gap).start()

    down(s)
    joined = 0
    for k in range(2, n - 1):
        serve((2,), k)
        have = k + 1
        if 2 * have >= n:
            if 2 * have == n:
                down(origin[0][have])
            else:
                down(origin[0][have], origin[0][n - have])
        if k == n - 2:
            upto = len(sent)
        else:
            upto = len(sent) - (1 if 2 * have == n else 2) if 2 * have >= n else len(sent)
        while joined < upto:
            join(joined)
            joined += 1

    for i, o in enumerate(sent):
        par, w, c, gap = place(o)

        @pl.when(par != core)
        def _():
            mate_copy(i).wait_send()

        @pl.when(par == core)
        def _():
            @pl.when(gap != 0)
            def _():
                far_copy(i, w, c, gap).wait_send()

    for g in range(1, chips):
        for w in range(per):
            pltpu.make_async_remote_copy(
                src_ref=partial.at[0], dst_ref=recvd.at[g - 1, w],
                send_sem=psend.at[0], recv_sem=precv.at[g - 1, w],
                device_id=(s, mate), device_id_type=MESH).wait_recv()

    def gather_sum(i, _):
        r = pl.multiple_of(i * BR, BR)
        for w in range(per):
            total = own[w, pl.ds(r, BR)].astype(F32)
            for j in range(chips - 1):
                total = total + recvd[j, w, pl.ds(r, BR)].astype(F32)
            out[pl.ds(r, BR), pl.ds(w * ncol, ncol)] = total.astype(BF16)
        return 0

    lax.fori_loop(0, tok // BR, gather_sum, 0)
    row_total(2, lambda r: out[pl.ds(r, BR)].astype(F32))
    wait_total(2)

    def finish(i, _):
        r = pl.multiple_of(i * BR, BR)
        f = out[pl.ds(r, BR)].astype(F32)
        out[pl.ds(r, BR)] = (mixed[pl.ds(r, BR)].astype(F32) + f * inverse_rms(2, r) * ffn_gain[...]).astype(BF16)
        return 0

    lax.fori_loop(0, tok // BR, finish, 0)

    for a in range(3):
        for d in range(2):
            for k in range(n - 1):
                ring(a, d, k).wait_send()
    for j in range(1, n):
        end_copy(j).wait_send()
    gather_sent(bview, bsend, brecv)
    gather_sent(nview, nsend, nrecv)
    for j in range(1, ntp):
        for q in range(3):
            tp_push(lambda o: ssq.at[q, o], qsend.at[q], qrecv.at[q], j, True).wait_send()


def plane_kernel(
    cfg,
    gate_branch_in, recur_in, ids, taps, gmap, imap, level, extra_in, out_w_in, residual_in,
    mix_gain, pre_gain, ffn_gain, gate_w, up_w, down_w,
    out_hbm,
    out, osem, gate_branch, recur, extra, out_w, residual, insem,
    gate_all, up_all, down_all, xpad, idpad, halo, ihalo, bd, fac, drv, ends, bfull,
    mixed, nloc, normed, gsum, usum, hidden, partial, recvd, ssq,
    lsem, ssend, srecv, zsend, zrecv, msend, mrecv,
    hsend, hrecv, esend, erecv, bsend, brecv, nsend, nrecv, qsend, qrecv, psend, precv,
):
    n, ntp, nz, ny, width = cfg
    s, t = lax.axis_index("sp"), lax.axis_index("tp")
    tok, loc = recur.shape
    dloc = residual.shape[1]
    krows = gate_w.shape[0]
    ncol = down_w.shape[1]
    ff = gate_w.shape[1]
    CH = math.gcd(tok, 64)
    BR = math.gcd(tok, 128)
    chips = ntp // 2
    z, y = lax.div(s, ny), lax.rem(s, ny)
    x, core = lax.div(t, 2), lax.rem(t, 2)
    mate = t + 1 - 2 * core
    per = dloc // ncol

    barrier = pltpu.get_barrier_semaphore()
    peers = [(z * ny + lax.rem(y + dy, ny), lax.rem(t + dt, ntp)) for dy in range(ny) for dt in range(ntp)][1:]
    peers += [(lax.rem(z + dz, nz) * ny + lax.rem(y + dy, ny), t) for dz in range(1, nz) for dy in range(ny)]
    for p in peers:
        pl.semaphore_signal(barrier, inc=1, device_id=p, device_id_type=MESH)

    inputs = ((recur_in, recur), (extra_in, extra), (gate_branch_in, gate_branch), (out_w_in, out_w), (residual_in, residual))

    def load_input(i):
        return pltpu.make_async_copy(inputs[i][0], inputs[i][1], insem.at[i])

    for i in range(len(inputs)):
        load_input(i).start()
    pl.semaphore_wait(barrier, len(peers))

    low = (2 * z < nz).astype(jnp.int32)
    near_first = []
    for k in range(1, nz):
        near_first += [z + (2 * low - 1) * k, z - (2 * low - 1) * k]
    origin = [z]
    seen = 0
    ranks = []
    for q in near_first:
        ok = jnp.logical_and(q >= 0, q < nz).astype(jnp.int32)
        seen = seen + ok
        ranks.append((q, ok, seen))
    for j in range(1, nz):
        origin.append(sum(jnp.where(jnp.logical_and(ok == 1, r == j), q, 0) for q, ok, r in ranks))

    hcol = ncol // 2
    hrow = krows // 2
    GATE, UP, DOWN = (0, 1), (2,), (3, 4)

    def block(a, o, b):
        i = o * ny + b
        if a in GATE:
            return gate_all.at[pl.ds(pl.multiple_of(i * krows + a * hrow, hrow), hrow)]
        if a in UP:
            return up_all.at[pl.ds(pl.multiple_of(i * krows, krows), krows)]
        return down_all.at[i, :, pl.ds((a - DOWN[0]) * hcol, hcol)]

    def own_shard(a):
        if a in GATE:
            return gate_w.at[pl.ds(a * hrow, hrow)]
        if a in UP:
            return up_w
        return down_w.at[:, pl.ds((a - DOWN[0]) * hcol, hcol)]

    def seed_local(a):
        return pltpu.make_async_copy(own_shard(a), block(a, z, y), lsem.at[a])

    def seed_swap(a):
        return pltpu.make_async_remote_copy(
            src_ref=own_shard(a), dst_ref=block(a, z, y), send_sem=ssend.at[a], recv_sem=srecv.at[a],
            device_id=(z * ny + 1 - y, mate), device_id_type=MESH)

    def z_copy(a, o, up):
        b = block(a, o, core)
        return pltpu.make_async_remote_copy(
            src_ref=b, dst_ref=b, send_sem=zsend.at[up, a, o], recv_sem=zrecv.at[a, o],
            device_id=((z + 2 * up - 1) * ny + y, t), device_id_type=MESH)

    def mate_copy(a, o, theirs=False):
        b = block(a, o, 1 - core if theirs else core)
        return pltpu.make_async_remote_copy(
            src_ref=b, dst_ref=b, send_sem=msend.at[a, o], recv_sem=mrecv.at[a, o],
            device_id=(s, mate), device_id_type=MESH)

    def fan_down(a, o, act):
        @pl.when(jnp.logical_and(o >= z, z > 0))
        def _():
            act(z_copy(a, o, 0))

    def fan_up(a, o, act):
        @pl.when(jnp.logical_and(o <= z, z < nz - 1))
        def _():
            act(z_copy(a, o, 1))

    def fan(a, o, act):
        fan_down(a, o, act)
        fan_up(a, o, act)
        act(mate_copy(a, o))

    def start(c):
        c.start()

    def seed_ready(a):
        @pl.when(y == core)
        def _():
            seed_local(a).wait()

        @pl.when(y != core)
        def _():
            pltpu.make_async_remote_copy(
                src_ref=block(a, z, core), dst_ref=block(a, z, core), send_sem=ssend.at[a], recv_sem=srecv.at[a],
                device_id=(z * ny + 1 - y, mate), device_id_type=MESH).wait_recv()

    def push_seed(a):
        seed_ready(a)
        fan(a, z, start)

    def relay_from(a, o):
        z_copy(a, o, 0).wait_recv()
        fan(a, o, start)

    def relay(items, j):
        for a in items:
            relay_from(a, origin[j])

    def load_seed(a):
        @pl.when(y == core)
        def _():
            seed_local(a).start()

        @pl.when(y != core)
        def _():
            seed_swap(a).start()

    def halo_copy(i):
        src, dst = ((recur_in.at[pl.ds(tok - 16, 16)], halo), (ids, ihalo))[i]
        return pltpu.make_async_remote_copy(
            src_ref=src, dst_ref=dst, send_sem=hsend.at[i], recv_sem=hrecv.at[i],
            device_id=(lax.rem(s + 1, n), t), device_id_type=MESH)

    for i in range(2):
        halo_copy(i).start()

    for a in GATE:
        load_seed(a)

    @pl.when(y == core)
    def _():
        for a in GATE:
            push_seed(a)

    head = gmap.shape[1]
    spread = (lax.rem(lax.broadcasted_iota(jnp.int32, (head, loc), 1), head)
              == lax.broadcasted_iota(jnp.int32, (head, loc), 0)).astype(BF16)
    diag = (lax.div(lax.broadcasted_iota(jnp.int32, (loc, loc), 0), head)
            == lax.div(lax.broadcasted_iota(jnp.int32, (loc, loc), 1), head))
    for i, m in enumerate((gmap, imap)):
        tiled = jnp.dot(m[...], spread, preferred_element_type=F32)
        bd[i] = jnp.where(diag, tiled, 0.0).astype(BF16)

    for i in range(2):
        load_input(i).wait()

    def down_rows(row):
        return jnp.transpose(jnp.broadcast_to(row, (128, 128)))

    for i in range(tok // 128):
        idpad[pl.ds(8 + i * 128, 128)] = down_rows(ids[i:i + 1])

    def fill(i, _):
        r = pl.multiple_of(i * CH, CH)
        xpad[pl.ds(pl.multiple_of(r + 8, 8), CH)] = recur[pl.ds(r, CH)].astype(F32)
        return 0

    lax.fori_loop(0, tok // CH, fill, 0)
    u = -level[...]
    rate = -GATE_POWER * (jnp.maximum(u, 0.0) + jnp.log1p(jnp.exp(-jnp.abs(u))))
    for i in range(2):
        halo_copy(i).wait()
    first = s == 0
    xpad[pl.ds(0, 8)] = halo[...].astype(F32)[8:16]
    idpad[pl.ds(0, 8)] = jnp.where(first, -1, down_rows(ihalo[tok // 128 - 1:tok // 128])[120:])
    reps = loc // 128
    ntaps = taps.shape[0]

    def front(i, _):
        r = pl.multiple_of(i * CH, CH)
        xw = xpad[pl.ds(r, CH + 8)]
        iw = idpad[pl.ds(r, CH + 8)]
        mine = iw[8:]
        tw = taps[...].astype(F32)
        conv = xw[8:] * tw[0:1]
        cont = None
        for k in range(1, ntaps):
            same1 = (pltpu.roll(iw, k, axis=0)[8:] == mine).astype(F32)
            same = jnp.concatenate([same1] * reps, axis=1)
            if k == 1:
                cont = same
            conv = conv + same * pltpu.roll(xw, k, axis=0)[8:] * tw[k:k + 1]
        cb = conv.astype(BF16)
        rg = jax.nn.sigmoid(jnp.dot(cb, bd[0], preferred_element_type=F32))
        ig = jax.nn.sigmoid(jnp.dot(cb, bd[1], preferred_element_type=F32))
        ld = rate * rg + extra[pl.ds(r, CH)]
        fac[pl.ds(r, CH)] = jnp.exp(ld) * cont
        drv[pl.ds(r, CH)] = jnp.sqrt(one_minus_exp(2.0 * ld)) * ig * cb.astype(F32)
        return 0

    lax.fori_loop(0, tok // CH, front, 0)

    @pl.when(y == core)
    def _():
        load_seed(UP[0])

    rows8 = lax.broadcasted_iota(jnp.int32, (8, loc), 0)

    def scan(i, carry):
        pc, hc = carry
        r = pl.multiple_of(i * 8, 8)
        a, b = fac[pl.ds(r, 8)], drv[pl.ds(r, 8)]
        for sh in (1, 2, 4):
            keep = rows8 >= sh
            b = b + a * jnp.where(keep, pltpu.roll(b, sh, axis=0), 0.0)
            a = a * jnp.where(keep, pltpu.roll(a, sh, axis=0), 1.0)
        h = b + a * hc
        p = a * pc
        fac[pl.ds(r, 8)] = p
        drv[pl.ds(r, 8)] = h
        return (jnp.broadcast_to(p[7:8], (8, loc)), jnp.broadcast_to(h[7:8], (8, loc)))

    pend, hend = lax.fori_loop(0, tok // 8, scan, (jnp.ones((8, loc), F32), jnp.zeros((8, loc), F32)))
    ends[s] = jnp.concatenate([pend, hend], axis=0)

    def end_copy(j):
        return pltpu.make_async_remote_copy(
            src_ref=ends.at[s], dst_ref=ends.at[s], send_sem=esend.at[j - 1], recv_sem=erecv.at[j - 1],
            device_id=(lax.rem(s + j, n), t), device_id_type=MESH)

    def end_arrived(j):
        o = lax.rem(s + n - j, n)
        pltpu.make_async_remote_copy(
            src_ref=ends.at[o], dst_ref=ends.at[o], send_sem=esend.at[j - 1], recv_sem=erecv.at[j - 1],
            device_id=(lax.rem(s + j, n), t), device_id_type=MESH).wait_recv()

    for j in range(1, n):
        end_copy(j).start()

    @pl.when(y != core)
    def _():
        for a in GATE:
            push_seed(a)
        load_seed(UP[0])

    for a in DOWN:
        load_seed(a)

    @pl.when(y == core)
    def _():
        push_seed(UP[0])

    inner = jnp.logical_and(z > 0, z < nz - 1)
    early = min(2, nz - 1)
    for j in range(1, n):
        end_arrived(j)
    carry = jnp.zeros((8, loc), F32)
    for o in range(n - 1):
        e = ends[o]
        carry = jnp.where(o < s, e[:8] * carry + e[8:], carry)
    cin = carry[0:1]

    for i in range(2, len(inputs)):
        load_input(i).wait()

    def branch(i, _):
        r = pl.multiple_of(i * CH, CH)
        st = drv[pl.ds(r, CH)] + fac[pl.ds(r, CH)] * cin
        bfull[t, pl.ds(r, CH)] = (st * jax.nn.gelu(gate_branch[pl.ds(r, CH)].astype(F32))).astype(BF16)
        return 0

    lax.fori_loop(0, tok // CH, branch, 0)

    def tp_push(view, send, recv, j, start):
        o = t if start else lax.rem(t + ntp - j, ntp)
        return pltpu.make_async_remote_copy(
            src_ref=view(o), dst_ref=view(o), send_sem=send.at[j - 1], recv_sem=recv.at[j - 1],
            device_id=(s, lax.rem(t + j, ntp)), device_id_type=MESH)

    def bview(o):
        return bfull.at[o]

    chips = ntp // 2
    core = lax.rem(t, 2)
    mate = t + 1 - 2 * core

    def far(view, send, recv, c, start):
        o = t if start else lax.rem(t + ntp - 2 * c, ntp)
        return pltpu.make_async_remote_copy(
            src_ref=view(o), dst_ref=view(o), send_sem=send.at[c - 1], recv_sem=recv.at[c - 1],
            device_id=(s, lax.rem(t + 2 * c, ntp)), device_id_type=MESH)

    def near(view, send, recv, c, start):
        base = t if start else mate
        o = lax.rem(base + ntp - 2 * c, ntp)
        return pltpu.make_async_remote_copy(
            src_ref=view(o), dst_ref=view(o), send_sem=send.at[chips - 1 + c], recv_sem=recv.at[chips - 1 + c],
            device_id=(s, mate), device_id_type=MESH)

    def gather_start(view, send, recv):
        for c in range(1, chips):
            far(view, send, recv, c, True).start()
        near(view, send, recv, 0, True).start()

    def gather_share(view, send, recv):
        for c in range(1, chips):
            far(view, send, recv, c, False).wait_recv()
            near(view, send, recv, c, True).start()

    def gather_wait(view, send, recv):
        for c in range(chips):
            near(view, send, recv, c, False).wait_recv()

    def gather_sent(view, send, recv):
        for c in range(1, chips):
            far(view, send, recv, c, True).wait_send()
        for c in range(chips):
            near(view, send, recv, c, True).wait_send()

    gather_start(bview, bsend, brecv)

    @pl.when(y != core)
    def _():
        push_seed(UP[0])

    @pl.when(inner)
    def _():
        for j in range(1, early + 1):
            relay(GATE, j)

    gather_share(bview, bsend, brecv)
    gather_wait(bview, bsend, brecv)

    def row_total(q, values):
        def write(i, _):
            r = pl.multiple_of(i * BR, BR)
            v = values(r)
            c = jnp.sum(v * v, axis=1, keepdims=True)
            ssq[q, t, :, pl.ds(r, BR)] = jnp.transpose(jnp.broadcast_to(c, (BR, 128)))[:8]
            return 0

        lax.fori_loop(0, tok // BR, write, 0, unroll=True)
        for j in range(1, ntp):
            tp_push(lambda o: ssq.at[q, o], qsend.at[q], qrecv.at[q], j, True).start()

    def wait_total(q):
        for j in range(1, ntp):
            tp_push(lambda o: ssq.at[q, o], qsend.at[q], qrecv.at[q], j, False).wait_recv()

    def inverse_rms(q, r):
        row = ssq[q, 0, 0:1, pl.ds(r, BR)]
        for o in range(1, ntp):
            row = row + ssq[q, o, 0:1, pl.ds(r, BR)]
        inv = lax.rsqrt(row / width + EPS)
        return jnp.transpose(jnp.broadcast_to(inv, (128, BR)))[:, 0:1]

    def project(i, _):
        r = pl.multiple_of(i * BR, BR)
        total = jnp.zeros((BR, dloc), F32)
        for o in range(ntp):
            total += jnp.dot(bfull[o, pl.ds(r, BR)], out_w[pl.ds(o * loc, loc)], preferred_element_type=F32)
        mixed[pl.ds(r, BR)] = total.astype(BF16)
        return 0

    lax.fori_loop(0, tok // BR, project, 0)
    row_total(0, lambda r: mixed[pl.ds(r, BR)].astype(F32))

    @pl.when(inner)
    def _():
        for j in range(1, early + 1):
            relay(UP, j)

    wait_total(0)

    def stream(i, _):
        r = pl.multiple_of(i * BR, BR)
        m = mixed[pl.ds(r, BR)].astype(F32)
        mixed[pl.ds(r, BR)] = (residual[pl.ds(r, BR)].astype(F32) + m * inverse_rms(0, r) * mix_gain[...]).astype(BF16)
        return 0

    lax.fori_loop(0, tok // BR, stream, 0, unroll=True)
    row_total(1, lambda r: mixed[pl.ds(r, BR)].astype(F32))
    wait_total(1)

    cols = pl.ds(pl.multiple_of(t * dloc, dloc), dloc)

    def norm(i, _):
        r = pl.multiple_of(i * BR, BR)
        m = mixed[pl.ds(r, BR)].astype(F32)
        v = (m * inverse_rms(1, r) * pre_gain[...]).astype(BF16)
        nloc[pl.ds(r, BR)] = v

        @pl.when(y == core)
        def _():
            normed[pl.ds(r, BR), cols] = v

        return 0

    lax.fori_loop(0, tok // BR, norm, 0, unroll=True)

    def n_copy(dy, dx):
        return pltpu.make_async_remote_copy(
            src_ref=nloc, dst_ref=normed.at[:, cols], send_sem=nsend.at[dy, dx], recv_sem=nrecv.at[t],
            device_id=(z * ny + lax.rem(y + dy, ny), 2 * lax.rem(x + dx, chips) + y), device_id_type=MESH)

    def to_plane(act):
        for dy in range(ny):
            for dx in range(chips):
                if dy or dx:
                    act(n_copy(dy, dx))
                else:
                    @pl.when(y != core)
                    def _():
                        act(n_copy(0, 0))

    def n_wait(dt):
        o = lax.rem(t + dt, ntp)
        view = normed.at[:, pl.ds(pl.multiple_of(o * dloc, dloc), dloc)]
        pltpu.make_async_remote_copy(
            src_ref=view, dst_ref=view, send_sem=nsend.at[0, 0], recv_sem=nrecv.at[o],
            device_id=(s, mate), device_id_type=MESH).wait_recv()

    to_plane(start)

    @pl.when(jnp.logical_not(inner))
    def _():
        for a in DOWN:
            push_seed(a)
        for j in range(1, early + 1):
            relay(GATE, j)
            relay(UP, j)

    def outward_seed():
        for a in DOWN:
            @pl.when(low == 1)
            def _():
                fan_down(a, z, start)

            @pl.when(low == 0)
            def _():
                fan_up(a, z, start)

    def mates(js):
        for j in js:
            for a in GATE + UP:
                mate_copy(a, origin[j], True).wait_recv()

    def n_ready():
        for dt in range(1, ntp):
            n_wait(dt)

        @pl.when(y != core)
        def _():
            n_wait(0)

    kblk = ny * krows
    TN = 256
    tiles = ff // TN

    def sums(js, cs):
        g = u = None
        for j in js:
            k = pl.ds(pl.multiple_of(origin[j] * kblk, kblk), kblk)
            a = normed[:, k]
            gj = jnp.dot(a, gate_all[k, cs], preferred_element_type=F32)
            uj = jnp.dot(a, up_all[k, cs], preferred_element_type=F32)
            g, u = (gj, uj) if g is None else (g + gj, u + uj)
        return g, u

    def first_tile(c, size):
        cs = pl.ds(c, size)
        gsum[:, cs], usum[:, cs] = sums(range(nz - 1), cs)

    def last_tile(c, size):
        cs = pl.ds(c, size)
        g, u = sums((nz - 1,), cs)
        g, u = g + gsum[:, cs], u + usum[:, cs]
        hidden[:, cs] = (jax.nn.silu(g) * u).astype(BF16)

    def over_tiles(tile):
        def step(j, _):
            tile(pl.multiple_of(j * TN, TN), TN)
            return 0

        lax.fori_loop(0, tiles, step, 0)
        if ff % TN:
            tile(tiles * TN, ff % TN)

    @pl.when(inner)
    def _():
        for j in range(early + 1, nz):
            relay(GATE, j)
            relay(UP, j)
        for a in DOWN:
            seed_ready(a)
            mate_copy(a, z).start()

            @pl.when(low == 1)
            def _():
                fan_up(a, z, start)

            @pl.when(low == 0)
            def _():
                fan_down(a, z, start)

        @pl.when(core == 0)
        def _():
            outward_seed()

    n_ready()
    mates(range(nz - 1))
    over_tiles(first_tile)

    @pl.when(jnp.logical_not(inner))
    def _():
        for j in range(early + 1, nz):
            relay(GATE, j)
            relay(UP, j)

    mates((nz - 1,))
    over_tiles(last_tile)

    me = y * chips + x

    def p_copy(i, h):
        c = pl.ds(h * hcol, hcol)
        return pltpu.make_async_remote_copy(
            src_ref=partial.at[i, :, c], dst_ref=recvd.at[me, lax.rem(i, per), :, c], send_sem=psend.at[i, h],
            recv_sem=precv.at[me, lax.rem(i, per), h],
            device_id=(z * ny + core, lax.div(i, per)), device_id_type=MESH)

    def owned(i):
        return jnp.logical_and(y == core, lax.div(i, per) == t)

    def ship(i, hs):
        @pl.when(owned(i))
        def _():
            for h in hs:
                c = pl.ds(h * hcol, hcol)
                recvd[me, lax.rem(i, per), :, c] = partial[i, :, c]

        @pl.when(jnp.logical_not(owned(i)))
        def _():
            for h in hs:
                p_copy(i, h).start()

    def mate_ready(a, o, b):
        @pl.when(b != core)
        def _():
            mate_copy(a, o, True).wait_recv()

    def order(b, j):
        if b == 0 or j == 0:
            return origin[j]
        return jnp.where(inner, origin[j], origin[1 + j % (nz - 1)])

    for j in range(nz):
        mine = jnp.where(core == 0, order(0, j), order(1, j))
        if j < nz - 1:
            if j:
                for a in DOWN:
                    relay_from(a, mine)
            for b in range(ny):
                i = order(b, j) * ny + b
                for a in DOWN:
                    mate_ready(a, order(b, j), b)
                partial[i] = jnp.dot(hidden[...], down_all[i], preferred_element_type=F32).astype(BF16)
                ship(i, (0, 1))
        else:
            for h in range(2):
                relay_from(DOWN[h], mine)
                if h == 1:
                    @pl.when(jnp.logical_and(inner, core == 1))
                    def _():
                        outward_seed()

                c = pl.ds(h * hcol, hcol)
                for b in range(ny):
                    i = order(b, j) * ny + b
                    mate_ready(DOWN[h], order(b, j), b)
                    partial[i, :, c] = jnp.dot(hidden[...], down_all[i, :, c], preferred_element_type=F32).astype(BF16)
                    ship(i, (h,))

    def p_wait(dy, dx):
        k = lax.rem(y + dy, ny) * chips + lax.rem(x + dx, chips)
        for w in range(per):
            for h in range(2):
                view = recvd.at[k, w, :, pl.ds(h * hcol, hcol)]
                pltpu.make_async_remote_copy(
                    src_ref=view, dst_ref=view, send_sem=psend.at[0, 0], recv_sem=precv.at[k, w, h],
                    device_id=(s, mate), device_id_type=MESH).wait_recv()

    for dy in range(ny):
        for dx in range(chips):
            if dy or dx:
                p_wait(dy, dx)

    @pl.when(y != core)
    def _():
        p_wait(0, 0)

    def ffn_rows(r):
        for w in range(per):
            total = recvd[0, w, pl.ds(r, BR)].astype(F32)
            for k in range(1, ny * chips):
                total = total + recvd[k, w, pl.ds(r, BR)].astype(F32)
            out[pl.ds(r, BR), pl.ds(w * ncol, ncol)] = total.astype(BF16)
        return out[pl.ds(r, BR)].astype(F32)

    row_total(2, ffn_rows)
    wait_total(2)

    def out_copy(i):
        rows = pl.ds(pl.multiple_of(i * BR, BR), BR)
        return pltpu.make_async_copy(out.at[rows], out_hbm.at[rows], osem.at[i])

    def finish(i, _):
        r = pl.multiple_of(i * BR, BR)
        f = out[pl.ds(r, BR)].astype(F32)
        out[pl.ds(r, BR)] = (mixed[pl.ds(r, BR)].astype(F32) + f * inverse_rms(2, r) * ffn_gain[...]).astype(BF16)
        out_copy(i).start()
        return 0

    lax.fori_loop(0, tok // BR, finish, 0, unroll=True)

    def sent(c):
        c.wait_send()

    for a in GATE + UP + DOWN:
        @pl.when(y != core)
        def _():
            seed_swap(a).wait_send()

        for j in range(nz):
            fan(a, origin[j], sent)
    for j in range(1, n):
        end_copy(j).wait_send()
    gather_sent(bview, bsend, brecv)
    to_plane(sent)
    for i in range(n):
        @pl.when(jnp.logical_not(owned(i)))
        def _():
            for h in range(2):
                p_copy(i, h).wait_send()
    for j in range(1, ntp):
        for q in range(3):
            tp_push(lambda o: ssq.at[q, o], qsend.at[q], qrecv.at[q], j, True).wait_send()
    for i in range(tok // BR):
        out_copy(i).wait()


def body(n, ntp, gate_branch, recur_input, doc_ids, conv_taps, gate_map, input_map, decay_level, decay_extra,
         out_weight, residual, mix_gain, pre_gain, ffn_gain, gate_weight, up_weight, down_weight):
    tok, loc = recur_input.shape
    dloc = residual.shape[1]
    krows, ff = gate_weight.shape
    ncol = down_weight.shape[1]
    heads, head, _ = gate_map.shape
    nz, ny = grid_of(n)
    planes = ny == 2 and tok % 128 == 0
    if planes:
        ids, taps, rate = doc_ids.reshape(tok // 128, 128), conv_taps, decay_level[None, :]
    else:
        ids = jnp.broadcast_to(doc_ids[:, None], (tok, 128))
        taps = conv_taps.astype(F32)
        rate = (GATE_POWER * -jax.nn.softplus(-decay_level))[None, :]
    args = (gate_branch, recur_input, ids, taps, gate_map.reshape(heads * head, head),
            input_map.reshape(heads * head, head), rate, decay_extra, out_weight, residual,
            mix_gain[None, :], pre_gain[None, :], ffn_gain[None, :], gate_weight, up_weight, down_weight)
    vm = pl.BlockSpec(memory_space=pltpu.VMEM)
    hbm = pl.BlockSpec(memory_space=pl.ANY)
    V, S = pltpu.VMEM, pltpu.SemaphoreType.DMA
    per = dloc // ncol
    chips = ntp // 2
    if planes:
        fn = plane_kernel
        in_specs = [hbm] * 2 + [vm] * 5 + [hbm] * 3 + [vm] * 3 + [hbm] * 3
        out_spec = hbm
        scratch = [
            V((tok, dloc), BF16), S((tok // math.gcd(tok, 128),)),
            V((tok, loc), BF16), V((tok, loc), BF16), V((tok, loc), F32), V(out_weight.shape, BF16), V((tok, dloc), BF16), S((5,)),
            V((n * krows, ff), BF16), V((n * krows, ff), BF16), V((n, ff, ncol), BF16),
            V((tok + 8, loc), F32), V((tok + 8, 128), jnp.int32), V((16, loc), BF16), V((tok // 128, 128), jnp.int32),
            V((2, loc, loc), BF16), V((tok, loc), F32), V((tok, loc), F32), V((n, 16, loc), F32),
            V((ntp, tok, loc), BF16), V((tok, dloc), BF16), V((tok, dloc), BF16), V((tok, dloc * ntp), BF16),
            V((tok, ff), F32), V((tok, ff), F32), V((tok, ff), BF16), V((n, tok, ncol), BF16), V((ny * chips, per, tok, ncol), BF16), V((3, ntp, 8, tok), F32),
            S((5,)), S((5,)), S((5,)), S((2, 5, nz)), S((5, nz)), S((5, nz)), S((5, nz)),
            S((2,)), S((2,)), S((n - 1,)), S((n - 1,)), S((ntp - 1,)), S((ntp - 1,)),
            S((ny, chips)), S((ntp,)), S((3, ntp - 1)), S((3, ntp - 1)), S((n, 2)), S((ny * chips, per, 2)),
        ]
    else:
        fn = kernel
        in_specs = [vm] * 13 + [hbm] * 3
        out_spec = vm
        scratch = [
            V((n * krows, ff), BF16), V((n * krows, ff), BF16), V((n, ff, ncol), BF16),
            V((tok + 8, loc), F32), V((tok + 8, 128), jnp.int32), V((16, loc), BF16), V((8, 128), jnp.int32),
            V((2, loc, loc), BF16), V((tok, loc), F32), V((tok, loc), F32), V((n, 16, loc), F32),
            V((ntp, tok, loc), BF16), V((tok, dloc), BF16), V((tok, dloc * ntp), BF16), V((tok, ff), BF16),
            V((n, tok, ncol), BF16), V((n, tok, ncol), BF16), V((chips - 1, per, tok, ncol), BF16), V((per, tok, ncol), BF16),
            V((3, ntp, 8, tok), F32),
            S((3, 2, n - 1)), S((3, 2, n - 1)), S((3,)), S((2,)), S((2,)), S((n - 1,)), S((n - 1,)),
            S((ntp - 1,)), S((ntp - 1,)), S((ntp - 1,)), S((ntp - 1,)), S((3, ntp - 1)), S((3, ntp - 1)),
            S((n,)), S((chips - 1, per)), S((n,)),
        ]
    return pl.pallas_call(
        functools.partial(fn, (n, ntp, nz, ny, dloc * ntp)),
        out_shape=jax.ShapeDtypeStruct((tok, dloc), BF16),
        in_specs=in_specs,
        out_specs=out_spec,
        scratch_shapes=scratch,
        compiler_params=pltpu.CompilerParams(
            collective_id=0, has_side_effects=True, vmem_limit_bytes=62 * 1024 * 1024),
    )(*args)


def solution(mesh):
    in_specs = (
        P("sp", "tp"), P("sp", "tp"), P("sp"), P(None, "tp"), P("tp", None, None), P("tp", None, None),
        P("tp"), P("sp", "tp"), P(None, "tp"), P("sp", "tp"), P("tp"), P("tp"), P("tp"),
        P("sp", "tp"), P("sp", "tp"), P("tp", "sp"),
    )
    fn = functools.partial(body, mesh.shape["sp"], mesh.shape["tp"])
    return jax.shard_map(fn, mesh=mesh, in_specs=in_specs, out_specs=P("sp", "tp"), check_vma=False)
```

```python
import functools
import math

import jax
import jax.numpy as jnp
from jax import lax
from jax.experimental import pallas as pl
from jax.experimental.pallas import tpu as pltpu
from jax.sharding import PartitionSpec as P

EPS = 1e-06
GATE_POWER = 8.0
F32 = jnp.float32
BF16 = jnp.bfloat16
MESH = pl.DeviceIdType.MESH


def grid_of(n):
    ny = 1
    for c in range(1, n + 1):
        if n % c == 0 and c * c <= n:
            ny = c
    return n // ny, ny


def ring_pos(s, nz, ny):
    z, y = lax.div(s, ny), lax.rem(s, ny)
    off = lax.div(y + ny - 1, ny)
    r = nz - 1 - z
    odd = lax.rem(r, 2)
    within = (1 - odd) * (y - 1) + odd * (ny - 1 - y)
    return (1 - off) * z + off * (nz + r * (ny - 1) + within)


def ring_dev(p, nz, ny):
    off = lax.div(lax.div(p, nz) + ny - 1, ny)
    q = off * (p - nz)
    r = lax.div(q, ny - 1)
    w = lax.rem(q, ny - 1)
    odd = lax.rem(r, 2)
    y = (1 - odd) * (1 + w) + odd * (ny - 1 - w)
    return (1 - off) * (p * ny) + off * ((nz - 1 - r) * ny + y)


def one_minus_exp(u):
    series = 1.0 + u * (1 / 8)
    for k in (7, 6, 5, 4, 3, 2):
        series = 1.0 + u * (1.0 / k) * series
    return jnp.where(u > -0.35, -u * series, 1.0 - jnp.exp(u))


def kernel(
    cfg,
    gate_branch, recur, ids, taps, gmap, imap, rate, extra, out_w, residual,
    mix_gain, pre_gain, ffn_gain, gate_w, up_w, down_w,
    out,
    gate_all, up_all, down_all, xpad, idpad, halo, ihalo, bd, fac, drv, ends, bfull,
    mixed, normed, hidden, partial, shared, recvd, own, ssq,
    wsend, wrecv, lsem, hsend, hrecv, esend, erecv, bsend, brecv, nsend, nrecv, qsend, qrecv, psend, precv, msem,
):
    n, ntp, nz, ny, width = cfg
    s, t = lax.axis_index("sp"), lax.axis_index("tp")
    tok, loc = recur.shape
    dloc = residual.shape[1]
    krows = gate_w.shape[0]
    ncol = down_w.shape[1]
    ff = gate_w.shape[1]
    CH = math.gcd(tok, 64)
    BR = math.gcd(tok, 128)
    pos = ring_pos(s, nz, ny)

    barrier = pltpu.get_barrier_semaphore()
    for j in range(1, n):
        pl.semaphore_signal(barrier, inc=1, device_id=(lax.rem(s + j, n), t), device_id_type=MESH)
    for j in range(1, ntp):
        pl.semaphore_signal(barrier, inc=1, device_id=(s, lax.rem(t + j, ntp)), device_id_type=MESH)
    pl.semaphore_wait(barrier, n - 1 + ntp - 1)

    shard = (gate_w, up_w, down_w)
    whole = (gate_all, up_all, down_all)
    nxt = [ring_dev(lax.rem(pos + 1, n), nz, ny), ring_dev(lax.rem(pos + n - 1, n), nz, ny)]
    origin = [[s] + [ring_dev(lax.rem(pos + (n - k if d == 0 else k), n), nz, ny) for k in range(1, n)] for d in range(2)]

    def half(a, o, d, local=False):
        if a < 2:
            h = krows // 2
            if local:
                return shard[a].at[pl.ds(d * h, h)]
            return whole[a].at[pl.ds(pl.multiple_of(o * krows + d * h, h), h)]
        h = ff // 2
        if local:
            return shard[a].at[pl.ds(d * h, h)]
        return whole[a].at[o, pl.ds(d * h, h)]

    def ring(a, d, k):
        o = origin[d][k]
        return pltpu.make_async_remote_copy(
            src_ref=half(a, o, d, k == 0), dst_ref=half(a, o, d),
            send_sem=wsend.at[a, d, k], recv_sem=wrecv.at[a, d, k],
            device_id=(nxt[d], t), device_id_type=MESH)

    def arrived(a, d, k):
        o = origin[d][k + 1]
        pltpu.make_async_remote_copy(
            src_ref=half(a, o, d), dst_ref=half(a, o, d),
            send_sem=wsend.at[a, d, k], recv_sem=wrecv.at[a, d, k],
            device_id=(nxt[d], t), device_id_type=MESH).wait_recv()

    def serve(arrays, k):
        for a in arrays:
            for d in range(2):
                arrived(a, d, k)
                if k < n - 2:
                    ring(a, d, k + 1).start()

    for a in range(3):
        for d in range(2):
            ring(a, d, 0).start()

    def halo_copy(i):
        src, dst = ((recur.at[pl.ds(tok - 16, 16)], halo), (ids.at[pl.ds(tok - 8, 8)], ihalo))[i]
        return pltpu.make_async_remote_copy(
            src_ref=src, dst_ref=dst, send_sem=hsend.at[i], recv_sem=hrecv.at[i],
            device_id=(lax.rem(s + 1, n), t), device_id_type=MESH)

    for i in range(2):
        halo_copy(i).start()

    def local_copy(a):
        if a < 2:
            dst = whole[a].at[pl.ds(pl.multiple_of(s * krows, krows), krows)]
        else:
            dst = whole[a].at[s]
        return pltpu.make_async_copy(shard[a], dst, lsem.at[a])

    for a in range(3):
        local_copy(a).start()

    head = gmap.shape[1]
    spread = (lax.rem(lax.broadcasted_iota(jnp.int32, (head, loc), 1), head)
              == lax.broadcasted_iota(jnp.int32, (head, loc), 0)).astype(BF16)
    diag = (lax.div(lax.broadcasted_iota(jnp.int32, (loc, loc), 0), head)
            == lax.div(lax.broadcasted_iota(jnp.int32, (loc, loc), 1), head))
    for i, m in enumerate((gmap, imap)):
        tiled = jnp.dot(m[...], spread, preferred_element_type=F32)
        bd[i] = jnp.where(diag, tiled, 0.0).astype(BF16)

    for i in range(2):
        halo_copy(i).wait()
    first = s == 0
    xpad[pl.ds(0, 8)] = halo[...].astype(F32)[8:16]
    idpad[pl.ds(0, 8)] = jnp.where(first, -1, ihalo[...])

    def fill(i, _):
        r = pl.multiple_of(i * CH, CH)
        xpad[pl.ds(pl.multiple_of(r + 8, 8), CH)] = recur[pl.ds(r, CH)].astype(F32)
        idpad[pl.ds(pl.multiple_of(r + 8, 8), CH)] = ids[pl.ds(r, CH)]
        return 0

    lax.fori_loop(0, tok // CH, fill, 0)
    reps = loc // 128
    ntaps = taps.shape[0]

    def front(i, _):
        r = pl.multiple_of(i * CH, CH)
        xw = xpad[pl.ds(r, CH + 8)]
        iw = idpad[pl.ds(r, CH + 8)]
        mine = iw[8:]
        tw = taps[...]
        conv = xw[8:] * tw[0:1]
        cont = None
        for k in range(1, ntaps):
            same1 = (pltpu.roll(iw, k, axis=0)[8:] == mine).astype(F32)
            same = jnp.concatenate([same1] * reps, axis=1)
            if k == 1:
                cont = same
            conv = conv + same * pltpu.roll(xw, k, axis=0)[8:] * tw[k:k + 1]
        cb = conv.astype(BF16)
        rg = jax.nn.sigmoid(jnp.dot(cb, bd[0], preferred_element_type=F32))
        ig = jax.nn.sigmoid(jnp.dot(cb, bd[1], preferred_element_type=F32))
        ld = rate[...] * rg + extra[pl.ds(r, CH)]
        fac[pl.ds(r, CH)] = jnp.exp(ld) * cont
        drv[pl.ds(r, CH)] = jnp.sqrt(one_minus_exp(2.0 * ld)) * ig * cb.astype(F32)
        return 0

    lax.fori_loop(0, tok // CH, front, 0)

    rows8 = lax.broadcasted_iota(jnp.int32, (8, loc), 0)

    def scan(i, carry):
        pc, hc = carry
        r = pl.multiple_of(i * 8, 8)
        a, b = fac[pl.ds(r, 8)], drv[pl.ds(r, 8)]
        for sh in (1, 2, 4):
            keep = rows8 >= sh
            b = b + a * jnp.where(keep, pltpu.roll(b, sh, axis=0), 0.0)
            a = a * jnp.where(keep, pltpu.roll(a, sh, axis=0), 1.0)
        h = b + a * hc
        p = a * pc
        fac[pl.ds(r, 8)] = p
        drv[pl.ds(r, 8)] = h
        return (jnp.broadcast_to(p[7:8], (8, loc)), jnp.broadcast_to(h[7:8], (8, loc)))

    pend, hend = lax.fori_loop(0, tok // 8, scan, (jnp.ones((8, loc), F32), jnp.zeros((8, loc), F32)))
    ends[s] = jnp.concatenate([pend, hend], axis=0)

    def end_copy(j):
        return pltpu.make_async_remote_copy(
            src_ref=ends.at[s], dst_ref=ends.at[s], send_sem=esend.at[j - 1], recv_sem=erecv.at[j - 1],
            device_id=(lax.rem(s + j, n), t), device_id_type=MESH)

    def end_arrived(j):
        o = lax.rem(s + n - j, n)
        pltpu.make_async_remote_copy(
            src_ref=ends.at[o], dst_ref=ends.at[o], send_sem=esend.at[j - 1], recv_sem=erecv.at[j - 1],
            device_id=(lax.rem(s + j, n), t), device_id_type=MESH).wait_recv()

    for j in range(1, n):
        end_copy(j).start()
    serve((0, 1), 0)
    for j in range(1, n):
        end_arrived(j)
    carry = jnp.zeros((8, loc), F32)
    for o in range(n - 1):
        e = ends[o]
        carry = jnp.where(o < s, e[:8] * carry + e[8:], carry)
    cin = carry[0:1]

    def branch(i, _):
        r = pl.multiple_of(i * CH, CH)
        st = drv[pl.ds(r, CH)] + fac[pl.ds(r, CH)] * cin
        bfull[t, pl.ds(r, CH)] = (st * jax.nn.gelu(gate_branch[pl.ds(r, CH)].astype(F32))).astype(BF16)
        return 0

    lax.fori_loop(0, tok // CH, branch, 0)

    def tp_push(view, send, recv, j, start):
        o = t if start else lax.rem(t + ntp - j, ntp)
        return pltpu.make_async_remote_copy(
            src_ref=view(o), dst_ref=view(o), send_sem=send.at[j - 1], recv_sem=recv.at[j - 1],
            device_id=(s, lax.rem(t + j, ntp)), device_id_type=MESH)

    def bview(o):
        return bfull.at[o]

    chips = ntp // 2
    core = lax.rem(t, 2)
    mate = t + 1 - 2 * core

    def far(view, send, recv, c, start):
        o = t if start else lax.rem(t + ntp - 2 * c, ntp)
        return pltpu.make_async_remote_copy(
            src_ref=view(o), dst_ref=view(o), send_sem=send.at[c - 1], recv_sem=recv.at[c - 1],
            device_id=(s, lax.rem(t + 2 * c, ntp)), device_id_type=MESH)

    def near(view, send, recv, c, start):
        base = t if start else mate
        o = lax.rem(base + ntp - 2 * c, ntp)
        return pltpu.make_async_remote_copy(
            src_ref=view(o), dst_ref=view(o), send_sem=send.at[chips - 1 + c], recv_sem=recv.at[chips - 1 + c],
            device_id=(s, mate), device_id_type=MESH)

    def gather_start(view, send, recv):
        for c in range(1, chips):
            far(view, send, recv, c, True).start()
        near(view, send, recv, 0, True).start()

    def gather_share(view, send, recv):
        for c in range(1, chips):
            far(view, send, recv, c, False).wait_recv()
            near(view, send, recv, c, True).start()

    def gather_wait(view, send, recv):
        for c in range(chips):
            near(view, send, recv, c, False).wait_recv()

    def gather_sent(view, send, recv):
        for c in range(1, chips):
            far(view, send, recv, c, True).wait_send()
        for c in range(chips):
            near(view, send, recv, c, True).wait_send()

    gather_start(bview, bsend, brecv)
    serve((0, 1), 1)
    gather_share(bview, bsend, brecv)
    gather_wait(bview, bsend, brecv)

    def row_total(q, values):
        def write(i, _):
            r = pl.multiple_of(i * BR, BR)
            v = values(r)
            c = jnp.sum(v * v, axis=1, keepdims=True)
            ssq[q, t, :, pl.ds(r, BR)] = jnp.transpose(jnp.broadcast_to(c, (BR, 128)))[:8]
            return 0

        lax.fori_loop(0, tok // BR, write, 0)
        for j in range(1, ntp):
            tp_push(lambda o: ssq.at[q, o], qsend.at[q], qrecv.at[q], j, True).start()

    def wait_total(q):
        for j in range(1, ntp):
            tp_push(lambda o: ssq.at[q, o], qsend.at[q], qrecv.at[q], j, False).wait_recv()

    def inverse_rms(q, r):
        row = ssq[q, 0, 0:1, pl.ds(r, BR)]
        for o in range(1, ntp):
            row = row + ssq[q, o, 0:1, pl.ds(r, BR)]
        inv = lax.rsqrt(row / width + EPS)
        return jnp.transpose(jnp.broadcast_to(inv, (128, BR)))[:, 0:1]

    def project(i, _):
        r = pl.multiple_of(i * BR, BR)
        total = jnp.zeros((BR, dloc), F32)
        for o in range(ntp):
            total += jnp.dot(bfull[o, pl.ds(r, BR)], out_w[pl.ds(o * loc, loc)], preferred_element_type=F32)
        mixed[pl.ds(r, BR)] = total.astype(BF16)
        return 0

    lax.fori_loop(0, tok // BR, project, 0)
    row_total(0, lambda r: mixed[pl.ds(r, BR)].astype(F32))
    wait_total(0)

    def stream(i, _):
        r = pl.multiple_of(i * BR, BR)
        m = mixed[pl.ds(r, BR)].astype(F32)
        mixed[pl.ds(r, BR)] = (residual[pl.ds(r, BR)].astype(F32) + m * inverse_rms(0, r) * mix_gain[...]).astype(BF16)
        return 0

    lax.fori_loop(0, tok // BR, stream, 0)
    row_total(1, lambda r: mixed[pl.ds(r, BR)].astype(F32))
    serve((0, 1), 2)
    wait_total(1)

    def norm(i, _):
        r = pl.multiple_of(i * BR, BR)
        m = mixed[pl.ds(r, BR)].astype(F32)
        normed[pl.ds(r, BR), pl.ds(pl.multiple_of(t * dloc, dloc), dloc)] = (m * inverse_rms(1, r) * pre_gain[...]).astype(BF16)
        return 0

    lax.fori_loop(0, tok // BR, norm, 0)

    def nview(o):
        return normed.at[:, pl.ds(pl.multiple_of(o * dloc, dloc), dloc)]

    gather_start(nview, nsend, nrecv)
    serve((0, 1), 3)
    gather_share(nview, nsend, nrecv)
    for k in range(4, n - 2):
        serve((0, 1), k)
    serve((2,), 0)
    serve((0, 1), n - 2)
    gather_wait(nview, nsend, nrecv)
    for a in range(3):
        local_copy(a).wait()

    def ffn_tile(c, size):
        cols = pl.ds(c, size)
        g = jnp.dot(normed[...], gate_all[:, cols], preferred_element_type=F32)
        u = jnp.dot(normed[...], up_all[:, cols], preferred_element_type=F32)
        hidden[:, cols] = (jax.nn.silu(g) * u).astype(BF16)

    TN = 256
    tiles = ff // TN

    def ffn_step(j, _):
        ffn_tile(pl.multiple_of(j * TN, TN), TN)
        return 0

    cut = (tiles + 1) // 2
    lax.fori_loop(0, cut, ffn_step, 0)
    serve((2,), 1)
    lax.fori_loop(cut, tiles, ffn_step, 0)
    if ff % TN:
        ffn_tile(tiles * TN, ff % TN)

    per = dloc // ncol

    def place(o):
        c = lax.div(o, per)
        w = lax.rem(o, per)
        gap = lax.rem(lax.div(c, 2) - lax.div(t, 2) + chips, chips)
        return lax.rem(c, 2), w, c, gap

    def mate_copy(i):
        return pltpu.make_async_remote_copy(
            src_ref=partial.at[i], dst_ref=shared.at[i], send_sem=psend.at[i], recv_sem=msem.at[i],
            device_id=(s, mate), device_id_type=MESH)

    def far_copy(i, w, c, gap):
        g = lax.rem(gap + chips - 1, chips)
        return pltpu.make_async_remote_copy(
            src_ref=partial.at[i], dst_ref=recvd.at[g, w], send_sem=psend.at[i], recv_sem=precv.at[g, w],
            device_id=(s, c), device_id_type=MESH)

    sent = []

    def down(*blocks):
        for o in blocks:
            i = len(sent)
            sent.append(o)
            partial[i] = jnp.dot(hidden[...], down_all[o], preferred_element_type=F32).astype(BF16)
            par, w, c, gap = place(o)

            @pl.when(par != core)
            def _():
                mate_copy(i).start()

    def join(i):
        par, w, c, gap = place(sent[i])

        @pl.when(par == core)
        def _():
            mate_copy(i).wait_recv()

            def add(b, _):
                r = pl.multiple_of(b * BR, BR)
                total = partial[i, pl.ds(r, BR)].astype(F32) + shared[i, pl.ds(r, BR)].astype(F32)
                partial[i, pl.ds(r, BR)] = total.astype(BF16)
                return 0

            lax.fori_loop(0, tok // BR, add, 0)

            @pl.when(gap == 0)
            def _():
                own[w] = partial[i]

            @pl.when(gap != 0)
            def _():
                far_copy(i, w, c, gap).start()

    down(s)
    joined = 0
    for k in range(2, n - 1):
        serve((2,), k)
        have = k + 1
        if 2 * have >= n:
            if 2 * have == n:
                down(origin[0][have])
            else:
                down(origin[0][have], origin[0][n - have])
        if k == n - 2:
            upto = len(sent)
        else:
            upto = len(sent) - (1 if 2 * have == n else 2) if 2 * have >= n else len(sent)
        while joined < upto:
            join(joined)
            joined += 1

    for i, o in enumerate(sent):
        par, w, c, gap = place(o)

        @pl.when(par != core)
        def _():
            mate_copy(i).wait_send()

        @pl.when(par == core)
        def _():
            @pl.when(gap != 0)
            def _():
                far_copy(i, w, c, gap).wait_send()

    for g in range(1, chips):
        for w in range(per):
            pltpu.make_async_remote_copy(
                src_ref=partial.at[0], dst_ref=recvd.at[g - 1, w],
                send_sem=psend.at[0], recv_sem=precv.at[g - 1, w],
                device_id=(s, mate), device_id_type=MESH).wait_recv()

    def gather_sum(i, _):
        r = pl.multiple_of(i * BR, BR)
        for w in range(per):
            total = own[w, pl.ds(r, BR)].astype(F32)
            for j in range(chips - 1):
                total = total + recvd[j, w, pl.ds(r, BR)].astype(F32)
            out[pl.ds(r, BR), pl.ds(w * ncol, ncol)] = total.astype(BF16)
        return 0

    lax.fori_loop(0, tok // BR, gather_sum, 0)
    row_total(2, lambda r: out[pl.ds(r, BR)].astype(F32))
    wait_total(2)

    def finish(i, _):
        r = pl.multiple_of(i * BR, BR)
        f = out[pl.ds(r, BR)].astype(F32)
        out[pl.ds(r, BR)] = (mixed[pl.ds(r, BR)].astype(F32) + f * inverse_rms(2, r) * ffn_gain[...]).astype(BF16)
        return 0

    lax.fori_loop(0, tok // BR, finish, 0)

    for a in range(3):
        for d in range(2):
            for k in range(n - 1):
                ring(a, d, k).wait_send()
    for j in range(1, n):
        end_copy(j).wait_send()
    gather_sent(bview, bsend, brecv)
    gather_sent(nview, nsend, nrecv)
    for j in range(1, ntp):
        for q in range(3):
            tp_push(lambda o: ssq.at[q, o], qsend.at[q], qrecv.at[q], j, True).wait_send()


def plane_kernel(
    cfg,
    gate_branch_in, recur_in, ids, taps, gmap, imap, level, extra_in, out_w_in, residual_in,
    mix_gain, pre_gain, ffn_gain, gate_w, up_w, down_w,
    out_hbm,
    out, osem, gate_branch, recur, extra, out_w, residual, insem,
    gate_all, up_all, down_all, xpad, idpad, halo, ihalo, bd, fac, drv, ends, bfull,
    mixed, nloc, gloc, normed, gnormed, ghid, gsum, usum, hidden, partial, recvd, ssq,
    lsem, ssend, srecv, zsend, zrecv, msend, mrecv,
    hsend, hrecv, esend, erecv, bsend, brecv, nsend, nrecv, fsend, frecv, gsend, grecv, qsend, qrecv, psend, precv,
):
    n, ntp, nz, ny, width = cfg
    s, t = lax.axis_index("sp"), lax.axis_index("tp")
    tok, loc = recur.shape
    dloc = residual.shape[1]
    krows = gate_w.shape[0]
    ncol = down_w.shape[1]
    ff = gate_w.shape[1]
    CH = math.gcd(tok, 64)
    BR = math.gcd(tok, 128)
    chips = ntp // 2
    z, y = lax.div(s, ny), lax.rem(s, ny)
    x, core = lax.div(t, 2), lax.rem(t, 2)
    mate = t + 1 - 2 * core
    per = dloc // ncol

    barrier = pltpu.get_barrier_semaphore()
    peers = [(z * ny + lax.rem(y + dy, ny), lax.rem(t + dt, ntp)) for dy in range(ny) for dt in range(ntp)][1:]
    peers += [(lax.rem(z + dz, nz) * ny + lax.rem(y + dy, ny), t) for dz in range(1, nz) for dy in range(ny)]
    for p in peers:
        pl.semaphore_signal(barrier, inc=1, device_id=p, device_id_type=MESH)

    inputs = ((recur_in, recur), (extra_in, extra), (gate_branch_in, gate_branch), (out_w_in, out_w), (residual_in, residual))

    def load_input(i):
        return pltpu.make_async_copy(inputs[i][0], inputs[i][1], insem.at[i])

    for i in range(len(inputs)):
        load_input(i).start()
    pl.semaphore_wait(barrier, len(peers))

    low = (2 * z < nz).astype(jnp.int32)
    near_first = []
    for k in range(1, nz):
        near_first += [z + (2 * low - 1) * k, z - (2 * low - 1) * k]
    origin = [z]
    seen = 0
    ranks = []
    for q in near_first:
        ok = jnp.logical_and(q >= 0, q < nz).astype(jnp.int32)
        seen = seen + ok
        ranks.append((q, ok, seen))
    for j in range(1, nz):
        origin.append(sum(jnp.where(jnp.logical_and(ok == 1, r == j), q, 0) for q, ok, r in ranks))

    hcol = ncol // 2
    hrow = krows // 2
    GATE, UP, DOWN, WIDE = (0, 1), (2,), (3, 4), (5, 6)
    fa = ff - ghid.shape[1]
    main, side = pl.ds(0, fa), pl.ds(fa, ff - fa)
    inner = jnp.logical_and(z > 0, z < nz - 1)
    host = jnp.logical_or(z == 1, z == nz - 2)
    guest_z = jnp.where(z == 1, 0, nz - 1)
    host_z = jnp.where(z == 0, 1, nz - 2)

    def block(a, o, b):
        i = o * ny + b
        if a in GATE:
            return gate_all.at[pl.ds(pl.multiple_of(i * krows + a * hrow, hrow), hrow), main]
        if a in UP:
            return up_all.at[pl.ds(pl.multiple_of(i * krows, krows), krows), main]
        if a in WIDE:
            return (gate_all, up_all)[a - WIDE[0]].at[pl.ds(pl.multiple_of(i * krows, krows), krows), side]
        return down_all.at[i, :, pl.ds((a - DOWN[0]) * hcol, hcol)]

    def own_shard(a):
        if a in GATE:
            return gate_w.at[pl.ds(a * hrow, hrow), main]
        if a in UP:
            return up_w.at[:, main]
        if a in WIDE:
            return (gate_w, up_w)[a - WIDE[0]].at[:, side]
        return down_w.at[:, pl.ds((a - DOWN[0]) * hcol, hcol)]

    def seed_local(a):
        return pltpu.make_async_copy(own_shard(a), block(a, z, y), lsem.at[a])

    def seed_swap(a):
        return pltpu.make_async_remote_copy(
            src_ref=own_shard(a), dst_ref=block(a, z, y), send_sem=ssend.at[a], recv_sem=srecv.at[a],
            device_id=(z * ny + 1 - y, mate), device_id_type=MESH)

    def z_copy(a, o, up):
        b = block(a, o, core)
        return pltpu.make_async_remote_copy(
            src_ref=b, dst_ref=b, send_sem=zsend.at[up, a, o], recv_sem=zrecv.at[a, o],
            device_id=((z + 2 * up - 1) * ny + y, t), device_id_type=MESH)

    def mate_copy(a, o, theirs=False):
        b = block(a, o, 1 - core if theirs else core)
        return pltpu.make_async_remote_copy(
            src_ref=b, dst_ref=b, send_sem=msend.at[a, o], recv_sem=mrecv.at[a, o],
            device_id=(s, mate), device_id_type=MESH)

    def fan_down(a, o, act):
        @pl.when(jnp.logical_and(o >= z, z > (1 if a in WIDE else 0)))
        def _():
            act(z_copy(a, o, 0))

    def fan_up(a, o, act):
        @pl.when(jnp.logical_and(o <= z, z < nz - (2 if a in WIDE else 1)))
        def _():
            act(z_copy(a, o, 1))

    def fan(a, o, act):
        fan_down(a, o, act)
        fan_up(a, o, act)
        if a in WIDE:
            @pl.when(inner)
            def _():
                act(mate_copy(a, o))
        else:
            act(mate_copy(a, o))

    def start(c):
        c.start()

    def seed_ready(a):
        @pl.when(y == core)
        def _():
            seed_local(a).wait()

        @pl.when(y != core)
        def _():
            pltpu.make_async_remote_copy(
                src_ref=block(a, z, core), dst_ref=block(a, z, core), send_sem=ssend.at[a], recv_sem=srecv.at[a],
                device_id=(z * ny + 1 - y, mate), device_id_type=MESH).wait_recv()

    def push_seed(a):
        seed_ready(a)
        fan(a, z, start)

    def relay_from(a, o):
        z_copy(a, o, 0).wait_recv()
        fan(a, o, start)

    def relay(items, j):
        for a in items:
            relay_from(a, origin[j])

    def load_seed(a):
        @pl.when(y == core)
        def _():
            seed_local(a).start()

        @pl.when(y != core)
        def _():
            seed_swap(a).start()

    def halo_copy(i):
        src, dst = ((recur_in.at[pl.ds(tok - 16, 16)], halo), (ids, ihalo))[i]
        return pltpu.make_async_remote_copy(
            src_ref=src, dst_ref=dst, send_sem=hsend.at[i], recv_sem=hrecv.at[i],
            device_id=(lax.rem(s + 1, n), t), device_id_type=MESH)

    for i in range(2):
        halo_copy(i).start()

    for a in GATE:
        load_seed(a)

    @pl.when(y == core)
    def _():
        for a in GATE:
            push_seed(a)

    head = gmap.shape[1]
    spread = (lax.rem(lax.broadcasted_iota(jnp.int32, (head, loc), 1), head)
              == lax.broadcasted_iota(jnp.int32, (head, loc), 0)).astype(BF16)
    diag = (lax.div(lax.broadcasted_iota(jnp.int32, (loc, loc), 0), head)
            == lax.div(lax.broadcasted_iota(jnp.int32, (loc, loc), 1), head))
    for i, m in enumerate((gmap, imap)):
        tiled = jnp.dot(m[...], spread, preferred_element_type=F32)
        bd[i] = jnp.where(diag, tiled, 0.0).astype(BF16)

    for i in range(2):
        load_input(i).wait()

    def down_rows(row):
        return jnp.transpose(jnp.broadcast_to(row, (128, 128)))

    for i in range(tok // 128):
        idpad[pl.ds(8 + i * 128, 128)] = down_rows(ids[i:i + 1])

    def fill(i, _):
        r = pl.multiple_of(i * CH, CH)
        xpad[pl.ds(pl.multiple_of(r + 8, 8), CH)] = recur[pl.ds(r, CH)].astype(F32)
        return 0

    lax.fori_loop(0, tok // CH, fill, 0)
    u = -level[...]
    rate = -GATE_POWER * (jnp.maximum(u, 0.0) + jnp.log1p(jnp.exp(-jnp.abs(u))))
    for i in range(2):
        halo_copy(i).wait()
    first = s == 0
    xpad[pl.ds(0, 8)] = halo[...].astype(F32)[8:16]
    idpad[pl.ds(0, 8)] = jnp.where(first, -1, down_rows(ihalo[tok // 128 - 1:tok // 128])[120:])
    reps = loc // 128
    ntaps = taps.shape[0]

    def front(i, _):
        r = pl.multiple_of(i * CH, CH)
        xw = xpad[pl.ds(r, CH + 8)]
        iw = idpad[pl.ds(r, CH + 8)]
        mine = iw[8:]
        tw = taps[...].astype(F32)
        conv = xw[8:] * tw[0:1]
        cont = None
        for k in range(1, ntaps):
            same1 = (pltpu.roll(iw, k, axis=0)[8:] == mine).astype(F32)
            same = jnp.concatenate([same1] * reps, axis=1)
            if k == 1:
                cont = same
            conv = conv + same * pltpu.roll(xw, k, axis=0)[8:] * tw[k:k + 1]
        cb = conv.astype(BF16)
        rg = jax.nn.sigmoid(jnp.dot(cb, bd[0], preferred_element_type=F32))
        ig = jax.nn.sigmoid(jnp.dot(cb, bd[1], preferred_element_type=F32))
        ld = rate * rg + extra[pl.ds(r, CH)]
        fac[pl.ds(r, CH)] = jnp.exp(ld) * cont
        drv[pl.ds(r, CH)] = jnp.sqrt(one_minus_exp(2.0 * ld)) * ig * cb.astype(F32)
        return 0

    lax.fori_loop(0, tok // CH, front, 0)

    @pl.when(y == core)
    def _():
        for a in UP + WIDE:
            load_seed(a)

    rows8 = lax.broadcasted_iota(jnp.int32, (8, loc), 0)

    def scan(i, carry):
        pc, hc = carry
        r = pl.multiple_of(i * 8, 8)
        a, b = fac[pl.ds(r, 8)], drv[pl.ds(r, 8)]
        for sh in (1, 2, 4):
            keep = rows8 >= sh
            b = b + a * jnp.where(keep, pltpu.roll(b, sh, axis=0), 0.0)
            a = a * jnp.where(keep, pltpu.roll(a, sh, axis=0), 1.0)
        h = b + a * hc
        p = a * pc
        fac[pl.ds(r, 8)] = p
        drv[pl.ds(r, 8)] = h
        return (jnp.broadcast_to(p[7:8], (8, loc)), jnp.broadcast_to(h[7:8], (8, loc)))

    pend, hend = lax.fori_loop(0, tok // 8, scan, (jnp.ones((8, loc), F32), jnp.zeros((8, loc), F32)))
    ends[s] = jnp.concatenate([pend, hend], axis=0)

    def end_copy(j):
        return pltpu.make_async_remote_copy(
            src_ref=ends.at[s], dst_ref=ends.at[s], send_sem=esend.at[j - 1], recv_sem=erecv.at[j - 1],
            device_id=(lax.rem(s + j, n), t), device_id_type=MESH)

    def end_arrived(j):
        o = lax.rem(s + n - j, n)
        pltpu.make_async_remote_copy(
            src_ref=ends.at[o], dst_ref=ends.at[o], send_sem=esend.at[j - 1], recv_sem=erecv.at[j - 1],
            device_id=(lax.rem(s + j, n), t), device_id_type=MESH).wait_recv()

    for j in range(1, n):
        end_copy(j).start()

    @pl.when(y != core)
    def _():
        for a in GATE:
            push_seed(a)
        for a in UP + WIDE:
            load_seed(a)

    for a in DOWN:
        load_seed(a)

    @pl.when(y == core)
    def _():
        for a in UP + WIDE:
            push_seed(a)

    early = min(2, nz - 1)
    for j in range(1, n):
        end_arrived(j)
    carry = jnp.zeros((8, loc), F32)
    for o in range(n - 1):
        e = ends[o]
        carry = jnp.where(o < s, e[:8] * carry + e[8:], carry)
    cin = carry[0:1]

    for i in range(2, len(inputs)):
        load_input(i).wait()

    def branch(i, _):
        r = pl.multiple_of(i * CH, CH)
        st = drv[pl.ds(r, CH)] + fac[pl.ds(r, CH)] * cin
        bfull[t, pl.ds(r, CH)] = (st * jax.nn.gelu(gate_branch[pl.ds(r, CH)].astype(F32))).astype(BF16)
        return 0

    lax.fori_loop(0, tok // CH, branch, 0)

    def tp_push(view, send, recv, j, start):
        o = t if start else lax.rem(t + ntp - j, ntp)
        return pltpu.make_async_remote_copy(
            src_ref=view(o), dst_ref=view(o), send_sem=send.at[j - 1], recv_sem=recv.at[j - 1],
            device_id=(s, lax.rem(t + j, ntp)), device_id_type=MESH)

    def bview(o):
        return bfull.at[o]

    chips = ntp // 2
    core = lax.rem(t, 2)
    mate = t + 1 - 2 * core

    def far(view, send, recv, c, start):
        o = t if start else lax.rem(t + ntp - 2 * c, ntp)
        return pltpu.make_async_remote_copy(
            src_ref=view(o), dst_ref=view(o), send_sem=send.at[c - 1], recv_sem=recv.at[c - 1],
            device_id=(s, lax.rem(t + 2 * c, ntp)), device_id_type=MESH)

    def near(view, send, recv, c, start):
        base = t if start else mate
        o = lax.rem(base + ntp - 2 * c, ntp)
        return pltpu.make_async_remote_copy(
            src_ref=view(o), dst_ref=view(o), send_sem=send.at[chips - 1 + c], recv_sem=recv.at[chips - 1 + c],
            device_id=(s, mate), device_id_type=MESH)

    def gather_start(view, send, recv):
        for c in range(1, chips):
            far(view, send, recv, c, True).start()
        near(view, send, recv, 0, True).start()

    def gather_share(view, send, recv):
        for c in range(1, chips):
            far(view, send, recv, c, False).wait_recv()
            near(view, send, recv, c, True).start()

    def gather_wait(view, send, recv):
        for c in range(chips):
            near(view, send, recv, c, False).wait_recv()

    def gather_sent(view, send, recv):
        for c in range(1, chips):
            far(view, send, recv, c, True).wait_send()
        for c in range(chips):
            near(view, send, recv, c, True).wait_send()

    gather_start(bview, bsend, brecv)

    @pl.when(y != core)
    def _():
        for a in UP + WIDE:
            push_seed(a)

    gather_share(bview, bsend, brecv)
    gather_wait(bview, bsend, brecv)

    def row_total(q, values):
        def write(i, _):
            r = pl.multiple_of(i * BR, BR)
            v = values(r)
            c = jnp.sum(v * v, axis=1, keepdims=True)
            ssq[q, t, :, pl.ds(r, BR)] = jnp.transpose(jnp.broadcast_to(c, (BR, 128)))[:8]
            return 0

        lax.fori_loop(0, tok // BR, write, 0, unroll=True)
        for j in range(1, ntp):
            tp_push(lambda o: ssq.at[q, o], qsend.at[q], qrecv.at[q], j, True).start()

    def wait_total(q):
        for j in range(1, ntp):
            tp_push(lambda o: ssq.at[q, o], qsend.at[q], qrecv.at[q], j, False).wait_recv()

    def inverse_rms(q, r):
        row = ssq[q, 0, 0:1, pl.ds(r, BR)]
        for o in range(1, ntp):
            row = row + ssq[q, o, 0:1, pl.ds(r, BR)]
        inv = lax.rsqrt(row / width + EPS)
        return jnp.transpose(jnp.broadcast_to(inv, (128, BR)))[:, 0:1]

    def project(i, _):
        r = pl.multiple_of(i * BR, BR)
        total = jnp.zeros((BR, dloc), F32)
        for o in range(ntp):
            total += jnp.dot(bfull[o, pl.ds(r, BR)], out_w[pl.ds(o * loc, loc)], preferred_element_type=F32)
        mixed[pl.ds(r, BR)] = total.astype(BF16)
        return 0

    lax.fori_loop(0, tok // BR, project, 0)
    row_total(0, lambda r: mixed[pl.ds(r, BR)].astype(F32))

    @pl.when(inner)
    def _():
        for j in range(1, early + 1):
            relay(GATE, j)

    wait_total(0)

    def stream(i, _):
        r = pl.multiple_of(i * BR, BR)
        m = mixed[pl.ds(r, BR)].astype(F32)
        mixed[pl.ds(r, BR)] = (residual[pl.ds(r, BR)].astype(F32) + m * inverse_rms(0, r) * mix_gain[...]).astype(BF16)
        return 0

    lax.fori_loop(0, tok // BR, stream, 0, unroll=True)
    row_total(1, lambda r: mixed[pl.ds(r, BR)].astype(F32))
    wait_total(1)

    cols = pl.ds(pl.multiple_of(t * dloc, dloc), dloc)

    def norm(i, _):
        r = pl.multiple_of(i * BR, BR)
        m = mixed[pl.ds(r, BR)].astype(F32)
        v = (m * inverse_rms(1, r) * pre_gain[...]).astype(BF16)
        nloc[pl.ds(r, BR)] = v

        @pl.when(y == core)
        def _():
            normed[pl.ds(r, BR), cols] = v

        return 0

    lax.fori_loop(0, tok // BR, norm, 0, unroll=True)
    htok = tok // 2
    piece, spot = (nloc, gloc), (normed, gnormed)

    def n_copy(q, dy, dx):
        return pltpu.make_async_remote_copy(
            src_ref=piece[q], dst_ref=spot[q].at[:, cols], send_sem=nsend.at[q, dy, dx], recv_sem=nrecv.at[q, t],
            device_id=(z * ny + lax.rem(y + dy, ny), 2 * lax.rem(x + dx, chips) + y), device_id_type=MESH)

    def to_plane(q, act):
        for dx in range(1, chips):
            act(n_copy(q, 0, dx))
        for dy in range(1, ny):
            act(n_copy(q, dy, 0))

        @pl.when(y != core)
        def _():
            act(n_copy(q, 0, 0))

    def n_wait(q, o):
        view = spot[q].at[:, pl.ds(pl.multiple_of(o * dloc, dloc), dloc)]
        pltpu.make_async_remote_copy(
            src_ref=view, dst_ref=view, send_sem=nsend.at[q, 0, 0], recv_sem=nrecv.at[q, o],
            device_id=(s, mate), device_id_type=MESH).wait_recv()

    def f_copy(q, o, h, device):
        view = spot[q].at[pl.ds(h * htok, htok), pl.ds(pl.multiple_of(o * dloc, dloc), dloc)]
        return pltpu.make_async_remote_copy(
            src_ref=view, dst_ref=view, send_sem=fsend.at[q, lax.rem(o, 2)], recv_sem=frecv.at[q, h, o],
            device_id=device, device_id_type=MESH)

    other = 1 - x

    def forward(q, act, wait):
        for e in range(2):
            @pl.when(y == core)
            def _():
                o = 2 * other + e
                if wait:
                    n_wait(q, o)
                act(f_copy(q, o, 0, (z * ny + 1 - y, t)))

            @pl.when(y != core)
            def _():
                o = 2 * x + e
                if wait:
                    n_wait(q, o)
                act(f_copy(q, o, 1, (s, 2 * other + core)))

    def n_ready(q):
        @pl.when(y == core)
        def _():
            n_wait(q, mate)

        @pl.when(y != core)
        def _():
            for e in range(2):
                for h in range(2):
                    f_copy(q, 2 * other + e, h, (s, mate)).wait_recv()

    def guest_hop():
        return pltpu.make_async_remote_copy(
            src_ref=nloc, dst_ref=gloc, send_sem=gsend.at[0], recv_sem=grecv.at[0],
            device_id=(host_z * ny + y, t), device_id_type=MESH)

    def guest_return():
        return pltpu.make_async_remote_copy(
            src_ref=ghid, dst_ref=hidden.at[:, side], send_sem=gsend.at[1], recv_sem=grecv.at[1],
            device_id=(guest_z * ny + y, t), device_id_type=MESH)

    to_plane(0, start)

    @pl.when(jnp.logical_not(inner))
    def _():
        guest_hop().start()
        for a in DOWN:
            push_seed(a)

    @pl.when(inner)
    def _():
        for j in range(1, early + 1):
            relay(UP, j)
            relay(WIDE, j)

    forward(0, start, True)

    @pl.when(host)
    def _():
        guest_hop().wait_recv()

        @pl.when(y == core)
        def _():
            gnormed[:, cols] = gloc[...]

        to_plane(1, start)

    @pl.when(jnp.logical_not(inner))
    def _():
        for j in range(1, early + 1):
            relay(GATE, j)
            relay(UP, j)

    def outward_seed(items):
        for a in items:
            @pl.when(low == 1)
            def _():
                fan_down(a, z, start)

            @pl.when(low == 0)
            def _():
                fan_up(a, z, start)

    def mates(items, js):
        for j in js:
            for a in items:
                mate_copy(a, origin[j], True).wait_recv()

    kblk = ny * krows
    TN = 256
    def sums(js, cs):
        g = u = None
        for j in js:
            k = pl.ds(pl.multiple_of(origin[j] * kblk, kblk), kblk)
            a = normed[:, k]
            gj = jnp.dot(a, gate_all[k, cs], preferred_element_type=F32)
            uj = jnp.dot(a, up_all[k, cs], preferred_element_type=F32)
            g, u = (gj, uj) if g is None else (g + gj, u + uj)
        return g, u

    def first_tile(c, size):
        cs = pl.ds(c, size)
        gsum[:, cs], usum[:, cs] = sums(range(nz - 1), cs)

    def last_tile(c, size):
        cs = pl.ds(c, size)
        g, u = sums((nz - 1,), cs)
        g, u = g + gsum[:, cs], u + usum[:, cs]
        hidden[:, cs] = (jax.nn.silu(g) * u).astype(BF16)

    def over_tiles(tile):
        def step(j, _):
            tile(pl.multiple_of(j * TN, TN), TN)
            return 0

        lax.fori_loop(0, fa // TN, step, 0)
        if fa % TN:
            tile(fa // TN * TN, fa % TN)

        @pl.when(inner)
        def _():
            tile(fa, ff - fa)

    @pl.when(inner)
    def _():
        for j in range(early + 1, nz):
            relay(GATE, j)
            relay(UP, j)
            relay(WIDE, j)
        for a in DOWN:
            seed_ready(a)
            mate_copy(a, z).start()

            @pl.when(low == 1)
            def _():
                fan_up(a, z, start)

            @pl.when(low == 0)
            def _():
                fan_down(a, z, start)

        outward_seed(DOWN[:1])
        relay(DOWN, 2)

    n_ready(0)
    mates(GATE + UP, range(nz - 1))

    @pl.when(inner)
    def _():
        mates(WIDE, range(nz - 1))

    over_tiles(first_tile)

    @pl.when(host)
    def _():
        forward(1, start, True)

    @pl.when(jnp.logical_not(inner))
    def _():
        for j in range(early + 1, nz):
            relay(GATE, j)
            relay(UP, j)

    mates(GATE + UP, (nz - 1,))

    @pl.when(inner)
    def _():
        mates(WIDE, (nz - 1,))

    over_tiles(last_tile)

    @pl.when(host)
    def _():
        n_ready(1)
        g = jnp.dot(gnormed[...], gate_all[:, side], preferred_element_type=F32)
        v = jnp.dot(gnormed[...], up_all[:, side], preferred_element_type=F32)
        ghid[...] = (jax.nn.silu(g) * v).astype(BF16)
        guest_return().start()

    @pl.when(jnp.logical_not(inner))
    def _():
        guest_return().wait_recv()

    me = y * chips + x

    def p_copy(i, h):
        c = pl.ds(h * hcol, hcol)
        return pltpu.make_async_remote_copy(
            src_ref=partial.at[i, :, c], dst_ref=recvd.at[me, lax.rem(i, per), :, c], send_sem=psend.at[i, h],
            recv_sem=precv.at[me, lax.rem(i, per), h],
            device_id=(z * ny + core, lax.div(i, per)), device_id_type=MESH)

    def owned(i):
        return jnp.logical_and(y == core, lax.div(i, per) == t)

    def ship(i, hs):
        @pl.when(owned(i))
        def _():
            for h in hs:
                c = pl.ds(h * hcol, hcol)
                recvd[me, lax.rem(i, per), :, c] = partial[i, :, c]

        @pl.when(jnp.logical_not(owned(i)))
        def _():
            for h in hs:
                p_copy(i, h).start()

    def mate_ready(a, o, b):
        @pl.when(b != core)
        def _():
            mate_copy(a, o, True).wait_recv()

    def order(b, j):
        if j == 0:
            return origin[j]
        line = origin[2:3] + (origin[1:2] + origin[3:] if b == 0 else origin[3:] + origin[1:2])
        return jnp.where(inner, origin[j], line[j - 1])

    for j in range(nz):
        mine = jnp.where(core == 0, order(0, j), order(1, j))
        if j < nz - 1:
            if j == 2:
                @pl.when(jnp.logical_not(inner))
                def _():
                    for a in DOWN:
                        relay_from(a, mine)
            elif j:
                for a in DOWN:
                    relay_from(a, mine)
            if j == 1:
                @pl.when(jnp.logical_and(inner, core == 0))
                def _():
                    outward_seed(DOWN[1:])

            for b in range(ny):
                i = order(b, j) * ny + b
                for a in DOWN:
                    mate_ready(a, order(b, j), b)
                partial[i] = jnp.dot(hidden[...], down_all[i], preferred_element_type=F32).astype(BF16)
                ship(i, (0, 1))
        else:
            for h in range(2):
                relay_from(DOWN[h], mine)
                if h == 1:
                    @pl.when(jnp.logical_and(inner, core == 1))
                    def _():
                        outward_seed(DOWN[1:])

                c = pl.ds(h * hcol, hcol)
                for b in range(ny):
                    i = order(b, j) * ny + b
                    mate_ready(DOWN[h], order(b, j), b)
                    partial[i, :, c] = jnp.dot(hidden[...], down_all[i, :, c], preferred_element_type=F32).astype(BF16)
                    ship(i, (h,))

    def p_wait(dy, dx):
        k = lax.rem(y + dy, ny) * chips + lax.rem(x + dx, chips)
        for w in range(per):
            for h in range(2):
                view = recvd.at[k, w, :, pl.ds(h * hcol, hcol)]
                pltpu.make_async_remote_copy(
                    src_ref=view, dst_ref=view, send_sem=psend.at[0, 0], recv_sem=precv.at[k, w, h],
                    device_id=(s, mate), device_id_type=MESH).wait_recv()

    for dy in range(ny):
        for dx in range(chips):
            if dy or dx:
                p_wait(dy, dx)

    @pl.when(y != core)
    def _():
        p_wait(0, 0)

    def ffn_rows(r):
        for w in range(per):
            total = recvd[0, w, pl.ds(r, BR)].astype(F32)
            for k in range(1, ny * chips):
                total = total + recvd[k, w, pl.ds(r, BR)].astype(F32)
            out[pl.ds(r, BR), pl.ds(w * ncol, ncol)] = total.astype(BF16)
        return out[pl.ds(r, BR)].astype(F32)

    row_total(2, ffn_rows)
    wait_total(2)

    def out_copy(i):
        rows = pl.ds(pl.multiple_of(i * BR, BR), BR)
        return pltpu.make_async_copy(out.at[rows], out_hbm.at[rows], osem.at[i])

    def finish(i, _):
        r = pl.multiple_of(i * BR, BR)
        f = out[pl.ds(r, BR)].astype(F32)
        out[pl.ds(r, BR)] = (mixed[pl.ds(r, BR)].astype(F32) + f * inverse_rms(2, r) * ffn_gain[...]).astype(BF16)
        out_copy(i).start()
        return 0

    lax.fori_loop(0, tok // BR, finish, 0, unroll=True)

    def sent(c):
        c.wait_send()

    for a in GATE + UP + DOWN + WIDE:
        @pl.when(y != core)
        def _():
            seed_swap(a).wait_send()

        for j in range(nz):
            fan(a, origin[j], sent)
    for j in range(1, n):
        end_copy(j).wait_send()
    gather_sent(bview, bsend, brecv)
    to_plane(0, sent)
    forward(0, sent, False)

    @pl.when(host)
    def _():
        to_plane(1, sent)
        forward(1, sent, False)
        guest_return().wait_send()

    @pl.when(jnp.logical_not(inner))
    def _():
        guest_hop().wait_send()

    for i in range(n):
        @pl.when(jnp.logical_not(owned(i)))
        def _():
            for h in range(2):
                p_copy(i, h).wait_send()
    for j in range(1, ntp):
        for q in range(3):
            tp_push(lambda o: ssq.at[q, o], qsend.at[q], qrecv.at[q], j, True).wait_send()
    for i in range(tok // BR):
        out_copy(i).wait()


def body(n, ntp, gate_branch, recur_input, doc_ids, conv_taps, gate_map, input_map, decay_level, decay_extra,
         out_weight, residual, mix_gain, pre_gain, ffn_gain, gate_weight, up_weight, down_weight):
    tok, loc = recur_input.shape
    dloc = residual.shape[1]
    krows, ff = gate_weight.shape
    ncol = down_weight.shape[1]
    heads, head, _ = gate_map.shape
    nz, ny = grid_of(n)
    planes = ny == 2 and nz > 3 and ntp == 4 and tok % 256 == 0 and ff % 128 == 0
    fb = ff // 128 * 2 // 11 * 128
    if planes:
        ids, taps, rate = doc_ids.reshape(tok // 128, 128), conv_taps, decay_level[None, :]
    else:
        ids = jnp.broadcast_to(doc_ids[:, None], (tok, 128))
        taps = conv_taps.astype(F32)
        rate = (GATE_POWER * -jax.nn.softplus(-decay_level))[None, :]
    args = (gate_branch, recur_input, ids, taps, gate_map.reshape(heads * head, head),
            input_map.reshape(heads * head, head), rate, decay_extra, out_weight, residual,
            mix_gain[None, :], pre_gain[None, :], ffn_gain[None, :], gate_weight, up_weight, down_weight)
    vm = pl.BlockSpec(memory_space=pltpu.VMEM)
    hbm = pl.BlockSpec(memory_space=pl.ANY)
    V, S = pltpu.VMEM, pltpu.SemaphoreType.DMA
    per = dloc // ncol
    chips = ntp // 2
    if planes:
        fn = plane_kernel
        in_specs = [hbm] * 2 + [vm] * 5 + [hbm] * 3 + [vm] * 3 + [hbm] * 3
        out_spec = hbm
        scratch = [
            V((tok, dloc), BF16), S((tok // math.gcd(tok, 128),)),
            V((tok, loc), BF16), V((tok, loc), BF16), V((tok, loc), F32), V(out_weight.shape, BF16), V((tok, dloc), BF16), S((5,)),
            V((n * krows, ff), BF16), V((n * krows, ff), BF16), V((n, ff, ncol), BF16),
            V((tok + 8, loc), F32), V((tok + 8, 128), jnp.int32), V((16, loc), BF16), V((tok // 128, 128), jnp.int32),
            V((2, loc, loc), BF16), V((tok, loc), F32), V((tok, loc), F32), V((n, 16, loc), F32),
            V((ntp, tok, loc), BF16), V((tok, dloc), BF16), V((tok, dloc), BF16), V((tok, dloc), BF16), V((tok, dloc * ntp), BF16),
            V((tok, dloc * ntp), BF16), V((tok, fb), BF16), V((tok, ff), F32), V((tok, ff), F32), V((tok, ff), BF16), V((n, tok, ncol), BF16), V((ny * chips, per, tok, ncol), BF16), V((3, ntp, 8, tok), F32),
            S((7,)), S((7,)), S((7,)), S((2, 7, nz)), S((7, nz)), S((7, nz)), S((7, nz)),
            S((2,)), S((2,)), S((n - 1,)), S((n - 1,)), S((ntp - 1,)), S((ntp - 1,)),
            S((2, ny, chips)), S((2, ntp)), S((2, 2)), S((2, 2, ntp)), S((2,)), S((2,)), S((3, ntp - 1)), S((3, ntp - 1)), S((n, 2)), S((ny * chips, per, 2)),
        ]
    else:
        fn = kernel
        in_specs = [vm] * 13 + [hbm] * 3
        out_spec = vm
        scratch = [
            V((n * krows, ff), BF16), V((n * krows, ff), BF16), V((n, ff, ncol), BF16),
            V((tok + 8, loc), F32), V((tok + 8, 128), jnp.int32), V((16, loc), BF16), V((8, 128), jnp.int32),
            V((2, loc, loc), BF16), V((tok, loc), F32), V((tok, loc), F32), V((n, 16, loc), F32),
            V((ntp, tok, loc), BF16), V((tok, dloc), BF16), V((tok, dloc * ntp), BF16), V((tok, ff), BF16),
            V((n, tok, ncol), BF16), V((n, tok, ncol), BF16), V((chips - 1, per, tok, ncol), BF16), V((per, tok, ncol), BF16),
            V((3, ntp, 8, tok), F32),
            S((3, 2, n - 1)), S((3, 2, n - 1)), S((3,)), S((2,)), S((2,)), S((n - 1,)), S((n - 1,)),
            S((ntp - 1,)), S((ntp - 1,)), S((ntp - 1,)), S((ntp - 1,)), S((3, ntp - 1)), S((3, ntp - 1)),
            S((n,)), S((chips - 1, per)), S((n,)),
        ]
    return pl.pallas_call(
        functools.partial(fn, (n, ntp, nz, ny, dloc * ntp)),
        out_shape=jax.ShapeDtypeStruct((tok, dloc), BF16),
        in_specs=in_specs,
        out_specs=out_spec,
        scratch_shapes=scratch,
        compiler_params=pltpu.CompilerParams(
            collective_id=0, has_side_effects=True, vmem_limit_bytes=62 * 1024 * 1024),
    )(*args)


def solution(mesh):
    in_specs = (
        P("sp", "tp"), P("sp", "tp"), P("sp"), P(None, "tp"), P("tp", None, None), P("tp", None, None),
        P("tp"), P("sp", "tp"), P(None, "tp"), P("sp", "tp"), P("tp"), P("tp"), P("tp"),
        P("sp", "tp"), P("sp", "tp"), P("tp", "sp"),
    )
    fn = functools.partial(body, mesh.shape["sp"], mesh.shape["tp"])
    return jax.shard_map(fn, mesh=mesh, in_specs=in_specs, out_specs=P("sp", "tp"), check_vma=False)
```

```python
import functools
import math

import jax
import jax.numpy as jnp
from jax import lax
from jax.experimental import pallas as pl
from jax.experimental.pallas import tpu as pltpu
from jax.sharding import PartitionSpec as P

EPS = 1e-06
GATE_POWER = 8.0
F32 = jnp.float32
BF16 = jnp.bfloat16
MESH = pl.DeviceIdType.MESH


def grid_of(n):
    ny = 1
    for c in range(1, n + 1):
        if n % c == 0 and c * c <= n:
            ny = c
    return n // ny, ny


def ring_pos(s, nz, ny):
    z, y = lax.div(s, ny), lax.rem(s, ny)
    off = lax.div(y + ny - 1, ny)
    r = nz - 1 - z
    odd = lax.rem(r, 2)
    within = (1 - odd) * (y - 1) + odd * (ny - 1 - y)
    return (1 - off) * z + off * (nz + r * (ny - 1) + within)


def ring_dev(p, nz, ny):
    off = lax.div(lax.div(p, nz) + ny - 1, ny)
    q = off * (p - nz)
    r = lax.div(q, ny - 1)
    w = lax.rem(q, ny - 1)
    odd = lax.rem(r, 2)
    y = (1 - odd) * (1 + w) + odd * (ny - 1 - w)
    return (1 - off) * (p * ny) + off * ((nz - 1 - r) * ny + y)


def one_minus_exp(u):
    series = 1.0 + u * (1 / 8)
    for k in (7, 6, 5, 4, 3, 2):
        series = 1.0 + u * (1.0 / k) * series
    return jnp.where(u > -0.35, -u * series, 1.0 - jnp.exp(u))


def kernel(
    cfg,
    gate_branch, recur, ids, taps, gmap, imap, rate, extra, out_w, residual,
    mix_gain, pre_gain, ffn_gain, gate_w, up_w, down_w,
    out,
    gate_all, up_all, down_all, xpad, idpad, halo, ihalo, bd, fac, drv, ends, bfull,
    mixed, normed, hidden, partial, shared, recvd, own, ssq,
    wsend, wrecv, lsem, hsend, hrecv, esend, erecv, bsend, brecv, nsend, nrecv, qsend, qrecv, psend, precv, msem,
):
    n, ntp, nz, ny, width = cfg
    s, t = lax.axis_index("sp"), lax.axis_index("tp")
    tok, loc = recur.shape
    dloc = residual.shape[1]
    krows = gate_w.shape[0]
    ncol = down_w.shape[1]
    ff = gate_w.shape[1]
    CH = math.gcd(tok, 64)
    BR = math.gcd(tok, 128)
    pos = ring_pos(s, nz, ny)

    barrier = pltpu.get_barrier_semaphore()
    for j in range(1, n):
        pl.semaphore_signal(barrier, inc=1, device_id=(lax.rem(s + j, n), t), device_id_type=MESH)
    for j in range(1, ntp):
        pl.semaphore_signal(barrier, inc=1, device_id=(s, lax.rem(t + j, ntp)), device_id_type=MESH)
    pl.semaphore_wait(barrier, n - 1 + ntp - 1)

    shard = (gate_w, up_w, down_w)
    whole = (gate_all, up_all, down_all)
    nxt = [ring_dev(lax.rem(pos + 1, n), nz, ny), ring_dev(lax.rem(pos + n - 1, n), nz, ny)]
    origin = [[s] + [ring_dev(lax.rem(pos + (n - k if d == 0 else k), n), nz, ny) for k in range(1, n)] for d in range(2)]

    def half(a, o, d, local=False):
        if a < 2:
            h = krows // 2
            if local:
                return shard[a].at[pl.ds(d * h, h)]
            return whole[a].at[pl.ds(pl.multiple_of(o * krows + d * h, h), h)]
        h = ff // 2
        if local:
            return shard[a].at[pl.ds(d * h, h)]
        return whole[a].at[o, pl.ds(d * h, h)]

    def ring(a, d, k):
        o = origin[d][k]
        return pltpu.make_async_remote_copy(
            src_ref=half(a, o, d, k == 0), dst_ref=half(a, o, d),
            send_sem=wsend.at[a, d, k], recv_sem=wrecv.at[a, d, k],
            device_id=(nxt[d], t), device_id_type=MESH)

    def arrived(a, d, k):
        o = origin[d][k + 1]
        pltpu.make_async_remote_copy(
            src_ref=half(a, o, d), dst_ref=half(a, o, d),
            send_sem=wsend.at[a, d, k], recv_sem=wrecv.at[a, d, k],
            device_id=(nxt[d], t), device_id_type=MESH).wait_recv()

    def serve(arrays, k):
        for a in arrays:
            for d in range(2):
                arrived(a, d, k)
                if k < n - 2:
                    ring(a, d, k + 1).start()

    for a in range(3):
        for d in range(2):
            ring(a, d, 0).start()

    def halo_copy(i):
        src, dst = ((recur.at[pl.ds(tok - 16, 16)], halo), (ids.at[pl.ds(tok - 8, 8)], ihalo))[i]
        return pltpu.make_async_remote_copy(
            src_ref=src, dst_ref=dst, send_sem=hsend.at[i], recv_sem=hrecv.at[i],
            device_id=(lax.rem(s + 1, n), t), device_id_type=MESH)

    for i in range(2):
        halo_copy(i).start()

    def local_copy(a):
        if a < 2:
            dst = whole[a].at[pl.ds(pl.multiple_of(s * krows, krows), krows)]
        else:
            dst = whole[a].at[s]
        return pltpu.make_async_copy(shard[a], dst, lsem.at[a])

    for a in range(3):
        local_copy(a).start()

    head = gmap.shape[1]
    spread = (lax.rem(lax.broadcasted_iota(jnp.int32, (head, loc), 1), head)
              == lax.broadcasted_iota(jnp.int32, (head, loc), 0)).astype(BF16)
    diag = (lax.div(lax.broadcasted_iota(jnp.int32, (loc, loc), 0), head)
            == lax.div(lax.broadcasted_iota(jnp.int32, (loc, loc), 1), head))
    for i, m in enumerate((gmap, imap)):
        tiled = jnp.dot(m[...], spread, preferred_element_type=F32)
        bd[i] = jnp.where(diag, tiled, 0.0).astype(BF16)

    for i in range(2):
        halo_copy(i).wait()
    first = s == 0
    xpad[pl.ds(0, 8)] = halo[...].astype(F32)[8:16]
    idpad[pl.ds(0, 8)] = jnp.where(first, -1, ihalo[...])

    def fill(i, _):
        r = pl.multiple_of(i * CH, CH)
        xpad[pl.ds(pl.multiple_of(r + 8, 8), CH)] = recur[pl.ds(r, CH)].astype(F32)
        idpad[pl.ds(pl.multiple_of(r + 8, 8), CH)] = ids[pl.ds(r, CH)]
        return 0

    lax.fori_loop(0, tok // CH, fill, 0)
    reps = loc // 128
    ntaps = taps.shape[0]

    def front(i, _):
        r = pl.multiple_of(i * CH, CH)
        xw = xpad[pl.ds(r, CH + 8)]
        iw = idpad[pl.ds(r, CH + 8)]
        mine = iw[8:]
        tw = taps[...]
        conv = xw[8:] * tw[0:1]
        cont = None
        for k in range(1, ntaps):
            same1 = (pltpu.roll(iw, k, axis=0)[8:] == mine).astype(F32)
            same = jnp.concatenate([same1] * reps, axis=1)
            if k == 1:
                cont = same
            conv = conv + same * pltpu.roll(xw, k, axis=0)[8:] * tw[k:k + 1]
        cb = conv.astype(BF16)
        rg = jax.nn.sigmoid(jnp.dot(cb, bd[0], preferred_element_type=F32))
        ig = jax.nn.sigmoid(jnp.dot(cb, bd[1], preferred_element_type=F32))
        ld = rate[...] * rg + extra[pl.ds(r, CH)]
        fac[pl.ds(r, CH)] = jnp.exp(ld) * cont
        drv[pl.ds(r, CH)] = jnp.sqrt(one_minus_exp(2.0 * ld)) * ig * cb.astype(F32)
        return 0

    lax.fori_loop(0, tok // CH, front, 0)

    rows8 = lax.broadcasted_iota(jnp.int32, (8, loc), 0)

    def scan(i, carry):
        pc, hc = carry
        r = pl.multiple_of(i * 8, 8)
        a, b = fac[pl.ds(r, 8)], drv[pl.ds(r, 8)]
        for sh in (1, 2, 4):
            keep = rows8 >= sh
            b = b + a * jnp.where(keep, pltpu.roll(b, sh, axis=0), 0.0)
            a = a * jnp.where(keep, pltpu.roll(a, sh, axis=0), 1.0)
        h = b + a * hc
        p = a * pc
        fac[pl.ds(r, 8)] = p
        drv[pl.ds(r, 8)] = h
        return (jnp.broadcast_to(p[7:8], (8, loc)), jnp.broadcast_to(h[7:8], (8, loc)))

    pend, hend = lax.fori_loop(0, tok // 8, scan, (jnp.ones((8, loc), F32), jnp.zeros((8, loc), F32)))
    ends[s] = jnp.concatenate([pend, hend], axis=0)

    def end_copy(j):
        return pltpu.make_async_remote_copy(
            src_ref=ends.at[s], dst_ref=ends.at[s], send_sem=esend.at[j - 1], recv_sem=erecv.at[j - 1],
            device_id=(lax.rem(s + j, n), t), device_id_type=MESH)

    def end_arrived(j):
        o = lax.rem(s + n - j, n)
        pltpu.make_async_remote_copy(
            src_ref=ends.at[o], dst_ref=ends.at[o], send_sem=esend.at[j - 1], recv_sem=erecv.at[j - 1],
            device_id=(lax.rem(s + j, n), t), device_id_type=MESH).wait_recv()

    for j in range(1, n):
        end_copy(j).start()
    serve((0, 1), 0)
    for j in range(1, n):
        end_arrived(j)
    carry = jnp.zeros((8, loc), F32)
    for o in range(n - 1):
        e = ends[o]
        carry = jnp.where(o < s, e[:8] * carry + e[8:], carry)
    cin = carry[0:1]

    def branch(i, _):
        r = pl.multiple_of(i * CH, CH)
        st = drv[pl.ds(r, CH)] + fac[pl.ds(r, CH)] * cin
        bfull[t, pl.ds(r, CH)] = (st * jax.nn.gelu(gate_branch[pl.ds(r, CH)].astype(F32))).astype(BF16)
        return 0

    lax.fori_loop(0, tok // CH, branch, 0)

    def tp_push(view, send, recv, j, start):
        o = t if start else lax.rem(t + ntp - j, ntp)
        return pltpu.make_async_remote_copy(
            src_ref=view(o), dst_ref=view(o), send_sem=send.at[j - 1], recv_sem=recv.at[j - 1],
            device_id=(s, lax.rem(t + j, ntp)), device_id_type=MESH)

    def bview(o):
        return bfull.at[o]

    chips = ntp // 2
    core = lax.rem(t, 2)
    mate = t + 1 - 2 * core

    def far(view, send, recv, c, start):
        o = t if start else lax.rem(t + ntp - 2 * c, ntp)
        return pltpu.make_async_remote_copy(
            src_ref=view(o), dst_ref=view(o), send_sem=send.at[c - 1], recv_sem=recv.at[c - 1],
            device_id=(s, lax.rem(t + 2 * c, ntp)), device_id_type=MESH)

    def near(view, send, recv, c, start):
        base = t if start else mate
        o = lax.rem(base + ntp - 2 * c, ntp)
        return pltpu.make_async_remote_copy(
            src_ref=view(o), dst_ref=view(o), send_sem=send.at[chips - 1 + c], recv_sem=recv.at[chips - 1 + c],
            device_id=(s, mate), device_id_type=MESH)

    def gather_start(view, send, recv):
        for c in range(1, chips):
            far(view, send, recv, c, True).start()
        near(view, send, recv, 0, True).start()

    def gather_share(view, send, recv):
        for c in range(1, chips):
            far(view, send, recv, c, False).wait_recv()
            near(view, send, recv, c, True).start()

    def gather_wait(view, send, recv):
        for c in range(chips):
            near(view, send, recv, c, False).wait_recv()

    def gather_sent(view, send, recv):
        for c in range(1, chips):
            far(view, send, recv, c, True).wait_send()
        for c in range(chips):
            near(view, send, recv, c, True).wait_send()

    gather_start(bview, bsend, brecv)
    serve((0, 1), 1)
    gather_share(bview, bsend, brecv)
    gather_wait(bview, bsend, brecv)

    def row_total(q, values):
        def write(i, _):
            r = pl.multiple_of(i * BR, BR)
            v = values(r)
            c = jnp.sum(v * v, axis=1, keepdims=True)
            ssq[q, t, :, pl.ds(r, BR)] = jnp.transpose(jnp.broadcast_to(c, (BR, 128)))[:8]
            return 0

        lax.fori_loop(0, tok // BR, write, 0)
        for j in range(1, ntp):
            tp_push(lambda o: ssq.at[q, o], qsend.at[q], qrecv.at[q], j, True).start()

    def wait_total(q):
        for j in range(1, ntp):
            tp_push(lambda o: ssq.at[q, o], qsend.at[q], qrecv.at[q], j, False).wait_recv()

    def inverse_rms(q, r):
        row = ssq[q, 0, 0:1, pl.ds(r, BR)]
        for o in range(1, ntp):
            row = row + ssq[q, o, 0:1, pl.ds(r, BR)]
        inv = lax.rsqrt(row / width + EPS)
        return jnp.transpose(jnp.broadcast_to(inv, (128, BR)))[:, 0:1]

    def project(i, _):
        r = pl.multiple_of(i * BR, BR)
        total = jnp.zeros((BR, dloc), F32)
        for o in range(ntp):
            total += jnp.dot(bfull[o, pl.ds(r, BR)], out_w[pl.ds(o * loc, loc)], preferred_element_type=F32)
        mixed[pl.ds(r, BR)] = total.astype(BF16)
        return 0

    lax.fori_loop(0, tok // BR, project, 0)
    row_total(0, lambda r: mixed[pl.ds(r, BR)].astype(F32))
    wait_total(0)

    def stream(i, _):
        r = pl.multiple_of(i * BR, BR)
        m = mixed[pl.ds(r, BR)].astype(F32)
        mixed[pl.ds(r, BR)] = (residual[pl.ds(r, BR)].astype(F32) + m * inverse_rms(0, r) * mix_gain[...]).astype(BF16)
        return 0

    lax.fori_loop(0, tok // BR, stream, 0)
    row_total(1, lambda r: mixed[pl.ds(r, BR)].astype(F32))
    serve((0, 1), 2)
    wait_total(1)

    def norm(i, _):
        r = pl.multiple_of(i * BR, BR)
        m = mixed[pl.ds(r, BR)].astype(F32)
        normed[pl.ds(r, BR), pl.ds(pl.multiple_of(t * dloc, dloc), dloc)] = (m * inverse_rms(1, r) * pre_gain[...]).astype(BF16)
        return 0

    lax.fori_loop(0, tok // BR, norm, 0)

    def nview(o):
        return normed.at[:, pl.ds(pl.multiple_of(o * dloc, dloc), dloc)]

    gather_start(nview, nsend, nrecv)
    serve((0, 1), 3)
    gather_share(nview, nsend, nrecv)
    for k in range(4, n - 2):
        serve((0, 1), k)
    serve((2,), 0)
    serve((0, 1), n - 2)
    gather_wait(nview, nsend, nrecv)
    for a in range(3):
        local_copy(a).wait()

    def ffn_tile(c, size):
        cols = pl.ds(c, size)
        g = jnp.dot(normed[...], gate_all[:, cols], preferred_element_type=F32)
        u = jnp.dot(normed[...], up_all[:, cols], preferred_element_type=F32)
        hidden[:, cols] = (jax.nn.silu(g) * u).astype(BF16)

    TN = 256
    tiles = ff // TN

    def ffn_step(j, _):
        ffn_tile(pl.multiple_of(j * TN, TN), TN)
        return 0

    cut = (tiles + 1) // 2
    lax.fori_loop(0, cut, ffn_step, 0)
    serve((2,), 1)
    lax.fori_loop(cut, tiles, ffn_step, 0)
    if ff % TN:
        ffn_tile(tiles * TN, ff % TN)

    per = dloc // ncol

    def place(o):
        c = lax.div(o, per)
        w = lax.rem(o, per)
        gap = lax.rem(lax.div(c, 2) - lax.div(t, 2) + chips, chips)
        return lax.rem(c, 2), w, c, gap

    def mate_copy(i):
        return pltpu.make_async_remote_copy(
            src_ref=partial.at[i], dst_ref=shared.at[i], send_sem=psend.at[i], recv_sem=msem.at[i],
            device_id=(s, mate), device_id_type=MESH)

    def far_copy(i, w, c, gap):
        g = lax.rem(gap + chips - 1, chips)
        return pltpu.make_async_remote_copy(
            src_ref=partial.at[i], dst_ref=recvd.at[g, w], send_sem=psend.at[i], recv_sem=precv.at[g, w],
            device_id=(s, c), device_id_type=MESH)

    sent = []

    def down(*blocks):
        for o in blocks:
            i = len(sent)
            sent.append(o)
            partial[i] = jnp.dot(hidden[...], down_all[o], preferred_element_type=F32).astype(BF16)
            par, w, c, gap = place(o)

            @pl.when(par != core)
            def _():
                mate_copy(i).start()

    def join(i):
        par, w, c, gap = place(sent[i])

        @pl.when(par == core)
        def _():
            mate_copy(i).wait_recv()

            def add(b, _):
                r = pl.multiple_of(b * BR, BR)
                total = partial[i, pl.ds(r, BR)].astype(F32) + shared[i, pl.ds(r, BR)].astype(F32)
                partial[i, pl.ds(r, BR)] = total.astype(BF16)
                return 0

            lax.fori_loop(0, tok // BR, add, 0)

            @pl.when(gap == 0)
            def _():
                own[w] = partial[i]

            @pl.when(gap != 0)
            def _():
                far_copy(i, w, c, gap).start()

    down(s)
    joined = 0
    for k in range(2, n - 1):
        serve((2,), k)
        have = k + 1
        if 2 * have >= n:
            if 2 * have == n:
                down(origin[0][have])
            else:
                down(origin[0][have], origin[0][n - have])
        if k == n - 2:
            upto = len(sent)
        else:
            upto = len(sent) - (1 if 2 * have == n else 2) if 2 * have >= n else len(sent)
        while joined < upto:
            join(joined)
            joined += 1

    for i, o in enumerate(sent):
        par, w, c, gap = place(o)

        @pl.when(par != core)
        def _():
            mate_copy(i).wait_send()

        @pl.when(par == core)
        def _():
            @pl.when(gap != 0)
            def _():
                far_copy(i, w, c, gap).wait_send()

    for g in range(1, chips):
        for w in range(per):
            pltpu.make_async_remote_copy(
                src_ref=partial.at[0], dst_ref=recvd.at[g - 1, w],
                send_sem=psend.at[0], recv_sem=precv.at[g - 1, w],
                device_id=(s, mate), device_id_type=MESH).wait_recv()

    def gather_sum(i, _):
        r = pl.multiple_of(i * BR, BR)
        for w in range(per):
            total = own[w, pl.ds(r, BR)].astype(F32)
            for j in range(chips - 1):
                total = total + recvd[j, w, pl.ds(r, BR)].astype(F32)
            out[pl.ds(r, BR), pl.ds(w * ncol, ncol)] = total.astype(BF16)
        return 0

    lax.fori_loop(0, tok // BR, gather_sum, 0)
    row_total(2, lambda r: out[pl.ds(r, BR)].astype(F32))
    wait_total(2)

    def finish(i, _):
        r = pl.multiple_of(i * BR, BR)
        f = out[pl.ds(r, BR)].astype(F32)
        out[pl.ds(r, BR)] = (mixed[pl.ds(r, BR)].astype(F32) + f * inverse_rms(2, r) * ffn_gain[...]).astype(BF16)
        return 0

    lax.fori_loop(0, tok // BR, finish, 0)

    for a in range(3):
        for d in range(2):
            for k in range(n - 1):
                ring(a, d, k).wait_send()
    for j in range(1, n):
        end_copy(j).wait_send()
    gather_sent(bview, bsend, brecv)
    gather_sent(nview, nsend, nrecv)
    for j in range(1, ntp):
        for q in range(3):
            tp_push(lambda o: ssq.at[q, o], qsend.at[q], qrecv.at[q], j, True).wait_send()


def plane_kernel(
    cfg,
    gate_branch_in, recur_in, ids, taps, gmap, imap, level, extra_in, out_w_in, residual_in,
    mix_gain, pre_gain, ffn_gain, gate_w, up_w, down_w,
    out_hbm,
    out, osem, gate_branch, recur, extra, out_w, residual, insem,
    gate_all, up_all, down_all, xpad, idpad, halo, ihalo, bd, fac, drv, ends, bfull,
    mixed, nloc, gloc, normed, gnormed, ghid, gsum, usum, hidden, partial, recvd, ssq,
    lsem, ssend, srecv, zsend, zrecv, msend, mrecv,
    hsend, hrecv, esend, erecv, bsend, brecv, nsend, nrecv, fsend, frecv, gsend, grecv, qsend, qrecv, psend, precv,
):
    n, ntp, nz, ny, width = cfg
    s, t = lax.axis_index("sp"), lax.axis_index("tp")
    tok, loc = recur.shape
    dloc = residual.shape[1]
    krows = gate_w.shape[0]
    ncol = down_w.shape[1]
    ff = gate_w.shape[1]
    CH = math.gcd(tok, 64)
    BR = math.gcd(tok, 128)
    chips = ntp // 2
    z, y = lax.div(s, ny), lax.rem(s, ny)
    x, core = lax.div(t, 2), lax.rem(t, 2)
    mate = t + 1 - 2 * core
    per = dloc // ncol

    barrier = pltpu.get_barrier_semaphore()
    peers = [(z * ny + lax.rem(y + dy, ny), lax.rem(t + dt, ntp)) for dy in range(ny) for dt in range(ntp)][1:]
    peers += [(lax.rem(z + dz, nz) * ny + lax.rem(y + dy, ny), t) for dz in range(1, nz) for dy in range(ny)]
    for p in peers:
        pl.semaphore_signal(barrier, inc=1, device_id=p, device_id_type=MESH)

    inputs = ((recur_in, recur), (extra_in, extra), (gate_branch_in, gate_branch), (out_w_in, out_w), (residual_in, residual))

    def load_input(i):
        return pltpu.make_async_copy(inputs[i][0], inputs[i][1], insem.at[i])

    for i in range(len(inputs)):
        load_input(i).start()
    pl.semaphore_wait(barrier, len(peers))

    low = (2 * z < nz).astype(jnp.int32)
    near_first = []
    for k in range(1, nz):
        near_first += [z + (2 * low - 1) * k, z - (2 * low - 1) * k]
    origin = [z]
    seen = 0
    ranks = []
    for q in near_first:
        ok = jnp.logical_and(q >= 0, q < nz).astype(jnp.int32)
        seen = seen + ok
        ranks.append((q, ok, seen))
    for j in range(1, nz):
        origin.append(sum(jnp.where(jnp.logical_and(ok == 1, r == j), q, 0) for q, ok, r in ranks))

    hcol = ncol // 2
    hrow = krows // 2
    GATE, UP, DOWN, WIDE = (0, 1), (2,), (3, 4), (5, 6)
    fa = ff - ghid.shape[1]
    main, side = pl.ds(0, fa), pl.ds(fa, ff - fa)
    inner = jnp.logical_and(z > 0, z < nz - 1)
    host = jnp.logical_or(z == 1, z == nz - 2)
    guest_z = jnp.where(z == 1, 0, nz - 1)
    host_z = jnp.where(z == 0, 1, nz - 2)

    def block(a, o, b):
        i = o * ny + b
        if a in GATE:
            return gate_all.at[pl.ds(pl.multiple_of(i * krows + a * hrow, hrow), hrow), main]
        if a in UP:
            return up_all.at[pl.ds(pl.multiple_of(i * krows, krows), krows), main]
        if a in WIDE:
            return (gate_all, up_all)[a - WIDE[0]].at[pl.ds(pl.multiple_of(i * krows, krows), krows), side]
        return down_all.at[i, :, pl.ds((a - DOWN[0]) * hcol, hcol)]

    def own_shard(a):
        if a in GATE:
            return gate_w.at[pl.ds(a * hrow, hrow), main]
        if a in UP:
            return up_w.at[:, main]
        if a in WIDE:
            return (gate_w, up_w)[a - WIDE[0]].at[:, side]
        return down_w.at[:, pl.ds((a - DOWN[0]) * hcol, hcol)]

    def seed_local(a):
        return pltpu.make_async_copy(own_shard(a), block(a, z, y), lsem.at[a])

    def seed_swap(a):
        return pltpu.make_async_remote_copy(
            src_ref=own_shard(a), dst_ref=block(a, z, y), send_sem=ssend.at[a], recv_sem=srecv.at[a],
            device_id=(z * ny + 1 - y, mate), device_id_type=MESH)

    def z_copy(a, o, up):
        b = block(a, o, core)
        return pltpu.make_async_remote_copy(
            src_ref=b, dst_ref=b, send_sem=zsend.at[up, a, o], recv_sem=zrecv.at[a, o],
            device_id=((z + 2 * up - 1) * ny + y, t), device_id_type=MESH)

    def mate_copy(a, o, theirs=False):
        b = block(a, o, 1 - core if theirs else core)
        return pltpu.make_async_remote_copy(
            src_ref=b, dst_ref=b, send_sem=msend.at[a, o], recv_sem=mrecv.at[a, o],
            device_id=(s, mate), device_id_type=MESH)

    def fan_down(a, o, act):
        @pl.when(jnp.logical_and(o >= z, z > (1 if a in WIDE else 0)))
        def _():
            act(z_copy(a, o, 0))

    def fan_up(a, o, act):
        @pl.when(jnp.logical_and(o <= z, z < nz - (2 if a in WIDE else 1)))
        def _():
            act(z_copy(a, o, 1))

    def fan(a, o, act):
        fan_down(a, o, act)
        fan_up(a, o, act)
        if a in WIDE:
            @pl.when(inner)
            def _():
                act(mate_copy(a, o))
        else:
            act(mate_copy(a, o))

    def start(c):
        c.start()

    def seed_ready(a):
        @pl.when(y == core)
        def _():
            seed_local(a).wait()

        @pl.when(y != core)
        def _():
            pltpu.make_async_remote_copy(
                src_ref=block(a, z, core), dst_ref=block(a, z, core), send_sem=ssend.at[a], recv_sem=srecv.at[a],
                device_id=(z * ny + 1 - y, mate), device_id_type=MESH).wait_recv()

    def push_seed(a):
        seed_ready(a)
        fan(a, z, start)

    def relay_from(a, o):
        z_copy(a, o, 0).wait_recv()
        fan(a, o, start)

    def relay(items, j):
        for a in items:
            relay_from(a, origin[j])

    def load_seed(a):
        @pl.when(y == core)
        def _():
            seed_local(a).start()

        @pl.when(y != core)
        def _():
            seed_swap(a).start()

    def halo_copy(i):
        src, dst = ((recur_in.at[pl.ds(tok - 16, 16)], halo), (ids, ihalo))[i]
        return pltpu.make_async_remote_copy(
            src_ref=src, dst_ref=dst, send_sem=hsend.at[i], recv_sem=hrecv.at[i],
            device_id=(lax.rem(s + 1, n), t), device_id_type=MESH)

    for i in range(2):
        halo_copy(i).start()

    for a in GATE:
        load_seed(a)

    @pl.when(y == core)
    def _():
        for a in GATE:
            push_seed(a)

    head = gmap.shape[1]
    spread = (lax.rem(lax.broadcasted_iota(jnp.int32, (head, loc), 1), head)
              == lax.broadcasted_iota(jnp.int32, (head, loc), 0)).astype(BF16)
    diag = (lax.div(lax.broadcasted_iota(jnp.int32, (loc, loc), 0), head)
            == lax.div(lax.broadcasted_iota(jnp.int32, (loc, loc), 1), head))
    for i, m in enumerate((gmap, imap)):
        tiled = jnp.dot(m[...], spread, preferred_element_type=F32)
        bd[i] = jnp.where(diag, tiled, 0.0).astype(BF16)

    for i in range(2):
        load_input(i).wait()

    def down_rows(row):
        return jnp.transpose(jnp.broadcast_to(row, (128, 128)))

    for i in range(tok // 128):
        idpad[pl.ds(8 + i * 128, 128)] = down_rows(ids[i:i + 1])

    def fill(i, _):
        r = pl.multiple_of(i * CH, CH)
        xpad[pl.ds(pl.multiple_of(r + 8, 8), CH)] = recur[pl.ds(r, CH)].astype(F32)
        return 0

    lax.fori_loop(0, tok // CH, fill, 0)
    u = -level[...]
    rate = -GATE_POWER * (jnp.maximum(u, 0.0) + jnp.log1p(jnp.exp(-jnp.abs(u))))
    for i in range(2):
        halo_copy(i).wait()
    first = s == 0
    xpad[pl.ds(0, 8)] = halo[...].astype(F32)[8:16]
    idpad[pl.ds(0, 8)] = jnp.where(first, -1, down_rows(ihalo[tok // 128 - 1:tok // 128])[120:])
    reps = loc // 128
    ntaps = taps.shape[0]

    def front(i, _):
        r = pl.multiple_of(i * CH, CH)
        xw = xpad[pl.ds(r, CH + 8)]
        iw = idpad[pl.ds(r, CH + 8)]
        mine = iw[8:]
        tw = taps[...].astype(F32)
        conv = xw[8:] * tw[0:1]
        cont = None
        for k in range(1, ntaps):
            same1 = (pltpu.roll(iw, k, axis=0)[8:] == mine).astype(F32)
            same = jnp.concatenate([same1] * reps, axis=1)
            if k == 1:
                cont = same
            conv = conv + same * pltpu.roll(xw, k, axis=0)[8:] * tw[k:k + 1]
        cb = conv.astype(BF16)
        rg = jax.nn.sigmoid(jnp.dot(cb, bd[0], preferred_element_type=F32))
        ig = jax.nn.sigmoid(jnp.dot(cb, bd[1], preferred_element_type=F32))
        ld = rate * rg + extra[pl.ds(r, CH)]
        fac[pl.ds(r, CH)] = jnp.exp(ld) * cont
        drv[pl.ds(r, CH)] = jnp.sqrt(one_minus_exp(2.0 * ld)) * ig * cb.astype(F32)
        return 0

    lax.fori_loop(0, tok // CH, front, 0)

    @pl.when(y == core)
    def _():
        for a in UP + WIDE:
            load_seed(a)

    rows8 = lax.broadcasted_iota(jnp.int32, (8, loc), 0)

    def scan(i, carry):
        pc, hc = carry
        r = pl.multiple_of(i * 8, 8)
        a, b = fac[pl.ds(r, 8)], drv[pl.ds(r, 8)]
        for sh in (1, 2, 4):
            keep = rows8 >= sh
            b = b + a * jnp.where(keep, pltpu.roll(b, sh, axis=0), 0.0)
            a = a * jnp.where(keep, pltpu.roll(a, sh, axis=0), 1.0)
        h = b + a * hc
        p = a * pc
        fac[pl.ds(r, 8)] = p
        drv[pl.ds(r, 8)] = h
        return (jnp.broadcast_to(p[7:8], (8, loc)), jnp.broadcast_to(h[7:8], (8, loc)))

    pend, hend = lax.fori_loop(0, tok // 8, scan, (jnp.ones((8, loc), F32), jnp.zeros((8, loc), F32)))
    ends[s] = jnp.concatenate([pend, hend], axis=0)

    def end_copy(j):
        return pltpu.make_async_remote_copy(
            src_ref=ends.at[s], dst_ref=ends.at[s], send_sem=esend.at[j - 1], recv_sem=erecv.at[j - 1],
            device_id=(lax.rem(s + j, n), t), device_id_type=MESH)

    def end_arrived(j):
        o = lax.rem(s + n - j, n)
        pltpu.make_async_remote_copy(
            src_ref=ends.at[o], dst_ref=ends.at[o], send_sem=esend.at[j - 1], recv_sem=erecv.at[j - 1],
            device_id=(lax.rem(s + j, n), t), device_id_type=MESH).wait_recv()

    for j in range(1, n):
        end_copy(j).start()

    @pl.when(y != core)
    def _():
        for a in GATE:
            push_seed(a)
        for a in UP + WIDE:
            load_seed(a)

    for a in DOWN:
        load_seed(a)

    @pl.when(y == core)
    def _():
        for a in UP + WIDE:
            push_seed(a)

    early = min(2, nz - 1)
    for j in range(1, n):
        end_arrived(j)
    carry = jnp.zeros((8, loc), F32)
    for o in range(n - 1):
        e = ends[o]
        carry = jnp.where(o < s, e[:8] * carry + e[8:], carry)
    cin = carry[0:1]

    for i in range(2, len(inputs)):
        load_input(i).wait()

    def branch(i, _):
        r = pl.multiple_of(i * CH, CH)
        st = drv[pl.ds(r, CH)] + fac[pl.ds(r, CH)] * cin
        bfull[t, pl.ds(r, CH)] = (st * jax.nn.gelu(gate_branch[pl.ds(r, CH)].astype(F32))).astype(BF16)
        return 0

    lax.fori_loop(0, tok // CH, branch, 0)

    def tp_push(view, send, recv, j, start):
        o = t if start else lax.rem(t + ntp - j, ntp)
        return pltpu.make_async_remote_copy(
            src_ref=view(o), dst_ref=view(o), send_sem=send.at[j - 1], recv_sem=recv.at[j - 1],
            device_id=(s, lax.rem(t + j, ntp)), device_id_type=MESH)

    def bview(o):
        return bfull.at[o]

    chips = ntp // 2
    core = lax.rem(t, 2)
    mate = t + 1 - 2 * core

    def far(view, send, recv, c, start):
        o = t if start else lax.rem(t + ntp - 2 * c, ntp)
        return pltpu.make_async_remote_copy(
            src_ref=view(o), dst_ref=view(o), send_sem=send.at[c - 1], recv_sem=recv.at[c - 1],
            device_id=(s, lax.rem(t + 2 * c, ntp)), device_id_type=MESH)

    def near(view, send, recv, c, start):
        base = t if start else mate
        o = lax.rem(base + ntp - 2 * c, ntp)
        return pltpu.make_async_remote_copy(
            src_ref=view(o), dst_ref=view(o), send_sem=send.at[chips - 1 + c], recv_sem=recv.at[chips - 1 + c],
            device_id=(s, mate), device_id_type=MESH)

    def gather_start(view, send, recv):
        for c in range(1, chips):
            far(view, send, recv, c, True).start()
        near(view, send, recv, 0, True).start()

    def gather_share(view, send, recv):
        for c in range(1, chips):
            far(view, send, recv, c, False).wait_recv()
            near(view, send, recv, c, True).start()

    def gather_wait(view, send, recv):
        for c in range(chips):
            near(view, send, recv, c, False).wait_recv()

    def gather_sent(view, send, recv):
        for c in range(1, chips):
            far(view, send, recv, c, True).wait_send()
        for c in range(chips):
            near(view, send, recv, c, True).wait_send()

    gather_start(bview, bsend, brecv)

    @pl.when(y != core)
    def _():
        for a in UP + WIDE:
            push_seed(a)

    gather_share(bview, bsend, brecv)
    gather_wait(bview, bsend, brecv)

    def row_total(q, values):
        def write(i, _):
            r = pl.multiple_of(i * BR, BR)
            v = values(r)
            c = jnp.sum(v * v, axis=1, keepdims=True)
            ssq[q, t, :, pl.ds(r, BR)] = jnp.transpose(jnp.broadcast_to(c, (BR, 128)))[:8]
            return 0

        lax.fori_loop(0, tok // BR, write, 0, unroll=True)
        for j in range(1, ntp):
            tp_push(lambda o: ssq.at[q, o], qsend.at[q], qrecv.at[q], j, True).start()

    def wait_total(q):
        for j in range(1, ntp):
            tp_push(lambda o: ssq.at[q, o], qsend.at[q], qrecv.at[q], j, False).wait_recv()

    def inverse_rms(q, r):
        row = ssq[q, 0, 0:1, pl.ds(r, BR)]
        for o in range(1, ntp):
            row = row + ssq[q, o, 0:1, pl.ds(r, BR)]
        inv = lax.rsqrt(row / width + EPS)
        return jnp.transpose(jnp.broadcast_to(inv, (128, BR)))[:, 0:1]

    def project(i, _):
        r = pl.multiple_of(i * BR, BR)
        total = jnp.zeros((BR, dloc), F32)
        for o in range(ntp):
            total += jnp.dot(bfull[o, pl.ds(r, BR)], out_w[pl.ds(o * loc, loc)], preferred_element_type=F32)
        mixed[pl.ds(r, BR)] = total.astype(BF16)
        return 0

    lax.fori_loop(0, tok // BR, project, 0)
    row_total(0, lambda r: mixed[pl.ds(r, BR)].astype(F32))

    @pl.when(inner)
    def _():
        for j in range(1, early + 1):
            relay(GATE, j)

    wait_total(0)

    def stream(i, _):
        r = pl.multiple_of(i * BR, BR)
        m = mixed[pl.ds(r, BR)].astype(F32)
        mixed[pl.ds(r, BR)] = (residual[pl.ds(r, BR)].astype(F32) + m * inverse_rms(0, r) * mix_gain[...]).astype(BF16)
        return 0

    lax.fori_loop(0, tok // BR, stream, 0, unroll=True)
    row_total(1, lambda r: mixed[pl.ds(r, BR)].astype(F32))
    wait_total(1)

    cols = pl.ds(pl.multiple_of(t * dloc, dloc), dloc)

    def norm(i, _):
        r = pl.multiple_of(i * BR, BR)
        m = mixed[pl.ds(r, BR)].astype(F32)
        v = (m * inverse_rms(1, r) * pre_gain[...]).astype(BF16)
        nloc[pl.ds(r, BR)] = v

        @pl.when(y == core)
        def _():
            normed[pl.ds(r, BR), cols] = v

        return 0

    lax.fori_loop(0, tok // BR, norm, 0, unroll=True)
    htok = tok // 2
    piece, spot = (nloc, gloc), (normed, gnormed)

    def n_copy(q, dy, dx):
        return pltpu.make_async_remote_copy(
            src_ref=piece[q], dst_ref=spot[q].at[:, cols], send_sem=nsend.at[q, dy, dx], recv_sem=nrecv.at[q, t],
            device_id=(z * ny + lax.rem(y + dy, ny), 2 * lax.rem(x + dx, chips) + y), device_id_type=MESH)

    def to_plane(q, act):
        for dx in range(1, chips):
            act(n_copy(q, 0, dx))
        for dy in range(1, ny):
            act(n_copy(q, dy, 0))

        @pl.when(y != core)
        def _():
            act(n_copy(q, 0, 0))

    def n_wait(q, o):
        view = spot[q].at[:, pl.ds(pl.multiple_of(o * dloc, dloc), dloc)]
        pltpu.make_async_remote_copy(
            src_ref=view, dst_ref=view, send_sem=nsend.at[q, 0, 0], recv_sem=nrecv.at[q, o],
            device_id=(s, mate), device_id_type=MESH).wait_recv()

    def f_copy(q, o, h, device):
        view = spot[q].at[pl.ds(h * htok, htok), pl.ds(pl.multiple_of(o * dloc, dloc), dloc)]
        return pltpu.make_async_remote_copy(
            src_ref=view, dst_ref=view, send_sem=fsend.at[q, lax.rem(o, 2)], recv_sem=frecv.at[q, h, o],
            device_id=device, device_id_type=MESH)

    other = 1 - x

    def forward(q, act, wait):
        for e in range(2):
            @pl.when(y == core)
            def _():
                o = 2 * other + e
                if wait:
                    n_wait(q, o)
                act(f_copy(q, o, 0, (z * ny + 1 - y, t)))

            @pl.when(y != core)
            def _():
                o = 2 * x + e
                if wait:
                    n_wait(q, o)
                act(f_copy(q, o, 1, (s, 2 * other + core)))

    def n_ready(q):
        @pl.when(y == core)
        def _():
            n_wait(q, mate)

        @pl.when(y != core)
        def _():
            for e in range(2):
                for h in range(2):
                    f_copy(q, 2 * other + e, h, (s, mate)).wait_recv()

    def guest_hop():
        return pltpu.make_async_remote_copy(
            src_ref=nloc, dst_ref=gloc, send_sem=gsend.at[0], recv_sem=grecv.at[0],
            device_id=(host_z * ny + y, t), device_id_type=MESH)

    def guest_return():
        return pltpu.make_async_remote_copy(
            src_ref=ghid, dst_ref=hidden.at[:, side], send_sem=gsend.at[1], recv_sem=grecv.at[1],
            device_id=(guest_z * ny + y, t), device_id_type=MESH)

    to_plane(0, start)

    @pl.when(jnp.logical_not(inner))
    def _():
        guest_hop().start()
        for a in DOWN:
            push_seed(a)

    @pl.when(inner)
    def _():
        for j in range(1, early + 1):
            relay(UP, j)
            relay(WIDE, j)

    forward(0, start, True)

    @pl.when(host)
    def _():
        guest_hop().wait_recv()

        @pl.when(y == core)
        def _():
            gnormed[:, cols] = gloc[...]

        to_plane(1, start)

    @pl.when(jnp.logical_not(inner))
    def _():
        for j in range(1, early + 1):
            relay(GATE, j)
            relay(UP, j)

    def outward_seed(items):
        for a in items:
            @pl.when(low == 1)
            def _():
                fan_down(a, z, start)

            @pl.when(low == 0)
            def _():
                fan_up(a, z, start)

    def mates(items, js):
        for j in js:
            for a in items:
                mate_copy(a, origin[j], True).wait_recv()

    kblk = ny * krows
    TN = 256
    def sums(js, cs):
        g = u = None
        for j in js:
            k = pl.ds(pl.multiple_of(origin[j] * kblk, kblk), kblk)
            a = normed[:, k]
            gj = jnp.dot(a, gate_all[k, cs], preferred_element_type=F32)
            uj = jnp.dot(a, up_all[k, cs], preferred_element_type=F32)
            g, u = (gj, uj) if g is None else (g + gj, u + uj)
        return g, u

    def first_tile(c, size):
        cs = pl.ds(c, size)
        gsum[:, cs], usum[:, cs] = sums(range(nz - 1), cs)

    def last_tile(c, size):
        cs = pl.ds(c, size)
        g, u = sums((nz - 1,), cs)
        g, u = g + gsum[:, cs], u + usum[:, cs]
        hidden[:, cs] = (jax.nn.silu(g) * u).astype(BF16)

    def over_tiles(tile):
        def step(j, _):
            tile(pl.multiple_of(j * TN, TN), TN)
            return 0

        lax.fori_loop(0, fa // TN, step, 0)
        if fa % TN:
            tile(fa // TN * TN, fa % TN)

        @pl.when(inner)
        def _():
            tile(fa, ff - fa)

    @pl.when(inner)
    def _():
        for j in range(early + 1, nz):
            relay(GATE, j)
            relay(UP, j)
            relay(WIDE, j)
        for a in DOWN:
            seed_ready(a)
            mate_copy(a, z).start()

            @pl.when(low == 1)
            def _():
                fan_up(a, z, start)

            @pl.when(low == 0)
            def _():
                fan_down(a, z, start)

        outward_seed(DOWN[:1])
        relay(DOWN, 2)

    n_ready(0)
    mates(GATE + UP, range(nz - 1))

    @pl.when(inner)
    def _():
        mates(WIDE, range(nz - 1))

    over_tiles(first_tile)

    @pl.when(host)
    def _():
        forward(1, start, True)

    @pl.when(jnp.logical_not(inner))
    def _():
        for j in range(early + 1, nz):
            relay(GATE, j)
            relay(UP, j)

    mates(GATE + UP, (nz - 1,))

    @pl.when(inner)
    def _():
        mates(WIDE, (nz - 1,))

    over_tiles(last_tile)

    @pl.when(host)
    def _():
        n_ready(1)
        g = jnp.dot(gnormed[...], gate_all[:, side], preferred_element_type=F32)
        v = jnp.dot(gnormed[...], up_all[:, side], preferred_element_type=F32)
        ghid[...] = (jax.nn.silu(g) * v).astype(BF16)
        guest_return().start()

    @pl.when(jnp.logical_not(inner))
    def _():
        guest_return().wait_recv()

    me = y * chips + x

    def p_copy(i, h):
        c = pl.ds(h * hcol, hcol)
        return pltpu.make_async_remote_copy(
            src_ref=partial.at[i, :, c], dst_ref=recvd.at[me, lax.rem(i, per), :, c], send_sem=psend.at[i, h],
            recv_sem=precv.at[me, lax.rem(i, per), h],
            device_id=(z * ny + core, lax.div(i, per)), device_id_type=MESH)

    def owned(i):
        return jnp.logical_and(y == core, lax.div(i, per) == t)

    def ship(i, hs):
        @pl.when(owned(i))
        def _():
            for h in hs:
                c = pl.ds(h * hcol, hcol)
                recvd[me, lax.rem(i, per), :, c] = partial[i, :, c]

        @pl.when(jnp.logical_not(owned(i)))
        def _():
            for h in hs:
                p_copy(i, h).start()

    def mate_ready(a, o, b):
        @pl.when(b != core)
        def _():
            mate_copy(a, o, True).wait_recv()

    last = nz - 1
    ends_order = [0] + list(range(2, nz)) + [1]
    line = [jnp.where(inner, origin[j], origin[ends_order[j]]) for j in range(nz)]
    roles = (y, 1 - y)

    def bring(j, k, items):
        @pl.when(jnp.logical_and(roles[k] == core, jnp.logical_not(inner) if j == 2 else True))
        def _():
            for a in items:
                relay_from(a, line[j])

    def whole_block(j, k):
        i = line[j] * ny + roles[k]
        if j:
            bring(j, k, DOWN)
        for a in DOWN:
            mate_ready(a, line[j], roles[k])
        partial[i] = jnp.dot(hidden[...], down_all[i], preferred_element_type=F32).astype(BF16)
        ship(i, (0, 1))

    def half_block(j, k, h):
        i = line[j] * ny + roles[k]
        c = pl.ds(h * hcol, hcol)
        mate_ready(DOWN[h], line[j], roles[k])
        partial[i, :, c] = jnp.dot(hidden[...], down_all[i, :, c], preferred_element_type=F32).astype(BF16)
        ship(i, (h,))

    def outward_rest(k):
        @pl.when(jnp.logical_and(inner, roles[k] == core))
        def _():
            outward_seed(DOWN[1:])

    for j in range(2):
        for k in range(2):
            whole_block(j, k)
    for k in range(2):
        bring(last, k, DOWN[:1])
        half_block(last, k, 0)
    for j in range(2, last):
        whole_block(j, 0)
    for j in range(2, last):
        for h in range(2):
            if j == last - 1 and h == 1:
                bring(last, 0, DOWN[1:])
                outward_rest(0)
            bring(j, 1, DOWN[h:h + 1])
            half_block(j, 1, h)
    bring(last, 1, DOWN[1:])
    outward_rest(1)
    for k in range(2):
        half_block(last, k, 1)

    def p_wait(dy, dx):
        k = lax.rem(y + dy, ny) * chips + lax.rem(x + dx, chips)
        for w in range(per):
            for h in range(2):
                view = recvd.at[k, w, :, pl.ds(h * hcol, hcol)]
                pltpu.make_async_remote_copy(
                    src_ref=view, dst_ref=view, send_sem=psend.at[0, 0], recv_sem=precv.at[k, w, h],
                    device_id=(s, mate), device_id_type=MESH).wait_recv()

    for dy in range(ny):
        for dx in range(chips):
            if dy or dx:
                p_wait(dy, dx)

    @pl.when(y != core)
    def _():
        p_wait(0, 0)

    def ffn_rows(r):
        for w in range(per):
            total = recvd[0, w, pl.ds(r, BR)].astype(F32)
            for k in range(1, ny * chips):
                total = total + recvd[k, w, pl.ds(r, BR)].astype(F32)
            out[pl.ds(r, BR), pl.ds(w * ncol, ncol)] = total.astype(BF16)
        return out[pl.ds(r, BR)].astype(F32)

    row_total(2, ffn_rows)
    wait_total(2)

    def out_copy(i):
        rows = pl.ds(pl.multiple_of(i * BR, BR), BR)
        return pltpu.make_async_copy(out.at[rows], out_hbm.at[rows], osem.at[i])

    def finish(i, _):
        r = pl.multiple_of(i * BR, BR)
        f = out[pl.ds(r, BR)].astype(F32)
        out[pl.ds(r, BR)] = (mixed[pl.ds(r, BR)].astype(F32) + f * inverse_rms(2, r) * ffn_gain[...]).astype(BF16)
        out_copy(i).start()
        return 0

    lax.fori_loop(0, tok // BR, finish, 0, unroll=True)

    def sent(c):
        c.wait_send()

    for a in GATE + UP + DOWN + WIDE:
        @pl.when(y != core)
        def _():
            seed_swap(a).wait_send()

        for j in range(nz):
            fan(a, origin[j], sent)
    for j in range(1, n):
        end_copy(j).wait_send()
    gather_sent(bview, bsend, brecv)
    to_plane(0, sent)
    forward(0, sent, False)

    @pl.when(host)
    def _():
        to_plane(1, sent)
        forward(1, sent, False)
        guest_return().wait_send()

    @pl.when(jnp.logical_not(inner))
    def _():
        guest_hop().wait_send()

    for i in range(n):
        @pl.when(jnp.logical_not(owned(i)))
        def _():
            for h in range(2):
                p_copy(i, h).wait_send()
    for j in range(1, ntp):
        for q in range(3):
            tp_push(lambda o: ssq.at[q, o], qsend.at[q], qrecv.at[q], j, True).wait_send()
    for i in range(tok // BR):
        out_copy(i).wait()


def body(n, ntp, gate_branch, recur_input, doc_ids, conv_taps, gate_map, input_map, decay_level, decay_extra,
         out_weight, residual, mix_gain, pre_gain, ffn_gain, gate_weight, up_weight, down_weight):
    tok, loc = recur_input.shape
    dloc = residual.shape[1]
    krows, ff = gate_weight.shape
    ncol = down_weight.shape[1]
    heads, head, _ = gate_map.shape
    nz, ny = grid_of(n)
    planes = ny == 2 and nz > 3 and ntp == 4 and tok % 256 == 0 and ff % 128 == 0
    fb = ff // 128 * 2 // 11 * 128
    if planes:
        ids, taps, rate = doc_ids.reshape(tok // 128, 128), conv_taps, decay_level[None, :]
    else:
        ids = jnp.broadcast_to(doc_ids[:, None], (tok, 128))
        taps = conv_taps.astype(F32)
        rate = (GATE_POWER * -jax.nn.softplus(-decay_level))[None, :]
    args = (gate_branch, recur_input, ids, taps, gate_map.reshape(heads * head, head),
            input_map.reshape(heads * head, head), rate, decay_extra, out_weight, residual,
            mix_gain[None, :], pre_gain[None, :], ffn_gain[None, :], gate_weight, up_weight, down_weight)
    vm = pl.BlockSpec(memory_space=pltpu.VMEM)
    hbm = pl.BlockSpec(memory_space=pl.ANY)
    V, S = pltpu.VMEM, pltpu.SemaphoreType.DMA
    per = dloc // ncol
    chips = ntp // 2
    if planes:
        fn = plane_kernel
        in_specs = [hbm] * 2 + [vm] * 5 + [hbm] * 3 + [vm] * 3 + [hbm] * 3
        out_spec = hbm
        scratch = [
            V((tok, dloc), BF16), S((tok // math.gcd(tok, 128),)),
            V((tok, loc), BF16), V((tok, loc), BF16), V((tok, loc), F32), V(out_weight.shape, BF16), V((tok, dloc), BF16), S((5,)),
            V((n * krows, ff), BF16), V((n * krows, ff), BF16), V((n, ff, ncol), BF16),
            V((tok + 8, loc), F32), V((tok + 8, 128), jnp.int32), V((16, loc), BF16), V((tok // 128, 128), jnp.int32),
            V((2, loc, loc), BF16), V((tok, loc), F32), V((tok, loc), F32), V((n, 16, loc), F32),
            V((ntp, tok, loc), BF16), V((tok, dloc), BF16), V((tok, dloc), BF16), V((tok, dloc), BF16), V((tok, dloc * ntp), BF16),
            V((tok, dloc * ntp), BF16), V((tok, fb), BF16), V((tok, ff), F32), V((tok, ff), F32), V((tok, ff), BF16), V((n, tok, ncol), BF16), V((ny * chips, per, tok, ncol), BF16), V((3, ntp, 8, tok), F32),
            S((7,)), S((7,)), S((7,)), S((2, 7, nz)), S((7, nz)), S((7, nz)), S((7, nz)),
            S((2,)), S((2,)), S((n - 1,)), S((n - 1,)), S((ntp - 1,)), S((ntp - 1,)),
            S((2, ny, chips)), S((2, ntp)), S((2, 2)), S((2, 2, ntp)), S((2,)), S((2,)), S((3, ntp - 1)), S((3, ntp - 1)), S((n, 2)), S((ny * chips, per, 2)),
        ]
    else:
        fn = kernel
        in_specs = [vm] * 13 + [hbm] * 3
        out_spec = vm
        scratch = [
            V((n * krows, ff), BF16), V((n * krows, ff), BF16), V((n, ff, ncol), BF16),
            V((tok + 8, loc), F32), V((tok + 8, 128), jnp.int32), V((16, loc), BF16), V((8, 128), jnp.int32),
            V((2, loc, loc), BF16), V((tok, loc), F32), V((tok, loc), F32), V((n, 16, loc), F32),
            V((ntp, tok, loc), BF16), V((tok, dloc), BF16), V((tok, dloc * ntp), BF16), V((tok, ff), BF16),
            V((n, tok, ncol), BF16), V((n, tok, ncol), BF16), V((chips - 1, per, tok, ncol), BF16), V((per, tok, ncol), BF16),
            V((3, ntp, 8, tok), F32),
            S((3, 2, n - 1)), S((3, 2, n - 1)), S((3,)), S((2,)), S((2,)), S((n - 1,)), S((n - 1,)),
            S((ntp - 1,)), S((ntp - 1,)), S((ntp - 1,)), S((ntp - 1,)), S((3, ntp - 1)), S((3, ntp - 1)),
            S((n,)), S((chips - 1, per)), S((n,)),
        ]
    return pl.pallas_call(
        functools.partial(fn, (n, ntp, nz, ny, dloc * ntp)),
        out_shape=jax.ShapeDtypeStruct((tok, dloc), BF16),
        in_specs=in_specs,
        out_specs=out_spec,
        scratch_shapes=scratch,
        compiler_params=pltpu.CompilerParams(
            collective_id=0, has_side_effects=True, vmem_limit_bytes=62 * 1024 * 1024),
    )(*args)


def solution(mesh):
    in_specs = (
        P("sp", "tp"), P("sp", "tp"), P("sp"), P(None, "tp"), P("tp", None, None), P("tp", None, None),
        P("tp"), P("sp", "tp"), P(None, "tp"), P("sp", "tp"), P("tp"), P("tp"), P("tp"),
        P("sp", "tp"), P("sp", "tp"), P("tp", "sp"),
    )
    fn = functools.partial(body, mesh.shape["sp"], mesh.shape["tp"])
    return jax.shard_map(fn, mesh=mesh, in_specs=in_specs, out_specs=P("sp", "tp"), check_vma=False)
```

```python
import functools
import math

import jax
import jax.numpy as jnp
from jax import lax
from jax.experimental import pallas as pl
from jax.experimental.pallas import tpu as pltpu
from jax.sharding import PartitionSpec as P

EPS = 1e-06
GATE_POWER = 8.0
F32 = jnp.float32
BF16 = jnp.bfloat16
MESH = pl.DeviceIdType.MESH


def grid_of(n):
    ny = 1
    for c in range(1, n + 1):
        if n % c == 0 and c * c <= n:
            ny = c
    return n // ny, ny


def ring_pos(s, nz, ny):
    z, y = lax.div(s, ny), lax.rem(s, ny)
    off = lax.div(y + ny - 1, ny)
    r = nz - 1 - z
    odd = lax.rem(r, 2)
    within = (1 - odd) * (y - 1) + odd * (ny - 1 - y)
    return (1 - off) * z + off * (nz + r * (ny - 1) + within)


def ring_dev(p, nz, ny):
    off = lax.div(lax.div(p, nz) + ny - 1, ny)
    q = off * (p - nz)
    r = lax.div(q, ny - 1)
    w = lax.rem(q, ny - 1)
    odd = lax.rem(r, 2)
    y = (1 - odd) * (1 + w) + odd * (ny - 1 - w)
    return (1 - off) * (p * ny) + off * ((nz - 1 - r) * ny + y)


def one_minus_exp(u):
    series = 1.0 + u * (1 / 8)
    for k in (7, 6, 5, 4, 3, 2):
        series = 1.0 + u * (1.0 / k) * series
    return jnp.where(u > -0.35, -u * series, 1.0 - jnp.exp(u))


def kernel(
    cfg,
    gate_branch, recur, ids, taps, gmap, imap, rate, extra, out_w, residual,
    mix_gain, pre_gain, ffn_gain, gate_w, up_w, down_w,
    out,
    gate_all, up_all, down_all, xpad, idpad, halo, ihalo, bd, fac, drv, ends, bfull,
    mixed, normed, hidden, partial, shared, recvd, own, ssq,
    wsend, wrecv, lsem, hsend, hrecv, esend, erecv, bsend, brecv, nsend, nrecv, qsend, qrecv, psend, precv, msem,
):
    n, ntp, nz, ny, width = cfg
    s, t = lax.axis_index("sp"), lax.axis_index("tp")
    tok, loc = recur.shape
    dloc = residual.shape[1]
    krows = gate_w.shape[0]
    ncol = down_w.shape[1]
    ff = gate_w.shape[1]
    CH = math.gcd(tok, 64)
    BR = math.gcd(tok, 128)
    pos = ring_pos(s, nz, ny)

    barrier = pltpu.get_barrier_semaphore()
    for j in range(1, n):
        pl.semaphore_signal(barrier, inc=1, device_id=(lax.rem(s + j, n), t), device_id_type=MESH)
    for j in range(1, ntp):
        pl.semaphore_signal(barrier, inc=1, device_id=(s, lax.rem(t + j, ntp)), device_id_type=MESH)
    pl.semaphore_wait(barrier, n - 1 + ntp - 1)

    shard = (gate_w, up_w, down_w)
    whole = (gate_all, up_all, down_all)
    nxt = [ring_dev(lax.rem(pos + 1, n), nz, ny), ring_dev(lax.rem(pos + n - 1, n), nz, ny)]
    origin = [[s] + [ring_dev(lax.rem(pos + (n - k if d == 0 else k), n), nz, ny) for k in range(1, n)] for d in range(2)]

    def half(a, o, d, local=False):
        if a < 2:
            h = krows // 2
            if local:
                return shard[a].at[pl.ds(d * h, h)]
            return whole[a].at[pl.ds(pl.multiple_of(o * krows + d * h, h), h)]
        h = ff // 2
        if local:
            return shard[a].at[pl.ds(d * h, h)]
        return whole[a].at[o, pl.ds(d * h, h)]

    def ring(a, d, k):
        o = origin[d][k]
        return pltpu.make_async_remote_copy(
            src_ref=half(a, o, d, k == 0), dst_ref=half(a, o, d),
            send_sem=wsend.at[a, d, k], recv_sem=wrecv.at[a, d, k],
            device_id=(nxt[d], t), device_id_type=MESH)

    def arrived(a, d, k):
        o = origin[d][k + 1]
        pltpu.make_async_remote_copy(
            src_ref=half(a, o, d), dst_ref=half(a, o, d),
            send_sem=wsend.at[a, d, k], recv_sem=wrecv.at[a, d, k],
            device_id=(nxt[d], t), device_id_type=MESH).wait_recv()

    def serve(arrays, k):
        for a in arrays:
            for d in range(2):
                arrived(a, d, k)
                if k < n - 2:
                    ring(a, d, k + 1).start()

    for a in range(3):
        for d in range(2):
            ring(a, d, 0).start()

    def halo_copy(i):
        src, dst = ((recur.at[pl.ds(tok - 16, 16)], halo), (ids.at[pl.ds(tok - 8, 8)], ihalo))[i]
        return pltpu.make_async_remote_copy(
            src_ref=src, dst_ref=dst, send_sem=hsend.at[i], recv_sem=hrecv.at[i],
            device_id=(lax.rem(s + 1, n), t), device_id_type=MESH)

    for i in range(2):
        halo_copy(i).start()

    def local_copy(a):
        if a < 2:
            dst = whole[a].at[pl.ds(pl.multiple_of(s * krows, krows), krows)]
        else:
            dst = whole[a].at[s]
        return pltpu.make_async_copy(shard[a], dst, lsem.at[a])

    for a in range(3):
        local_copy(a).start()

    head = gmap.shape[1]
    spread = (lax.rem(lax.broadcasted_iota(jnp.int32, (head, loc), 1), head)
              == lax.broadcasted_iota(jnp.int32, (head, loc), 0)).astype(BF16)
    diag = (lax.div(lax.broadcasted_iota(jnp.int32, (loc, loc), 0), head)
            == lax.div(lax.broadcasted_iota(jnp.int32, (loc, loc), 1), head))
    for i, m in enumerate((gmap, imap)):
        tiled = jnp.dot(m[...], spread, preferred_element_type=F32)
        bd[i] = jnp.where(diag, tiled, 0.0).astype(BF16)

    for i in range(2):
        halo_copy(i).wait()
    first = s == 0
    xpad[pl.ds(0, 8)] = halo[...].astype(F32)[8:16]
    idpad[pl.ds(0, 8)] = jnp.where(first, -1, ihalo[...])

    def fill(i, _):
        r = pl.multiple_of(i * CH, CH)
        xpad[pl.ds(pl.multiple_of(r + 8, 8), CH)] = recur[pl.ds(r, CH)].astype(F32)
        idpad[pl.ds(pl.multiple_of(r + 8, 8), CH)] = ids[pl.ds(r, CH)]
        return 0

    lax.fori_loop(0, tok // CH, fill, 0)
    reps = loc // 128
    ntaps = taps.shape[0]

    def front(i, _):
        r = pl.multiple_of(i * CH, CH)
        xw = xpad[pl.ds(r, CH + 8)]
        iw = idpad[pl.ds(r, CH + 8)]
        mine = iw[8:]
        tw = taps[...]
        conv = xw[8:] * tw[0:1]
        cont = None
        for k in range(1, ntaps):
            same1 = (pltpu.roll(iw, k, axis=0)[8:] == mine).astype(F32)
            same = jnp.concatenate([same1] * reps, axis=1)
            if k == 1:
                cont = same
            conv = conv + same * pltpu.roll(xw, k, axis=0)[8:] * tw[k:k + 1]
        cb = conv.astype(BF16)
        rg = jax.nn.sigmoid(jnp.dot(cb, bd[0], preferred_element_type=F32))
        ig = jax.nn.sigmoid(jnp.dot(cb, bd[1], preferred_element_type=F32))
        ld = rate[...] * rg + extra[pl.ds(r, CH)]
        fac[pl.ds(r, CH)] = jnp.exp(ld) * cont
        drv[pl.ds(r, CH)] = jnp.sqrt(one_minus_exp(2.0 * ld)) * ig * cb.astype(F32)
        return 0

    lax.fori_loop(0, tok // CH, front, 0)

    rows8 = lax.broadcasted_iota(jnp.int32, (8, loc), 0)

    def scan(i, carry):
        pc, hc = carry
        r = pl.multiple_of(i * 8, 8)
        a, b = fac[pl.ds(r, 8)], drv[pl.ds(r, 8)]
        for sh in (1, 2, 4):
            keep = rows8 >= sh
            b = b + a * jnp.where(keep, pltpu.roll(b, sh, axis=0), 0.0)
            a = a * jnp.where(keep, pltpu.roll(a, sh, axis=0), 1.0)
        h = b + a * hc
        p = a * pc
        fac[pl.ds(r, 8)] = p
        drv[pl.ds(r, 8)] = h
        return (jnp.broadcast_to(p[7:8], (8, loc)), jnp.broadcast_to(h[7:8], (8, loc)))

    pend, hend = lax.fori_loop(0, tok // 8, scan, (jnp.ones((8, loc), F32), jnp.zeros((8, loc), F32)))
    ends[s] = jnp.concatenate([pend, hend], axis=0)

    def end_copy(j):
        return pltpu.make_async_remote_copy(
            src_ref=ends.at[s], dst_ref=ends.at[s], send_sem=esend.at[j - 1], recv_sem=erecv.at[j - 1],
            device_id=(lax.rem(s + j, n), t), device_id_type=MESH)

    def end_arrived(j):
        o = lax.rem(s + n - j, n)
        pltpu.make_async_remote_copy(
            src_ref=ends.at[o], dst_ref=ends.at[o], send_sem=esend.at[j - 1], recv_sem=erecv.at[j - 1],
            device_id=(lax.rem(s + j, n), t), device_id_type=MESH).wait_recv()

    for j in range(1, n):
        end_copy(j).start()
    serve((0, 1), 0)
    for j in range(1, n):
        end_arrived(j)
    carry = jnp.zeros((8, loc), F32)
    for o in range(n - 1):
        e = ends[o]
        carry = jnp.where(o < s, e[:8] * carry + e[8:], carry)
    cin = carry[0:1]

    def branch(i, _):
        r = pl.multiple_of(i * CH, CH)
        st = drv[pl.ds(r, CH)] + fac[pl.ds(r, CH)] * cin
        bfull[t, pl.ds(r, CH)] = (st * jax.nn.gelu(gate_branch[pl.ds(r, CH)].astype(F32))).astype(BF16)
        return 0

    lax.fori_loop(0, tok // CH, branch, 0)

    def tp_push(view, send, recv, j, start):
        o = t if start else lax.rem(t + ntp - j, ntp)
        return pltpu.make_async_remote_copy(
            src_ref=view(o), dst_ref=view(o), send_sem=send.at[j - 1], recv_sem=recv.at[j - 1],
            device_id=(s, lax.rem(t + j, ntp)), device_id_type=MESH)

    def bview(o):
        return bfull.at[o]

    chips = ntp // 2
    core = lax.rem(t, 2)
    mate = t + 1 - 2 * core

    def far(view, send, recv, c, start):
        o = t if start else lax.rem(t + ntp - 2 * c, ntp)
        return pltpu.make_async_remote_copy(
            src_ref=view(o), dst_ref=view(o), send_sem=send.at[c - 1], recv_sem=recv.at[c - 1],
            device_id=(s, lax.rem(t + 2 * c, ntp)), device_id_type=MESH)

    def near(view, send, recv, c, start):
        base = t if start else mate
        o = lax.rem(base + ntp - 2 * c, ntp)
        return pltpu.make_async_remote_copy(
            src_ref=view(o), dst_ref=view(o), send_sem=send.at[chips - 1 + c], recv_sem=recv.at[chips - 1 + c],
            device_id=(s, mate), device_id_type=MESH)

    def gather_start(view, send, recv):
        for c in range(1, chips):
            far(view, send, recv, c, True).start()
        near(view, send, recv, 0, True).start()

    def gather_share(view, send, recv):
        for c in range(1, chips):
            far(view, send, recv, c, False).wait_recv()
            near(view, send, recv, c, True).start()

    def gather_wait(view, send, recv):
        for c in range(chips):
            near(view, send, recv, c, False).wait_recv()

    def gather_sent(view, send, recv):
        for c in range(1, chips):
            far(view, send, recv, c, True).wait_send()
        for c in range(chips):
            near(view, send, recv, c, True).wait_send()

    gather_start(bview, bsend, brecv)
    serve((0, 1), 1)
    gather_share(bview, bsend, brecv)
    gather_wait(bview, bsend, brecv)

    def row_total(q, values):
        def write(i, _):
            r = pl.multiple_of(i * BR, BR)
            v = values(r)
            c = jnp.sum(v * v, axis=1, keepdims=True)
            ssq[q, t, :, pl.ds(r, BR)] = jnp.transpose(jnp.broadcast_to(c, (BR, 128)))[:8]
            return 0

        lax.fori_loop(0, tok // BR, write, 0)
        for j in range(1, ntp):
            tp_push(lambda o: ssq.at[q, o], qsend.at[q], qrecv.at[q], j, True).start()

    def wait_total(q):
        for j in range(1, ntp):
            tp_push(lambda o: ssq.at[q, o], qsend.at[q], qrecv.at[q], j, False).wait_recv()

    def inverse_rms(q, r):
        row = ssq[q, 0, 0:1, pl.ds(r, BR)]
        for o in range(1, ntp):
            row = row + ssq[q, o, 0:1, pl.ds(r, BR)]
        inv = lax.rsqrt(row / width + EPS)
        return jnp.transpose(jnp.broadcast_to(inv, (128, BR)))[:, 0:1]

    def project(i, _):
        r = pl.multiple_of(i * BR, BR)
        total = jnp.zeros((BR, dloc), F32)
        for o in range(ntp):
            total += jnp.dot(bfull[o, pl.ds(r, BR)], out_w[pl.ds(o * loc, loc)], preferred_element_type=F32)
        mixed[pl.ds(r, BR)] = total.astype(BF16)
        return 0

    lax.fori_loop(0, tok // BR, project, 0)
    row_total(0, lambda r: mixed[pl.ds(r, BR)].astype(F32))
    wait_total(0)

    def stream(i, _):
        r = pl.multiple_of(i * BR, BR)
        m = mixed[pl.ds(r, BR)].astype(F32)
        mixed[pl.ds(r, BR)] = (residual[pl.ds(r, BR)].astype(F32) + m * inverse_rms(0, r) * mix_gain[...]).astype(BF16)
        return 0

    lax.fori_loop(0, tok // BR, stream, 0)
    row_total(1, lambda r: mixed[pl.ds(r, BR)].astype(F32))
    serve((0, 1), 2)
    wait_total(1)

    def norm(i, _):
        r = pl.multiple_of(i * BR, BR)
        m = mixed[pl.ds(r, BR)].astype(F32)
        normed[pl.ds(r, BR), pl.ds(pl.multiple_of(t * dloc, dloc), dloc)] = (m * inverse_rms(1, r) * pre_gain[...]).astype(BF16)
        return 0

    lax.fori_loop(0, tok // BR, norm, 0)

    def nview(o):
        return normed.at[:, pl.ds(pl.multiple_of(o * dloc, dloc), dloc)]

    gather_start(nview, nsend, nrecv)
    serve((0, 1), 3)
    gather_share(nview, nsend, nrecv)
    for k in range(4, n - 2):
        serve((0, 1), k)
    serve((2,), 0)
    serve((0, 1), n - 2)
    gather_wait(nview, nsend, nrecv)
    for a in range(3):
        local_copy(a).wait()

    def ffn_tile(c, size):
        cols = pl.ds(c, size)
        g = jnp.dot(normed[...], gate_all[:, cols], preferred_element_type=F32)
        u = jnp.dot(normed[...], up_all[:, cols], preferred_element_type=F32)
        hidden[:, cols] = (jax.nn.silu(g) * u).astype(BF16)

    TN = 256
    tiles = ff // TN

    def ffn_step(j, _):
        ffn_tile(pl.multiple_of(j * TN, TN), TN)
        return 0

    cut = (tiles + 1) // 2
    lax.fori_loop(0, cut, ffn_step, 0)
    serve((2,), 1)
    lax.fori_loop(cut, tiles, ffn_step, 0)
    if ff % TN:
        ffn_tile(tiles * TN, ff % TN)

    per = dloc // ncol

    def place(o):
        c = lax.div(o, per)
        w = lax.rem(o, per)
        gap = lax.rem(lax.div(c, 2) - lax.div(t, 2) + chips, chips)
        return lax.rem(c, 2), w, c, gap

    def mate_copy(i):
        return pltpu.make_async_remote_copy(
            src_ref=partial.at[i], dst_ref=shared.at[i], send_sem=psend.at[i], recv_sem=msem.at[i],
            device_id=(s, mate), device_id_type=MESH)

    def far_copy(i, w, c, gap):
        g = lax.rem(gap + chips - 1, chips)
        return pltpu.make_async_remote_copy(
            src_ref=partial.at[i], dst_ref=recvd.at[g, w], send_sem=psend.at[i], recv_sem=precv.at[g, w],
            device_id=(s, c), device_id_type=MESH)

    sent = []

    def down(*blocks):
        for o in blocks:
            i = len(sent)
            sent.append(o)
            partial[i] = jnp.dot(hidden[...], down_all[o], preferred_element_type=F32).astype(BF16)
            par, w, c, gap = place(o)

            @pl.when(par != core)
            def _():
                mate_copy(i).start()

    def join(i):
        par, w, c, gap = place(sent[i])

        @pl.when(par == core)
        def _():
            mate_copy(i).wait_recv()

            def add(b, _):
                r = pl.multiple_of(b * BR, BR)
                total = partial[i, pl.ds(r, BR)].astype(F32) + shared[i, pl.ds(r, BR)].astype(F32)
                partial[i, pl.ds(r, BR)] = total.astype(BF16)
                return 0

            lax.fori_loop(0, tok // BR, add, 0)

            @pl.when(gap == 0)
            def _():
                own[w] = partial[i]

            @pl.when(gap != 0)
            def _():
                far_copy(i, w, c, gap).start()

    down(s)
    joined = 0
    for k in range(2, n - 1):
        serve((2,), k)
        have = k + 1
        if 2 * have >= n:
            if 2 * have == n:
                down(origin[0][have])
            else:
                down(origin[0][have], origin[0][n - have])
        if k == n - 2:
            upto = len(sent)
        else:
            upto = len(sent) - (1 if 2 * have == n else 2) if 2 * have >= n else len(sent)
        while joined < upto:
            join(joined)
            joined += 1

    for i, o in enumerate(sent):
        par, w, c, gap = place(o)

        @pl.when(par != core)
        def _():
            mate_copy(i).wait_send()

        @pl.when(par == core)
        def _():
            @pl.when(gap != 0)
            def _():
                far_copy(i, w, c, gap).wait_send()

    for g in range(1, chips):
        for w in range(per):
            pltpu.make_async_remote_copy(
                src_ref=partial.at[0], dst_ref=recvd.at[g - 1, w],
                send_sem=psend.at[0], recv_sem=precv.at[g - 1, w],
                device_id=(s, mate), device_id_type=MESH).wait_recv()

    def gather_sum(i, _):
        r = pl.multiple_of(i * BR, BR)
        for w in range(per):
            total = own[w, pl.ds(r, BR)].astype(F32)
            for j in range(chips - 1):
                total = total + recvd[j, w, pl.ds(r, BR)].astype(F32)
            out[pl.ds(r, BR), pl.ds(w * ncol, ncol)] = total.astype(BF16)
        return 0

    lax.fori_loop(0, tok // BR, gather_sum, 0)
    row_total(2, lambda r: out[pl.ds(r, BR)].astype(F32))
    wait_total(2)

    def finish(i, _):
        r = pl.multiple_of(i * BR, BR)
        f = out[pl.ds(r, BR)].astype(F32)
        out[pl.ds(r, BR)] = (mixed[pl.ds(r, BR)].astype(F32) + f * inverse_rms(2, r) * ffn_gain[...]).astype(BF16)
        return 0

    lax.fori_loop(0, tok // BR, finish, 0)

    for a in range(3):
        for d in range(2):
            for k in range(n - 1):
                ring(a, d, k).wait_send()
    for j in range(1, n):
        end_copy(j).wait_send()
    gather_sent(bview, bsend, brecv)
    gather_sent(nview, nsend, nrecv)
    for j in range(1, ntp):
        for q in range(3):
            tp_push(lambda o: ssq.at[q, o], qsend.at[q], qrecv.at[q], j, True).wait_send()


def plane_kernel(
    cfg,
    gate_branch_in, recur_in, ids, taps, gmap, imap, level, extra_in, out_w_in, residual_in,
    mix_gain, pre_gain, ffn_gain, gate_w, up_w, down_w,
    out_hbm,
    out, osem, gate_branch, recur, extra, out_w, residual, insem,
    gate_all, up_all, down_all, xpad, idpad, halo, ihalo, bd, fac, drv, ends, bfull,
    mixed, nloc, gloc, normed, gnormed, ghid, gsum, usum, hidden, partial, recvd, ssq,
    lsem, ssend, srecv, zsend, zrecv, msend, mrecv,
    hsend, hrecv, esend, erecv, bsend, brecv, nsend, nrecv, fsend, frecv, gsend, grecv, qsend, qrecv, psend, precv,
):
    n, ntp, nz, ny, width = cfg
    s, t = lax.axis_index("sp"), lax.axis_index("tp")
    tok, loc = recur.shape
    dloc = residual.shape[1]
    krows = gate_w.shape[0]
    ncol = down_w.shape[1]
    ff = gate_w.shape[1]
    CH = math.gcd(tok, 64)
    BR = math.gcd(tok, 128)
    chips = ntp // 2
    z, y = lax.div(s, ny), lax.rem(s, ny)
    x, core = lax.div(t, 2), lax.rem(t, 2)
    mate = t + 1 - 2 * core
    per = dloc // ncol

    barrier = pltpu.get_barrier_semaphore()
    peers = [(z * ny + lax.rem(y + dy, ny), lax.rem(t + dt, ntp)) for dy in range(ny) for dt in range(ntp)][1:]
    peers += [(lax.rem(z + dz, nz) * ny + lax.rem(y + dy, ny), t) for dz in range(1, nz) for dy in range(ny)]
    for p in peers:
        pl.semaphore_signal(barrier, inc=1, device_id=p, device_id_type=MESH)

    inputs = ((recur_in, recur), (extra_in, extra), (gate_branch_in, gate_branch), (out_w_in, out_w), (residual_in, residual))

    def load_input(i):
        return pltpu.make_async_copy(inputs[i][0], inputs[i][1], insem.at[i])

    for i in range(len(inputs)):
        load_input(i).start()
    pl.semaphore_wait(barrier, len(peers))

    low = (2 * z < nz).astype(jnp.int32)
    near_first = []
    for k in range(1, nz):
        near_first += [z + (2 * low - 1) * k, z - (2 * low - 1) * k]
    origin = [z]
    seen = 0
    ranks = []
    for q in near_first:
        ok = jnp.logical_and(q >= 0, q < nz).astype(jnp.int32)
        seen = seen + ok
        ranks.append((q, ok, seen))
    for j in range(1, nz):
        origin.append(sum(jnp.where(jnp.logical_and(ok == 1, r == j), q, 0) for q, ok, r in ranks))

    hcol = ncol // 2
    hrow = krows // 2
    GATE, UP, DOWN, WIDE = (0, 1), (2,), (3, 4), (5, 6)
    fa = ff - ghid.shape[1]
    main, side = pl.ds(0, fa), pl.ds(fa, ff - fa)
    inner = jnp.logical_and(z > 0, z < nz - 1)
    host = jnp.logical_or(z == 1, z == nz - 2)
    guest_z = jnp.where(z == 1, 0, nz - 1)
    host_z = jnp.where(z == 0, 1, nz - 2)

    def block(a, o, b):
        i = o * ny + b
        if a in GATE:
            return gate_all.at[pl.ds(pl.multiple_of(i * krows + a * hrow, hrow), hrow), main]
        if a in UP:
            return up_all.at[pl.ds(pl.multiple_of(i * krows, krows), krows), main]
        if a in WIDE:
            return (gate_all, up_all)[a - WIDE[0]].at[pl.ds(pl.multiple_of(i * krows, krows), krows), side]
        return down_all.at[i, :, pl.ds((a - DOWN[0]) * hcol, hcol)]

    def own_shard(a):
        if a in GATE:
            return gate_w.at[pl.ds(a * hrow, hrow), main]
        if a in UP:
            return up_w.at[:, main]
        if a in WIDE:
            return (gate_w, up_w)[a - WIDE[0]].at[:, side]
        return down_w.at[:, pl.ds((a - DOWN[0]) * hcol, hcol)]

    def seed_local(a):
        return pltpu.make_async_copy(own_shard(a), block(a, z, y), lsem.at[a])

    def seed_swap(a):
        return pltpu.make_async_remote_copy(
            src_ref=own_shard(a), dst_ref=block(a, z, y), send_sem=ssend.at[a], recv_sem=srecv.at[a],
            device_id=(z * ny + 1 - y, mate), device_id_type=MESH)

    def z_copy(a, o, up):
        b = block(a, o, core)
        return pltpu.make_async_remote_copy(
            src_ref=b, dst_ref=b, send_sem=zsend.at[up, a, o], recv_sem=zrecv.at[a, o],
            device_id=((z + 2 * up - 1) * ny + y, t), device_id_type=MESH)

    def mate_copy(a, o, theirs=False):
        b = block(a, o, 1 - core if theirs else core)
        return pltpu.make_async_remote_copy(
            src_ref=b, dst_ref=b, send_sem=msend.at[a, o], recv_sem=mrecv.at[a, o],
            device_id=(s, mate), device_id_type=MESH)

    def fan_down(a, o, act):
        @pl.when(jnp.logical_and(o >= z, z > (1 if a in WIDE else 0)))
        def _():
            act(z_copy(a, o, 0))

    def fan_up(a, o, act):
        @pl.when(jnp.logical_and(o <= z, z < nz - (2 if a in WIDE else 1)))
        def _():
            act(z_copy(a, o, 1))

    def fan(a, o, act):
        fan_down(a, o, act)
        fan_up(a, o, act)
        if a in WIDE:
            @pl.when(inner)
            def _():
                act(mate_copy(a, o))
        else:
            act(mate_copy(a, o))

    def start(c):
        c.start()

    def seed_ready(a):
        @pl.when(y == core)
        def _():
            seed_local(a).wait()

        @pl.when(y != core)
        def _():
            pltpu.make_async_remote_copy(
                src_ref=block(a, z, core), dst_ref=block(a, z, core), send_sem=ssend.at[a], recv_sem=srecv.at[a],
                device_id=(z * ny + 1 - y, mate), device_id_type=MESH).wait_recv()

    def push_seed(a):
        seed_ready(a)
        fan(a, z, start)

    def relay_from(a, o):
        z_copy(a, o, 0).wait_recv()
        fan(a, o, start)

    def relay(items, j):
        for a in items:
            relay_from(a, origin[j])

    def load_seed(a):
        @pl.when(y == core)
        def _():
            seed_local(a).start()

        @pl.when(y != core)
        def _():
            seed_swap(a).start()

    def halo_copy(i):
        src, dst = ((recur_in.at[pl.ds(tok - 16, 16)], halo), (ids, ihalo))[i]
        return pltpu.make_async_remote_copy(
            src_ref=src, dst_ref=dst, send_sem=hsend.at[i], recv_sem=hrecv.at[i],
            device_id=(lax.rem(s + 1, n), t), device_id_type=MESH)

    for i in range(2):
        halo_copy(i).start()

    for a in GATE:
        load_seed(a)

    @pl.when(y == core)
    def _():
        for a in GATE:
            push_seed(a)

    head = gmap.shape[1]
    spread = (lax.rem(lax.broadcasted_iota(jnp.int32, (head, loc), 1), head)
              == lax.broadcasted_iota(jnp.int32, (head, loc), 0)).astype(BF16)
    diag = (lax.div(lax.broadcasted_iota(jnp.int32, (loc, loc), 0), head)
            == lax.div(lax.broadcasted_iota(jnp.int32, (loc, loc), 1), head))
    for i, m in enumerate((gmap, imap)):
        tiled = jnp.dot(m[...], spread, preferred_element_type=F32)
        bd[i] = jnp.where(diag, tiled, 0.0).astype(BF16)

    for i in range(2):
        load_input(i).wait()

    def down_rows(row):
        return jnp.transpose(jnp.broadcast_to(row, (128, 128)))

    for i in range(tok // 128):
        idpad[pl.ds(8 + i * 128, 128)] = down_rows(ids[i:i + 1])

    def fill(i, _):
        r = pl.multiple_of(i * CH, CH)
        xpad[pl.ds(pl.multiple_of(r + 8, 8), CH)] = recur[pl.ds(r, CH)].astype(F32)
        return 0

    lax.fori_loop(0, tok // CH, fill, 0)
    u = -level[...]
    rate = -GATE_POWER * (jnp.maximum(u, 0.0) + jnp.log1p(jnp.exp(-jnp.abs(u))))
    for i in range(2):
        halo_copy(i).wait()
    first = s == 0
    xpad[pl.ds(0, 8)] = halo[...].astype(F32)[8:16]
    idpad[pl.ds(0, 8)] = jnp.where(first, -1, down_rows(ihalo[tok // 128 - 1:tok // 128])[120:])
    reps = loc // 128
    ntaps = taps.shape[0]

    def front(i, _):
        r = pl.multiple_of(i * CH, CH)
        xw = xpad[pl.ds(r, CH + 8)]
        iw = idpad[pl.ds(r, CH + 8)]
        mine = iw[8:]
        tw = taps[...].astype(F32)
        conv = xw[8:] * tw[0:1]
        cont = None
        for k in range(1, ntaps):
            same1 = (pltpu.roll(iw, k, axis=0)[8:] == mine).astype(F32)
            same = jnp.concatenate([same1] * reps, axis=1)
            if k == 1:
                cont = same
            conv = conv + same * pltpu.roll(xw, k, axis=0)[8:] * tw[k:k + 1]
        cb = conv.astype(BF16)
        rg = jax.nn.sigmoid(jnp.dot(cb, bd[0], preferred_element_type=F32))
        ig = jax.nn.sigmoid(jnp.dot(cb, bd[1], preferred_element_type=F32))
        ld = rate * rg + extra[pl.ds(r, CH)]
        fac[pl.ds(r, CH)] = jnp.exp(ld) * cont
        drv[pl.ds(r, CH)] = jnp.sqrt(one_minus_exp(2.0 * ld)) * ig * cb.astype(F32)
        return 0

    lax.fori_loop(0, tok // CH, front, 0)

    @pl.when(y == core)
    def _():
        for a in UP + WIDE:
            load_seed(a)

    rows8 = lax.broadcasted_iota(jnp.int32, (8, loc), 0)

    def scan(i, carry):
        pc, hc = carry
        r = pl.multiple_of(i * 8, 8)
        a, b = fac[pl.ds(r, 8)], drv[pl.ds(r, 8)]
        for sh in (1, 2, 4):
            keep = rows8 >= sh
            b = b + a * jnp.where(keep, pltpu.roll(b, sh, axis=0), 0.0)
            a = a * jnp.where(keep, pltpu.roll(a, sh, axis=0), 1.0)
        h = b + a * hc
        p = a * pc
        fac[pl.ds(r, 8)] = p
        drv[pl.ds(r, 8)] = h
        return (jnp.broadcast_to(p[7:8], (8, loc)), jnp.broadcast_to(h[7:8], (8, loc)))

    pend, hend = lax.fori_loop(0, tok // 8, scan, (jnp.ones((8, loc), F32), jnp.zeros((8, loc), F32)))
    ends[s] = jnp.concatenate([pend, hend], axis=0)

    def end_copy(j):
        return pltpu.make_async_remote_copy(
            src_ref=ends.at[s], dst_ref=ends.at[s], send_sem=esend.at[j - 1], recv_sem=erecv.at[j - 1],
            device_id=(lax.rem(s + j, n), t), device_id_type=MESH)

    def end_arrived(j):
        o = lax.rem(s + n - j, n)
        pltpu.make_async_remote_copy(
            src_ref=ends.at[o], dst_ref=ends.at[o], send_sem=esend.at[j - 1], recv_sem=erecv.at[j - 1],
            device_id=(lax.rem(s + j, n), t), device_id_type=MESH).wait_recv()

    for j in range(1, n):
        end_copy(j).start()

    @pl.when(y != core)
    def _():
        for a in GATE:
            push_seed(a)
        for a in UP + WIDE:
            load_seed(a)

    for a in DOWN:
        load_seed(a)

    @pl.when(y == core)
    def _():
        for a in UP + WIDE:
            push_seed(a)

    early = min(2, nz - 1)
    for j in range(1, n):
        end_arrived(j)
    carry = jnp.zeros((8, loc), F32)
    for o in range(n - 1):
        e = ends[o]
        carry = jnp.where(o < s, e[:8] * carry + e[8:], carry)
    cin = carry[0:1]

    for i in range(2, len(inputs)):
        load_input(i).wait()

    def branch(i, _):
        r = pl.multiple_of(i * CH, CH)
        st = drv[pl.ds(r, CH)] + fac[pl.ds(r, CH)] * cin
        bfull[t, pl.ds(r, CH)] = (st * jax.nn.gelu(gate_branch[pl.ds(r, CH)].astype(F32))).astype(BF16)
        return 0

    lax.fori_loop(0, tok // CH, branch, 0)

    def tp_push(view, send, recv, j, start):
        o = t if start else lax.rem(t + ntp - j, ntp)
        return pltpu.make_async_remote_copy(
            src_ref=view(o), dst_ref=view(o), send_sem=send.at[j - 1], recv_sem=recv.at[j - 1],
            device_id=(s, lax.rem(t + j, ntp)), device_id_type=MESH)

    def bview(o):
        return bfull.at[o]

    chips = ntp // 2
    core = lax.rem(t, 2)
    mate = t + 1 - 2 * core

    def far(view, send, recv, c, start):
        o = t if start else lax.rem(t + ntp - 2 * c, ntp)
        return pltpu.make_async_remote_copy(
            src_ref=view(o), dst_ref=view(o), send_sem=send.at[c - 1], recv_sem=recv.at[c - 1],
            device_id=(s, lax.rem(t + 2 * c, ntp)), device_id_type=MESH)

    def near(view, send, recv, c, start):
        base = t if start else mate
        o = lax.rem(base + ntp - 2 * c, ntp)
        return pltpu.make_async_remote_copy(
            src_ref=view(o), dst_ref=view(o), send_sem=send.at[chips - 1 + c], recv_sem=recv.at[chips - 1 + c],
            device_id=(s, mate), device_id_type=MESH)

    def gather_start(view, send, recv):
        for c in range(1, chips):
            far(view, send, recv, c, True).start()
        near(view, send, recv, 0, True).start()

    def gather_share(view, send, recv):
        for c in range(1, chips):
            far(view, send, recv, c, False).wait_recv()
            near(view, send, recv, c, True).start()

    def gather_wait(view, send, recv):
        for c in range(chips):
            near(view, send, recv, c, False).wait_recv()

    def gather_sent(view, send, recv):
        for c in range(1, chips):
            far(view, send, recv, c, True).wait_send()
        for c in range(chips):
            near(view, send, recv, c, True).wait_send()

    gather_start(bview, bsend, brecv)

    @pl.when(y != core)
    def _():
        for a in UP + WIDE:
            push_seed(a)

    gather_share(bview, bsend, brecv)
    gather_wait(bview, bsend, brecv)

    def row_total(q, values):
        def write(i, _):
            r = pl.multiple_of(i * BR, BR)
            v = values(r)
            c = jnp.sum(v * v, axis=1, keepdims=True)
            ssq[q, t, :, pl.ds(r, BR)] = jnp.transpose(jnp.broadcast_to(c, (BR, 128)))[:8]
            return 0

        lax.fori_loop(0, tok // BR, write, 0, unroll=True)
        for j in range(1, ntp):
            tp_push(lambda o: ssq.at[q, o], qsend.at[q], qrecv.at[q], j, True).start()

    def wait_total(q):
        for j in range(1, ntp):
            tp_push(lambda o: ssq.at[q, o], qsend.at[q], qrecv.at[q], j, False).wait_recv()

    def inverse_rms(q, r):
        row = ssq[q, 0, 0:1, pl.ds(r, BR)]
        for o in range(1, ntp):
            row = row + ssq[q, o, 0:1, pl.ds(r, BR)]
        inv = lax.rsqrt(row / width + EPS)
        return jnp.transpose(jnp.broadcast_to(inv, (128, BR)))[:, 0:1]

    def project(i, _):
        r = pl.multiple_of(i * BR, BR)
        total = jnp.zeros((BR, dloc), F32)
        for o in range(ntp):
            total += jnp.dot(bfull[o, pl.ds(r, BR)], out_w[pl.ds(o * loc, loc)], preferred_element_type=F32)
        mixed[pl.ds(r, BR)] = total.astype(BF16)
        return 0

    lax.fori_loop(0, tok // BR, project, 0)
    row_total(0, lambda r: mixed[pl.ds(r, BR)].astype(F32))

    @pl.when(inner)
    def _():
        for j in range(1, early + 1):
            relay(GATE, j)

    wait_total(0)

    def stream(i, _):
        r = pl.multiple_of(i * BR, BR)
        m = mixed[pl.ds(r, BR)].astype(F32)
        mixed[pl.ds(r, BR)] = (residual[pl.ds(r, BR)].astype(F32) + m * inverse_rms(0, r) * mix_gain[...]).astype(BF16)
        return 0

    lax.fori_loop(0, tok // BR, stream, 0, unroll=True)
    row_total(1, lambda r: mixed[pl.ds(r, BR)].astype(F32))
    wait_total(1)

    cols = pl.ds(pl.multiple_of(t * dloc, dloc), dloc)

    def norm(i, _):
        r = pl.multiple_of(i * BR, BR)
        m = mixed[pl.ds(r, BR)].astype(F32)
        v = (m * inverse_rms(1, r) * pre_gain[...]).astype(BF16)
        nloc[pl.ds(r, BR)] = v

        @pl.when(y == core)
        def _():
            normed[pl.ds(r, BR), cols] = v

        return 0

    lax.fori_loop(0, tok // BR, norm, 0, unroll=True)
    htok = tok // 2
    piece, spot = (nloc, gloc), (normed, gnormed)

    def n_copy(q, dy, dx):
        return pltpu.make_async_remote_copy(
            src_ref=piece[q], dst_ref=spot[q].at[:, cols], send_sem=nsend.at[q, dy, dx], recv_sem=nrecv.at[q, t],
            device_id=(z * ny + lax.rem(y + dy, ny), 2 * lax.rem(x + dx, chips) + y), device_id_type=MESH)

    def to_plane(q, act):
        for dx in range(1, chips):
            act(n_copy(q, 0, dx))
        for dy in range(1, ny):
            act(n_copy(q, dy, 0))

        @pl.when(y != core)
        def _():
            act(n_copy(q, 0, 0))

    def n_wait(q, o):
        view = spot[q].at[:, pl.ds(pl.multiple_of(o * dloc, dloc), dloc)]
        pltpu.make_async_remote_copy(
            src_ref=view, dst_ref=view, send_sem=nsend.at[q, 0, 0], recv_sem=nrecv.at[q, o],
            device_id=(s, mate), device_id_type=MESH).wait_recv()

    def f_copy(q, o, h, device):
        view = spot[q].at[pl.ds(h * htok, htok), pl.ds(pl.multiple_of(o * dloc, dloc), dloc)]
        return pltpu.make_async_remote_copy(
            src_ref=view, dst_ref=view, send_sem=fsend.at[q, lax.rem(o, 2)], recv_sem=frecv.at[q, h, o],
            device_id=device, device_id_type=MESH)

    other = 1 - x

    def forward(q, act, wait):
        for e in range(2):
            @pl.when(y == core)
            def _():
                o = 2 * other + e
                if wait:
                    n_wait(q, o)
                act(f_copy(q, o, 0, (z * ny + 1 - y, t)))

            @pl.when(y != core)
            def _():
                o = 2 * x + e
                if wait:
                    n_wait(q, o)
                act(f_copy(q, o, 1, (s, 2 * other + core)))

    def n_ready(q):
        @pl.when(y == core)
        def _():
            n_wait(q, mate)

        @pl.when(y != core)
        def _():
            for e in range(2):
                for h in range(2):
                    f_copy(q, 2 * other + e, h, (s, mate)).wait_recv()

    def guest_hop():
        return pltpu.make_async_remote_copy(
            src_ref=nloc, dst_ref=gloc, send_sem=gsend.at[0], recv_sem=grecv.at[0],
            device_id=(host_z * ny + y, t), device_id_type=MESH)

    def guest_return():
        return pltpu.make_async_remote_copy(
            src_ref=ghid, dst_ref=hidden.at[:, side], send_sem=gsend.at[1], recv_sem=grecv.at[1],
            device_id=(guest_z * ny + y, t), device_id_type=MESH)

    to_plane(0, start)

    @pl.when(jnp.logical_not(inner))
    def _():
        guest_hop().start()
        for a in DOWN:
            push_seed(a)

    @pl.when(inner)
    def _():
        for j in range(1, early + 1):
            relay(UP, j)
            relay(WIDE, j)

    forward(0, start, True)

    @pl.when(host)
    def _():
        guest_hop().wait_recv()

        @pl.when(y == core)
        def _():
            gnormed[:, cols] = gloc[...]

        to_plane(1, start)

    @pl.when(jnp.logical_not(inner))
    def _():
        for j in range(1, early + 1):
            relay(GATE, j)
            relay(UP, j)

    def outward_seed(items):
        for a in items:
            @pl.when(low == 1)
            def _():
                fan_down(a, z, start)

            @pl.when(low == 0)
            def _():
                fan_up(a, z, start)

    def mates(items, js):
        for j in js:
            for a in items:
                mate_copy(a, origin[j], True).wait_recv()

    kblk = ny * krows
    TN = 256
    def sums(js, cs):
        g = u = None
        for j in js:
            k = pl.ds(pl.multiple_of(origin[j] * kblk, kblk), kblk)
            a = normed[:, k]
            gj = jnp.dot(a, gate_all[k, cs], preferred_element_type=F32)
            uj = jnp.dot(a, up_all[k, cs], preferred_element_type=F32)
            g, u = (gj, uj) if g is None else (g + gj, u + uj)
        return g, u

    def first_tile(c, size):
        cs = pl.ds(c, size)
        gsum[:, cs], usum[:, cs] = sums(range(nz - 1), cs)

    def last_tile(c, size):
        cs = pl.ds(c, size)
        g, u = sums((nz - 1,), cs)
        g, u = g + gsum[:, cs], u + usum[:, cs]
        hidden[:, cs] = (jax.nn.silu(g) * u).astype(BF16)

    def over_tiles(tile):
        def step(j, _):
            tile(pl.multiple_of(j * TN, TN), TN)
            return 0

        lax.fori_loop(0, fa // TN, step, 0)
        if fa % TN:
            tile(fa // TN * TN, fa % TN)

        @pl.when(inner)
        def _():
            tile(fa, ff - fa)

    @pl.when(inner)
    def _():
        for j in range(early + 1, nz):
            relay(GATE, j)
            relay(UP, j)
            relay(WIDE, j)
        for a in DOWN:
            seed_ready(a)
            mate_copy(a, z).start()

            @pl.when(low == 1)
            def _():
                fan_up(a, z, start)

            @pl.when(low == 0)
            def _():
                fan_down(a, z, start)

        outward_seed(DOWN[:1])
        relay(DOWN, 2)

    n_ready(0)
    mates(GATE + UP, range(nz - 1))

    @pl.when(inner)
    def _():
        mates(WIDE, range(nz - 1))

    over_tiles(first_tile)

    @pl.when(host)
    def _():
        forward(1, start, True)

    @pl.when(jnp.logical_not(inner))
    def _():
        for j in range(early + 1, nz):
            relay(GATE, j)
            relay(UP, j)

    mates(GATE + UP, (nz - 1,))

    @pl.when(inner)
    def _():
        mates(WIDE, (nz - 1,))

    over_tiles(last_tile)

    @pl.when(host)
    def _():
        n_ready(1)
        g = jnp.dot(gnormed[...], gate_all[:, side], preferred_element_type=F32)
        v = jnp.dot(gnormed[...], up_all[:, side], preferred_element_type=F32)
        ghid[...] = (jax.nn.silu(g) * v).astype(BF16)
        guest_return().start()

    @pl.when(jnp.logical_not(inner))
    def _():
        guest_return().wait_recv()

    me = y * chips + x

    def p_copy(i, h):
        c = pl.ds(h * hcol, hcol)
        return pltpu.make_async_remote_copy(
            src_ref=partial.at[i, :, c], dst_ref=recvd.at[me, lax.rem(i, per), :, c], send_sem=psend.at[i, h],
            recv_sem=precv.at[me, lax.rem(i, per), h],
            device_id=(z * ny + core, lax.div(i, per)), device_id_type=MESH)

    def owned(i):
        return jnp.logical_and(y == core, lax.div(i, per) == t)

    def ship(i, hs):
        @pl.when(owned(i))
        def _():
            for h in hs:
                c = pl.ds(h * hcol, hcol)
                recvd[me, lax.rem(i, per), :, c] = partial[i, :, c]

        @pl.when(jnp.logical_not(owned(i)))
        def _():
            for h in hs:
                p_copy(i, h).start()

    def mate_ready(a, o, b):
        @pl.when(b != core)
        def _():
            mate_copy(a, o, True).wait_recv()

    last = nz - 1
    ends_order = [0] + list(range(2, nz)) + [1]
    line = [jnp.where(inner, origin[j], origin[ends_order[j]]) for j in range(nz)]
    roles = (y, 1 - y)

    def bring(j, k, items):
        @pl.when(jnp.logical_and(roles[k] == core, jnp.logical_not(inner) if j == 2 else True))
        def _():
            for a in items:
                relay_from(a, line[j])

    def whole_block(j, k):
        i = line[j] * ny + roles[k]
        for a in DOWN:
            mate_ready(a, line[j], roles[k])
        partial[i] = jnp.dot(hidden[...], down_all[i], preferred_element_type=F32).astype(BF16)
        ship(i, (0, 1))

    def half_block(j, k, h):
        i = line[j] * ny + roles[k]
        c = pl.ds(h * hcol, hcol)
        mate_ready(DOWN[h], line[j], roles[k])
        partial[i, :, c] = jnp.dot(hidden[...], down_all[i, :, c], preferred_element_type=F32).astype(BF16)
        ship(i, (h,))

    def outward_rest(k):
        @pl.when(jnp.logical_and(inner, roles[k] == core))
        def _():
            outward_seed(DOWN[1:])

    @pl.when(jnp.logical_not(inner))
    def _():
        for k in range(2):
            bring(last, k, DOWN[:1])

    for k in range(2):
        whole_block(0, k)
    bring(1, 0, DOWN)
    whole_block(1, 0)
    bring(1, 1, DOWN)
    whole_block(1, 1)

    @pl.when(inner)
    def _():
        for k in range(2):
            bring(last, k, DOWN[:1])

    for k in range(2):
        half_block(last, k, 0)
    for j in range(2, last):
        bring(j, 0, DOWN)
        bring(j, 1, DOWN[:1])
        whole_block(j, 0)
    for j in range(2, last):
        half_block(j, 1, 0)
        if j == last - 1:
            bring(last, 0, DOWN[1:])
            outward_rest(0)
        bring(j, 1, DOWN[1:])
        half_block(j, 1, 1)
    bring(last, 1, DOWN[1:])
    outward_rest(1)
    for k in range(2):
        half_block(last, k, 1)

    def p_wait(dy, dx):
        k = lax.rem(y + dy, ny) * chips + lax.rem(x + dx, chips)
        for w in range(per):
            for h in range(2):
                view = recvd.at[k, w, :, pl.ds(h * hcol, hcol)]
                pltpu.make_async_remote_copy(
                    src_ref=view, dst_ref=view, send_sem=psend.at[0, 0], recv_sem=precv.at[k, w, h],
                    device_id=(s, mate), device_id_type=MESH).wait_recv()

    for dy in range(ny):
        for dx in range(chips):
            if dy or dx:
                p_wait(dy, dx)

    @pl.when(y != core)
    def _():
        p_wait(0, 0)

    def ffn_rows(r):
        for w in range(per):
            total = recvd[0, w, pl.ds(r, BR)].astype(F32)
            for k in range(1, ny * chips):
                total = total + recvd[k, w, pl.ds(r, BR)].astype(F32)
            out[pl.ds(r, BR), pl.ds(w * ncol, ncol)] = total.astype(BF16)
        return out[pl.ds(r, BR)].astype(F32)

    row_total(2, ffn_rows)
    wait_total(2)

    def out_copy(i):
        rows = pl.ds(pl.multiple_of(i * BR, BR), BR)
        return pltpu.make_async_copy(out.at[rows], out_hbm.at[rows], osem.at[i])

    def finish(i, _):
        r = pl.multiple_of(i * BR, BR)
        f = out[pl.ds(r, BR)].astype(F32)
        out[pl.ds(r, BR)] = (mixed[pl.ds(r, BR)].astype(F32) + f * inverse_rms(2, r) * ffn_gain[...]).astype(BF16)
        out_copy(i).start()
        return 0

    lax.fori_loop(0, tok // BR, finish, 0, unroll=True)

    def sent(c):
        c.wait_send()

    for a in GATE + UP + DOWN + WIDE:
        @pl.when(y != core)
        def _():
            seed_swap(a).wait_send()

        for j in range(nz):
            fan(a, origin[j], sent)
    for j in range(1, n):
        end_copy(j).wait_send()
    gather_sent(bview, bsend, brecv)
    to_plane(0, sent)
    forward(0, sent, False)

    @pl.when(host)
    def _():
        to_plane(1, sent)
        forward(1, sent, False)
        guest_return().wait_send()

    @pl.when(jnp.logical_not(inner))
    def _():
        guest_hop().wait_send()

    for i in range(n):
        @pl.when(jnp.logical_not(owned(i)))
        def _():
            for h in range(2):
                p_copy(i, h).wait_send()
    for j in range(1, ntp):
        for q in range(3):
            tp_push(lambda o: ssq.at[q, o], qsend.at[q], qrecv.at[q], j, True).wait_send()
    for i in range(tok // BR):
        out_copy(i).wait()


def body(n, ntp, gate_branch, recur_input, doc_ids, conv_taps, gate_map, input_map, decay_level, decay_extra,
         out_weight, residual, mix_gain, pre_gain, ffn_gain, gate_weight, up_weight, down_weight):
    tok, loc = recur_input.shape
    dloc = residual.shape[1]
    krows, ff = gate_weight.shape
    ncol = down_weight.shape[1]
    heads, head, _ = gate_map.shape
    nz, ny = grid_of(n)
    planes = ny == 2 and nz > 3 and ntp == 4 and tok % 256 == 0 and ff % 128 == 0
    fb = ff // 128 * 2 // 11 * 128
    if planes:
        ids, taps, rate = doc_ids.reshape(tok // 128, 128), conv_taps, decay_level[None, :]
    else:
        ids = jnp.broadcast_to(doc_ids[:, None], (tok, 128))
        taps = conv_taps.astype(F32)
        rate = (GATE_POWER * -jax.nn.softplus(-decay_level))[None, :]
    args = (gate_branch, recur_input, ids, taps, gate_map.reshape(heads * head, head),
            input_map.reshape(heads * head, head), rate, decay_extra, out_weight, residual,
            mix_gain[None, :], pre_gain[None, :], ffn_gain[None, :], gate_weight, up_weight, down_weight)
    vm = pl.BlockSpec(memory_space=pltpu.VMEM)
    hbm = pl.BlockSpec(memory_space=pl.ANY)
    V, S = pltpu.VMEM, pltpu.SemaphoreType.DMA
    per = dloc // ncol
    chips = ntp // 2
    if planes:
        fn = plane_kernel
        in_specs = [hbm] * 2 + [vm] * 5 + [hbm] * 3 + [vm] * 3 + [hbm] * 3
        out_spec = hbm
        scratch = [
            V((tok, dloc), BF16), S((tok // math.gcd(tok, 128),)),
            V((tok, loc), BF16), V((tok, loc), BF16), V((tok, loc), F32), V(out_weight.shape, BF16), V((tok, dloc), BF16), S((5,)),
            V((n * krows, ff), BF16), V((n * krows, ff), BF16), V((n, ff, ncol), BF16),
            V((tok + 8, loc), F32), V((tok + 8, 128), jnp.int32), V((16, loc), BF16), V((tok // 128, 128), jnp.int32),
            V((2, loc, loc), BF16), V((tok, loc), F32), V((tok, loc), F32), V((n, 16, loc), F32),
            V((ntp, tok, loc), BF16), V((tok, dloc), BF16), V((tok, dloc), BF16), V((tok, dloc), BF16), V((tok, dloc * ntp), BF16),
            V((tok, dloc * ntp), BF16), V((tok, fb), BF16), V((tok, ff), F32), V((tok, ff), F32), V((tok, ff), BF16), V((n, tok, ncol), BF16), V((ny * chips, per, tok, ncol), BF16), V((3, ntp, 8, tok), F32),
            S((7,)), S((7,)), S((7,)), S((2, 7, nz)), S((7, nz)), S((7, nz)), S((7, nz)),
            S((2,)), S((2,)), S((n - 1,)), S((n - 1,)), S((ntp - 1,)), S((ntp - 1,)),
            S((2, ny, chips)), S((2, ntp)), S((2, 2)), S((2, 2, ntp)), S((2,)), S((2,)), S((3, ntp - 1)), S((3, ntp - 1)), S((n, 2)), S((ny * chips, per, 2)),
        ]
    else:
        fn = kernel
        in_specs = [vm] * 13 + [hbm] * 3
        out_spec = vm
        scratch = [
            V((n * krows, ff), BF16), V((n * krows, ff), BF16), V((n, ff, ncol), BF16),
            V((tok + 8, loc), F32), V((tok + 8, 128), jnp.int32), V((16, loc), BF16), V((8, 128), jnp.int32),
            V((2, loc, loc), BF16), V((tok, loc), F32), V((tok, loc), F32), V((n, 16, loc), F32),
            V((ntp, tok, loc), BF16), V((tok, dloc), BF16), V((tok, dloc * ntp), BF16), V((tok, ff), BF16),
            V((n, tok, ncol), BF16), V((n, tok, ncol), BF16), V((chips - 1, per, tok, ncol), BF16), V((per, tok, ncol), BF16),
            V((3, ntp, 8, tok), F32),
            S((3, 2, n - 1)), S((3, 2, n - 1)), S((3,)), S((2,)), S((2,)), S((n - 1,)), S((n - 1,)),
            S((ntp - 1,)), S((ntp - 1,)), S((ntp - 1,)), S((ntp - 1,)), S((3, ntp - 1)), S((3, ntp - 1)),
            S((n,)), S((chips - 1, per)), S((n,)),
        ]
    return pl.pallas_call(
        functools.partial(fn, (n, ntp, nz, ny, dloc * ntp)),
        out_shape=jax.ShapeDtypeStruct((tok, dloc), BF16),
        in_specs=in_specs,
        out_specs=out_spec,
        scratch_shapes=scratch,
        compiler_params=pltpu.CompilerParams(
            collective_id=0, has_side_effects=True, vmem_limit_bytes=62 * 1024 * 1024),
    )(*args)


def solution(mesh):
    in_specs = (
        P("sp", "tp"), P("sp", "tp"), P("sp"), P(None, "tp"), P("tp", None, None), P("tp", None, None),
        P("tp"), P("sp", "tp"), P(None, "tp"), P("sp", "tp"), P("tp"), P("tp"), P("tp"),
        P("sp", "tp"), P("sp", "tp"), P("tp", "sp"),
    )
    fn = functools.partial(body, mesh.shape["sp"], mesh.shape["tp"])
    return jax.shard_map(fn, mesh=mesh, in_specs=in_specs, out_specs=P("sp", "tp"), check_vma=False)
```
